32 devices in a mesh: kv: 16 (over z, y, x), tp: 2 (over core).
Axes of the slice: x: 2, y: 2, z: 4, core: 2. Of those that a mesh axis runs over, the one named last changes fastest.
Arguments:
- tokens: bfloat16 [16, 4096], P(None, ('kv', 'tp')), may hold values from -12 to 12
- lengths: int32 [16], replicated, may hold values from 1 to 2048, 10922 in all
- attn_gain: bfloat16 [4096], P('kv'), may hold values from 0.099609375 to 1.8984375
- w_query: bfloat16 [4096, 2048], P('kv', 'tp'), may hold values from -0.09375 to 0.09375
- w_key: bfloat16 [4096, 2048], P('kv', 'tp'), may hold values from -0.09375 to 0.09375
- w_value: bfloat16 [4096, 4096], P('kv', 'tp'), may hold values from -0.09375 to 0.09375
- w_gate: bfloat16 [4096, 4096], P('kv', 'tp'), may hold values from -0.09375 to 0.09375
- decay_rate: float32 [32], P('tp'), may hold values from 4.8828125e-05 to 0.05
- key_cache: bfloat16 [16, 2048, 2048], P(None, 'kv', 'tp'), may hold values from -6 to 6
- value_cache: bfloat16 [16, 2048, 4096], P(None, 'kv', 'tp'), may hold values from -6 to 6
- head_gain: bfloat16 [4096], P('tp'), may hold values from 0.099609375 to 1.8984375
- w_output: bfloat16 [4096, 4096], P('tp', 'kv'), may hold values from -0.09375 to 0.09375
- mlp_gain: bfloat16 [4096], replicated, may hold values from 0.099609375 to 1.8984375
- w_up: bfloat16 [4096, 16384], P(None, ('kv', 'tp')), may hold values from -0.09375 to 0.09375
- w_down: bfloat16 [16384, 4096], P(('kv', 'tp')), may hold values from -0.09375 to 0.09375
Outputs:
- layer_out: bfloat16 [16, 4096], P(None, ('kv', 'tp'))
The draws below stay inside these ranges and needn't reach their ends.
Inputs may be any that keep to these rules, and one draw needn't show every extreme that they name: Sequence s has lengths[s] live cache positions, 0 to lengths[s] - 1, and its new token stands at position lengths[s]; the longest fills all 2048 positions.
All inputs are finite; a program needn't handle non-finite values.
Results may differ from the reference program's by a relative error of at most 0.012.
Values may be sent and summed in bfloat16 or wider, within the bound.
No kernel may reach another device: no remote copies, remote signals or barrier semaphores. Data moves between devices by JAX's collectives and lax.ppermute only.
A program may use at most 64 MiB of HBM per device.

```python
import math
import jax
import jax.numpy as jnp
import numpy as np
from jax import lax

WIDTH = 4096
HEADS = 32
HEAD_KEY = 64
HEAD_VALUE = 128
MLP_UNITS = 16384
SEQS = 16
CACHE = 2048
GROUP_HEADS = 16
N_TP = 2


def draw_tokens(key, part):
    subkeys = jax.random.split(key, 4)
    column = jnp.arange(WIDTH, dtype=jnp.float32) / WIDTH
    col_scale = 0.5 * jnp.exp(column * jnp.log(6.0)) * jnp.exp(0.3 * jax.random.normal(subkeys[0], (WIDTH,), jnp.float32))
    drawn = col_scale * jax.random.normal(subkeys[3], (SEQS, WIDTH), jnp.float32)
    return jnp.clip(drawn, -12.0, 12.0).astype(jnp.bfloat16)


def draw_decay_rate(key, part):
    subkeys = jax.random.split(key, 3)
    slow_rate = jnp.exp(jax.random.uniform(subkeys[0], (HEADS,), jnp.float32, jnp.log(0.1 / CACHE), jnp.log(2.0 / CACHE)))
    fast_rate = jnp.exp(jax.random.uniform(subkeys[1], (HEADS,), jnp.float32, jnp.log(1.0 / 60.0), jnp.log(1.0 / 20.0)))
    chance = 0.5
    is_fast = jax.random.uniform(subkeys[2], (HEADS,), jnp.float32) < chance
    return jnp.where(is_fast, fast_rate, slow_rate).astype(jnp.float32)


def with_spikes(values, stream_key, source, target, parts, factor):
    owner, partner = [(jnp.arange(values.shape[dim]) // (values.shape[dim] // parts)).reshape([-1 if axis == dim else 1 for axis in range(values.ndim)]) for dim in (source, target)]
    chosen = jax.random.permutation(stream_key, parts)[partner]
    strong = (owner == chosen) | (owner == (partner + parts // 2) % parts)
    return jnp.where(strong, factor * values, values)


def block_levels(rng, shape, pieces, least, largest):
    level = 1.0
    for dim, blocks in pieces:
        heights = jax.random.uniform(jax.random.fold_in(jax.random.fold_in(rng, 6), dim), (blocks,), jnp.float32, least / len(pieces), largest / len(pieces))
        level = level * jnp.repeat(jnp.exp(heights), shape[dim] // blocks).reshape((-1,) + (1,) * (len(shape) - 1 - dim))
    return level


def length_profile(number_of, total, most, lean):
    portions = [(1 << 20) // math.isqrt(rank ** lean) + 1 for rank in range(2, number_of + 1)]
    surplus, counts = total - most - (number_of - 1), [1] * (number_of - 1)
    while surplus > 0:
        candidates = [i for i in range(number_of - 1) if counts[i] < most]
        whole, left = sum([portions[i] for i in candidates]), surplus
        for i in candidates:
            extra = min(most - counts[i], max(1, left * portions[i] // whole), surplus)
            counts[i] = counts[i] + extra
            surplus = surplus - extra
    return np.array([most] + counts)


def ragged(key, count, total, limit, skew):
    if count == 2:
        one = jax.random.randint(key, (), max(1, total - limit), min(limit, total - 1) + 1)
        return jnp.stack([one, total - one])
    sizes = jnp.asarray(length_profile(count, total, limit, skew), jnp.int32)
    couples = (count - 1) // 2
    giver, sink = sizes[1:1 + 2 * couples:2], sizes[2:2 + 2 * couples:2]
    room = jnp.minimum(giver - 1, limit - sink)
    shifted = jax.random.randint(jax.random.fold_in(key, 1), (couples,), 0, 1 << 20) % (room + 1)
    sizes = sizes.at[1:1 + 2 * couples:2].set(giver - shifted).at[2:2 + 2 * couples:2].set(sink + shifted)
    return sizes[jax.random.permutation(jax.random.fold_in(key, 2), count)]


def bell_draw(own_key, dims, deviation, limit, cuts=(), held_as=jnp.bfloat16):
    gain = block_levels(own_key, dims, cuts, -0.22, 0.18) if cuts else 1.0
    values = jax.random.normal(own_key, dims, jnp.float32) * deviation * gain
    return jnp.minimum(jnp.maximum(values, -limit), limit).astype(held_as)


def gaussian_with(key, dims, width, bound, shards, heavy, kind=jnp.bfloat16):
    values = width * jax.random.normal(key, dims, jnp.float32)
    if shards:
        values = values * block_levels(key, dims, shards, -0.22, 0.18)
    return jnp.clip(with_spikes(values, jax.random.fold_in(key, 3), *heavy), -bound, bound).astype(kind)


def setup_inputs(seed: int = 0) -> dict:
    arg_keys = jax.random.split(jax.random.key(seed), 16)
    return {
        "tokens": draw_tokens(jax.random.fold_in(arg_keys[15], 71), 0),
        "lengths": ragged(arg_keys[1], SEQS, SEQS * CACHE // 3, CACHE, 2).astype(jnp.int32),
        "attn_gain": jnp.clip(1.0 + 0.18 * jax.random.normal(arg_keys[2], (WIDTH,), jnp.float32), 0.099609375, 1.8984375).astype(jnp.bfloat16),
        "w_query": bell_draw(arg_keys[3], (WIDTH, HEADS * HEAD_KEY), WIDTH ** -0.5, 0.09375, ((0, 16), (1, 2))),
        "w_key": bell_draw(arg_keys[4], (WIDTH, HEADS * HEAD_KEY), WIDTH ** -0.5, 0.09375, ((0, 16), (1, 2))),
        "w_value": bell_draw(arg_keys[5], (WIDTH, HEADS * HEAD_VALUE), WIDTH ** -0.5, 0.09375, ((0, 16), (1, 2))),
        "w_gate": bell_draw(arg_keys[6], (WIDTH, HEADS * HEAD_VALUE), WIDTH ** -0.5, 0.09375, ((0, 16), (1, 2))),
        "decay_rate": draw_decay_rate(jax.random.fold_in(arg_keys[15], 71), 0),
        "key_cache": bell_draw(arg_keys[8], (SEQS, CACHE, HEADS * HEAD_KEY), 1.0, 6.0, ((1, 16), (2, 2))),
        "value_cache": bell_draw(arg_keys[9], (SEQS, CACHE, HEADS * HEAD_VALUE), 1.0, 6.0, ((1, 16), (2, 2))),
        "head_gain": jnp.clip(1.0 + 0.18 * jax.random.normal(arg_keys[10], (HEADS * HEAD_VALUE,), jnp.float32), 0.099609375, 1.8984375).astype(jnp.bfloat16),
        "w_output": bell_draw(arg_keys[11], (HEADS * HEAD_VALUE, WIDTH), (HEADS * HEAD_VALUE) ** -0.5, 0.09375, ((0, 2), (1, 16))),
        "mlp_gain": jnp.clip(1.0 + 0.18 * jax.random.normal(arg_keys[12], (WIDTH,), jnp.float32), 0.099609375, 1.8984375).astype(jnp.bfloat16),
        "w_up": bell_draw(arg_keys[13], (WIDTH, MLP_UNITS), WIDTH ** -0.5, 0.09375, ((1, 32),)),
        "w_down": gaussian_with(arg_keys[14], (MLP_UNITS, WIDTH), MLP_UNITS ** -0.5, 0.09375, ((0, 32),), (0, 1, 32, 2.75)),
    }


EPS = 1e-05
THETA = 10000.0

def scale_after(inputs, gain_vec, weights):
    scaled = (inputs.astype(jnp.float32) * gain_vec.astype(jnp.float32)).astype(jnp.bfloat16)
    product_sum = jnp.dot(scaled, weights, preferred_element_type=jnp.float32)
    column = jnp.dot(gain_vec[None, :], weights, preferred_element_type=jnp.float32)
    widened = inputs.astype(jnp.float32)
    average = lax.optimization_barrier(jnp.sum(widened, -1, keepdims=True)) / WIDTH
    spread = lax.optimization_barrier(jnp.sum(widened * widened, -1, keepdims=True)) / WIDTH - average * average
    return lax.rsqrt(spread + EPS) * (product_sum - average * column)

def rotate(flattened, position):
    row_count = flattened.shape[0]
    grouped = flattened.reshape(row_count, -1, HEAD_KEY)
    halfway = HEAD_KEY // 2
    inverse = jnp.power(THETA, -jnp.arange(halfway, dtype=jnp.float32) / halfway)
    angles = position.astype(jnp.float32)[:, None] * inverse[None, :]
    cosine = jnp.cos(angles)[:, None, :]
    sine_part = jnp.sin(angles)[:, None, :]
    first_half = grouped[..., :halfway]
    second_half = grouped[..., halfway:]
    turned = jnp.concatenate([first_half * cosine - second_half * sine_part, second_half * cosine + first_half * sine_part], -1)
    return turned.reshape(row_count, -1)

def attend_cache(queries, key_cache, value_cache, lengths, decay_rate):
    places = jnp.arange(CACHE, dtype=jnp.int32)

    def one_sequence(bundle):
        query_row, key_rows, value_rows, length_one = bundle
        key_rows = key_rows.reshape(CACHE, HEADS, HEAD_KEY).astype(jnp.float32)
        value_rows = value_rows.reshape(CACHE, HEADS, HEAD_VALUE).astype(jnp.float32)
        scores = jnp.einsum('hd,jhd->hj', query_row.astype(jnp.float32), key_rows) * HEAD_KEY ** (-0.5)
        distance = jnp.maximum(length_one - places, 0).astype(jnp.float32)
        weights = jnp.where((places < length_one)[None, :], jnp.exp(-decay_rate[:, None] * distance[None, :]), 0.0)
        coefficients = lax.optimization_barrier((scores * weights).astype(jnp.bfloat16)).astype(jnp.float32)
        return jnp.einsum('hj,jhe->he', coefficients, value_rows)
    return lax.map(one_sequence, (queries, key_cache, value_cache, lengths))

def reference(tokens, lengths, attn_gain, w_query, w_key, w_value, w_gate, decay_rate, key_cache, value_cache, head_gain, w_output, mlp_gain, w_up, w_down):
    seq_count = tokens.shape[0]
    query_rows = rotate(scale_after(tokens, attn_gain, w_query), lengths).astype(jnp.bfloat16)
    new_key = rotate(scale_after(tokens, attn_gain, w_key), lengths).astype(jnp.bfloat16)
    new_value = scale_after(tokens, attn_gain, w_value).astype(jnp.bfloat16)
    gate_value = scale_after(tokens, attn_gain, w_gate)
    queries = query_rows.reshape(seq_count, HEADS, HEAD_KEY)
    cached = attend_cache(queries, key_cache, value_cache, lengths, decay_rate)
    own_score = lax.optimization_barrier(jnp.sum(queries.astype(jnp.float32) * new_key.reshape(seq_count, HEADS, HEAD_KEY).astype(jnp.float32), -1)) * HEAD_KEY ** (-0.5)
    retained = cached + own_score[:, :, None] * new_value.reshape(seq_count, HEADS, HEAD_VALUE).astype(jnp.float32)
    centered = retained - lax.optimization_barrier(jnp.mean(retained, -1, keepdims=True))
    normed = centered * lax.rsqrt(lax.optimization_barrier(jnp.mean(centered * centered, -1, keepdims=True)) + EPS) * head_gain.reshape(HEADS, HEAD_VALUE).astype(jnp.float32)
    gated_out = (jax.nn.silu(gate_value) * normed.reshape(seq_count, -1)).astype(jnp.bfloat16)
    group_cols = GROUP_HEADS * HEAD_VALUE
    branch = jnp.zeros((seq_count, WIDTH), jnp.float32)
    for member in range(N_TP):
        piece_out = jnp.dot(gated_out[:, member * group_cols:(member + 1) * group_cols], w_output[member * group_cols:(member + 1) * group_cols], preferred_element_type=jnp.float32).astype(jnp.bfloat16)
        branch = branch + lax.optimization_barrier(piece_out).astype(jnp.float32)
    residual = (tokens.astype(jnp.float32) + branch).astype(jnp.bfloat16)
    hidden = jnp.square(jax.nn.relu(scale_after(residual, mlp_gain, w_up))).astype(jnp.bfloat16)
    layer_out = residual.astype(jnp.float32) + jnp.dot(hidden, w_down, preferred_element_type=jnp.float32)
    return layer_out.astype(jnp.bfloat16)
```

```python
import jax
import jax.numpy as jnp
from jax import lax
from jax.sharding import PartitionSpec as P

HEAD_KEY = 64
HEAD_VALUE = 128
EPS = 1e-05
THETA = 10000.0

BF = jnp.bfloat16
F32 = jnp.float32


def split_two(x):
    high = x.astype(BF)
    return high, (x - high.astype(F32)).astype(BF)


def rotate(flat, cosine, sine):
    rows = flat.shape[0]
    grouped = flat.reshape(rows, -1, HEAD_KEY)
    half = HEAD_KEY // 2
    a, b = grouped[..., :half], grouped[..., half:]
    c, s = cosine[:, None, :], sine[:, None, :]
    return jnp.concatenate([a * c - b * s, b * c + a * s], -1).reshape(rows, -1)


def broadcast_gather(x, axes, size):
    spread = jnp.broadcast_to(x[None], (size,) + x.shape)
    return lax.all_to_all(spread, axes, 0, 0, tiled=True)


def make_on_device(kv, tp):
    def on_device(
        tokens,
        lengths,
        attn_gain,
        w_query,
        w_key,
        w_value,
        w_gate,
        decay_rate,
        key_cache,
        value_cache,
        head_gain,
        w_output,
        mlp_gain,
        w_up,
        w_down,
    ):
        S = tokens.shape[0]
        H = decay_rate.shape[0]
        span = key_cache.shape[1]
        width = tokens.shape[1] * kv * tp
        own = tokens.shape[1]
        kvi = lax.axis_index("kv")
        tpi = lax.axis_index("tp")
        groups = kv // H
        rows = S // groups

        if tp == 2:
            other = lax.ppermute(tokens, "tp", [(0, 1), (1, 0)])
            low = jnp.where(tpi == 0, tokens, other)
            high = jnp.where(tpi == 0, other, tokens)
            block = jnp.concatenate([low, high], 1)
        else:
            block = lax.all_gather(tokens, "tp", axis=1, tiled=True)
        wide = block.astype(F32)
        scaled = (wide * attn_gain.astype(F32)).astype(BF)
        lhs = jnp.concatenate([scaled, attn_gain[None, :]], 0)
        part_q = jnp.dot(lhs, w_query, preferred_element_type=F32)
        moments = jnp.stack([jnp.sum(wide, -1), jnp.sum(wide * wide, -1)], -1)

        small = jnp.concatenate([part_q[S], moments.reshape(-1)])
        q_sum = part_q[:S]
        stride = 1
        while stride < kv:
            count = 4 if kv % (stride * 4) == 0 else 2
            high, low = split_two(small)
            tail = jnp.concatenate([high, low])
            pad = -tail.shape[0] % S
            tail = jnp.pad(tail, (0, pad)).reshape(S, -1)
            message = jnp.concatenate([q_sum.astype(BF), tail], 1)
            for j in range(1, count):
                got = lax.ppermute(message, "kv", [(i, i ^ (j * stride)) for i in range(kv)])
                got = got.astype(F32)
                q_sum = q_sum + got[:, : q_sum.shape[1]]
                flat = got[:, q_sum.shape[1] :].reshape(-1)
                n = small.shape[0]
                small = small + flat[:n] + flat[n : 2 * n]
            stride *= count
        csum_q = small[: q_sum.shape[1]]
        moments = small[q_sum.shape[1] :].reshape(S, 2)
        average = moments[:, 0] / width
        inverse = lax.rsqrt(moments[:, 1] / width - average * average + EPS)

        half = HEAD_KEY // 2
        turn = jnp.power(THETA, -jnp.arange(half, dtype=F32) / half)
        angles = lengths.astype(F32)[:, None] * turn[None, :]
        q_plain = inverse[:, None] * (q_sum - average[:, None] * csum_q[None, :])
        queries = rotate(q_plain, jnp.cos(angles), jnp.sin(angles)).astype(BF)
        queries = queries.reshape(S, H, HEAD_KEY)

        def partial(w):
            p = jnp.dot(lhs, w, preferred_element_type=F32)
            return inverse[:, None] * (p[:S] - average[:, None] * p[S:])

        part_k = partial(w_key).reshape(S, H, HEAD_KEY)
        part_v = partial(w_value).reshape(S, H, HEAD_VALUE)
        part_g = partial(w_gate).reshape(S, H, HEAD_VALUE)
        part_score = jnp.sum(q_plain.reshape(S, H, HEAD_KEY) * part_k, -1) * HEAD_KEY ** (-0.5)

        keys = key_cache.reshape(S, span, H, HEAD_KEY)
        values = value_cache.reshape(S, span, H, HEAD_VALUE)
        scores = jnp.einsum("bhd,bjhd->bhj", queries, keys, preferred_element_type=F32)
        places = kvi * span + jnp.arange(span, dtype=jnp.int32)
        distance = jnp.maximum(lengths[:, None] - places[None, :], 0).astype(F32)
        live = (places[None, :] < lengths[:, None])[:, None, :]
        decays = jnp.where(
            live, jnp.exp(-decay_rate[None, :, None] * distance[:, None, :]), 0.0
        )
        coefficients = (scores * HEAD_KEY ** (-0.5) * decays).astype(BF)
        part_c = jnp.einsum("bhj,bjhe->bhe", coefficients, values, preferred_element_type=F32)

        high, low = split_two(part_score)
        pieces = jnp.concatenate(
            [
                part_c.astype(BF),
                part_v.astype(BF),
                part_g.astype(BF),
                high[..., None],
                low[..., None],
                jnp.zeros((S, H, 126), BF),
            ],
            -1,
        )
        pieces = pieces.transpose(1, 0, 2).reshape(kv, rows, 4 * HEAD_VALUE)
        mine = jnp.sum(
            lax.all_to_all(pieces, "kv", 0, 0, tiled=True).astype(F32), 0
        )
        cached, value, gate = (
            mine[:, i * HEAD_VALUE : (i + 1) * HEAD_VALUE] for i in range(3)
        )
        score = mine[:, 3 * HEAD_VALUE] + mine[:, 3 * HEAD_VALUE + 1]
        retained = cached + score[:, None] * value
        centered = retained - jnp.mean(retained, -1, keepdims=True)
        gain = lax.dynamic_slice(head_gain, ((kvi // groups) * HEAD_VALUE,), (HEAD_VALUE,))
        normed = (
            centered
            * lax.rsqrt(jnp.mean(centered * centered, -1, keepdims=True) + EPS)
            * gain.astype(F32)
        )
        gated = (jax.nn.silu(gate) * normed).astype(BF)
        gathered = broadcast_gather(gated, "kv", kv).reshape(H, S, HEAD_VALUE)
        gathered = gathered.transpose(1, 0, 2).reshape(S, H * HEAD_VALUE)
        part_b = jnp.dot(gathered, w_output, preferred_element_type=F32).astype(BF)
        part_b = part_b.reshape(S, tp, own).transpose(1, 0, 2)
        if tp == 2:
            keep = jnp.where(tpi == 0, part_b[0], part_b[1])
            send = jnp.where(tpi == 0, part_b[1], part_b[0])
            got = lax.ppermute(send, "tp", [(0, 1), (1, 0)])
            branch = keep.astype(F32) + got.astype(F32)
        else:
            branch = jnp.sum(
                lax.all_to_all(part_b, "tp", 0, 0, tiled=True).astype(F32), 0
            )
        own_residual = (tokens.astype(F32) + branch).astype(BF)

        residual = broadcast_gather(own_residual, ("kv", "tp"), kv * tp)
        residual = residual.transpose(1, 0, 2).reshape(S, width)
        wide = residual.astype(F32)
        scaled = (wide * mlp_gain.astype(F32)).astype(BF)
        lhs = jnp.concatenate([scaled, mlp_gain[None, :]], 0)
        up = jnp.dot(lhs, w_up, preferred_element_type=F32)
        average = jnp.sum(wide, -1) / width
        inverse = lax.rsqrt(jnp.sum(wide * wide, -1) / width - average * average + EPS)
        hidden = inverse[:, None] * (up[:S] - average[:, None] * up[S:])
        hidden = jnp.square(jax.nn.relu(hidden)).astype(BF)
        down = jnp.dot(hidden, w_down, preferred_element_type=F32).astype(BF)
        down = down.reshape(S, kv * tp, own).transpose(1, 0, 2)
        mixer = jnp.sum(
            lax.all_to_all(down, ("kv", "tp"), 0, 0, tiled=True).astype(F32), 0
        )
        return (own_residual.astype(F32) + mixer).astype(BF)

    return on_device


def solution(mesh):
    in_specs = (
        P(None, ("kv", "tp")),
        P(),
        P("kv"),
        P("kv", "tp"),
        P("kv", "tp"),
        P("kv", "tp"),
        P("kv", "tp"),
        P("tp"),
        P(None, "kv", "tp"),
        P(None, "kv", "tp"),
        P("tp"),
        P("tp", "kv"),
        P(),
        P(None, ("kv", "tp")),
        P(("kv", "tp"), None),
    )
    return jax.shard_map(
        make_on_device(mesh.shape["kv"], mesh.shape["tp"]),
        mesh=mesh,
        in_specs=in_specs,
        out_specs=P(None, ("kv", "tp")),
        check_vma=False,
    )
```

```python
import functools
import math

import jax
import jax.numpy as jnp
from jax import lax
from jax.experimental import pallas as pl
from jax.experimental.pallas import tpu as pltpu
from jax.sharding import PartitionSpec as P

HEAD_KEY = 64
HEAD_VALUE = 128
EPS = 1e-05
THETA = 10000.0
LANES = 128

BF = jnp.bfloat16
F32 = jnp.float32


def split_two(x):
    high = x.astype(BF)
    return high, (x - high.astype(F32)).astype(BF)


def rotate(flat, cosine, sine):
    rows = flat.shape[0]
    grouped = flat.reshape(rows, -1, HEAD_KEY)
    half = HEAD_KEY // 2
    a, b = grouped[..., :half], grouped[..., half:]
    c, s = cosine[:, None, :], sine[:, None, :]
    return jnp.concatenate([a * c - b * s, b * c + a * s], -1).reshape(rows, -1)


def broadcast_gather(x, axes, size):
    spread = jnp.broadcast_to(x[None], (size,) + x.shape)
    return lax.all_to_all(spread, axes, 0, 0, tiled=True)


def make_on_device(kv, tp):
    def on_device(
        tokens,
        lengths,
        attn_gain,
        w_query,
        w_key,
        w_value,
        w_gate,
        decay_rate,
        key_cache,
        value_cache,
        head_gain,
        w_output,
        mlp_gain,
        w_up,
        w_down,
    ):
        S = tokens.shape[0]
        H = decay_rate.shape[0]
        span = key_cache.shape[1]
        width = tokens.shape[1] * kv * tp
        own = tokens.shape[1]
        kvi = lax.axis_index("kv")
        tpi = lax.axis_index("tp")
        groups = kv // H
        rows = S // groups

        if tp == 2:
            other = lax.ppermute(tokens, "tp", [(0, 1), (1, 0)])
            low = jnp.where(tpi == 0, tokens, other)
            high = jnp.where(tpi == 0, other, tokens)
            block = jnp.concatenate([low, high], 1)
        else:
            block = lax.all_gather(tokens, "tp", axis=1, tiled=True)
        wide = block.astype(F32)
        scaled = (wide * attn_gain.astype(F32)).astype(BF)
        lhs = jnp.concatenate([scaled, attn_gain[None, :]], 0)
        part_q = jnp.dot(lhs, w_query, preferred_element_type=F32)
        moments = jnp.stack([jnp.sum(wide, -1), jnp.sum(wide * wide, -1)], -1)

        small = jnp.concatenate([part_q[S], moments.reshape(-1)])
        q_sum = part_q[:S]
        stride = 1
        while stride < kv:
            count = 4 if kv % (stride * 4) == 0 else 2
            high, low = split_two(small)
            tail = jnp.concatenate([high, low])
            pad = -tail.shape[0] % S
            tail = jnp.pad(tail, (0, pad)).reshape(S, -1)
            message = jnp.concatenate([q_sum.astype(BF), tail], 1)
            for j in range(1, count):
                got = lax.ppermute(message, "kv", [(i, i ^ (j * stride)) for i in range(kv)])
                got = got.astype(F32)
                q_sum = q_sum + got[:, : q_sum.shape[1]]
                flat = got[:, q_sum.shape[1] :].reshape(-1)
                n = small.shape[0]
                small = small + flat[:n] + flat[n : 2 * n]
            stride *= count
        csum_q = small[: q_sum.shape[1]]
        moments = small[q_sum.shape[1] :].reshape(S, 2)
        average = moments[:, 0] / width
        inverse = lax.rsqrt(moments[:, 1] / width - average * average + EPS)

        half = HEAD_KEY // 2
        turn = jnp.power(THETA, -jnp.arange(half, dtype=F32) / half)
        angles = lengths.astype(F32)[:, None] * turn[None, :]
        q_plain = inverse[:, None] * (q_sum - average[:, None] * csum_q[None, :])
        queries = rotate(q_plain, jnp.cos(angles), jnp.sin(angles)).astype(BF)
        queries = queries.reshape(S, H, HEAD_KEY)

        def partial(w):
            p = jnp.dot(lhs, w, preferred_element_type=F32)
            return inverse[:, None] * (p[:S] - average[:, None] * p[S:])

        part_k = partial(w_key).reshape(S, H, HEAD_KEY)
        part_v = partial(w_value).reshape(S, H, HEAD_VALUE)
        part_g = partial(w_gate).reshape(S, H, HEAD_VALUE)
        part_score = jnp.sum(q_plain.reshape(S, H, HEAD_KEY) * part_k, -1) * HEAD_KEY ** (-0.5)

        keys = key_cache.reshape(S, span, H, HEAD_KEY)
        values = value_cache.reshape(S, span, H, HEAD_VALUE)
        scores = jnp.einsum("bhd,bjhd->bhj", queries, keys, preferred_element_type=F32)
        places = kvi * span + jnp.arange(span, dtype=jnp.int32)
        distance = jnp.maximum(lengths[:, None] - places[None, :], 0).astype(F32)
        live = (places[None, :] < lengths[:, None])[:, None, :]
        decays = jnp.where(
            live, jnp.exp(-decay_rate[None, :, None] * distance[:, None, :]), 0.0
        )
        coefficients = (scores * HEAD_KEY ** (-0.5) * decays).astype(BF)
        part_c = jnp.einsum("bhj,bjhe->bhe", coefficients, values, preferred_element_type=F32)

        high, low = split_two(part_score)
        pieces = jnp.concatenate(
            [
                part_c.astype(BF),
                part_v.astype(BF),
                part_g.astype(BF),
                high[..., None],
                low[..., None],
                jnp.zeros((S, H, 126), BF),
            ],
            -1,
        )
        pieces = pieces.transpose(1, 0, 2).reshape(kv, rows, 4 * HEAD_VALUE)
        mine = jnp.sum(
            lax.all_to_all(pieces, "kv", 0, 0, tiled=True).astype(F32), 0
        )
        cached, value, gate = (
            mine[:, i * HEAD_VALUE : (i + 1) * HEAD_VALUE] for i in range(3)
        )
        score = mine[:, 3 * HEAD_VALUE] + mine[:, 3 * HEAD_VALUE + 1]
        retained = cached + score[:, None] * value
        centered = retained - jnp.mean(retained, -1, keepdims=True)
        gain = lax.dynamic_slice(head_gain, ((kvi // groups) * HEAD_VALUE,), (HEAD_VALUE,))
        normed = (
            centered
            * lax.rsqrt(jnp.mean(centered * centered, -1, keepdims=True) + EPS)
            * gain.astype(F32)
        )
        gated = (jax.nn.silu(gate) * normed).astype(BF)
        gathered = broadcast_gather(gated, "kv", kv).reshape(H, S, HEAD_VALUE)
        gathered = gathered.transpose(1, 0, 2).reshape(S, H * HEAD_VALUE)
        part_b = jnp.dot(gathered, w_output, preferred_element_type=F32).astype(BF)
        part_b = part_b.reshape(S, tp, own).transpose(1, 0, 2)
        if tp == 2:
            keep = jnp.where(tpi == 0, part_b[0], part_b[1])
            send = jnp.where(tpi == 0, part_b[1], part_b[0])
            got = lax.ppermute(send, "tp", [(0, 1), (1, 0)])
            branch = keep.astype(F32) + got.astype(F32)
        else:
            branch = jnp.sum(
                lax.all_to_all(part_b, "tp", 0, 0, tiled=True).astype(F32), 0
            )
        own_residual = (tokens.astype(F32) + branch).astype(BF)

        residual = broadcast_gather(own_residual, ("kv", "tp"), kv * tp)
        residual = residual.transpose(1, 0, 2).reshape(S, width)
        wide = residual.astype(F32)
        scaled = (wide * mlp_gain.astype(F32)).astype(BF)
        lhs = jnp.concatenate([scaled, mlp_gain[None, :]], 0)
        up = jnp.dot(lhs, w_up, preferred_element_type=F32)
        average = jnp.sum(wide, -1) / width
        inverse = lax.rsqrt(jnp.sum(wide * wide, -1) / width - average * average + EPS)
        hidden = inverse[:, None] * (up[:S] - average[:, None] * up[S:])
        hidden = jnp.square(jax.nn.relu(hidden)).astype(BF)
        down = jnp.dot(hidden, w_down, preferred_element_type=F32).astype(BF)
        down = down.reshape(S, kv * tp, own).transpose(1, 0, 2)
        mixer = jnp.sum(
            lax.all_to_all(down, ("kv", "tp"), 0, 0, tiled=True).astype(F32), 0
        )
        return (own_residual.astype(F32) + mixer).astype(BF)

    return on_device


def lane_ids(rows):
    return lax.broadcasted_iota(jnp.int32, (rows, LANES), 1)


def row_ids(rows, columns=LANES):
    return lax.broadcasted_iota(jnp.int32, (rows, columns), 0)


def column_of(scalars, rows, dtype):
    ids = row_ids(rows)
    out = jnp.zeros((rows, LANES), dtype)
    for i in range(rows):
        out = jnp.where(ids == i, scalars[i].astype(dtype), out)
    return out


def projection_rows(first, second, gain):
    t = lax.axis_index("tp")
    a, b = first[...].astype(F32), second[...].astype(F32)
    wide = jnp.concatenate([jnp.where(t == 0, a, b), jnp.where(t == 0, b, a)], 1)
    row = gain[...]
    scaled = (wide * row.astype(F32)).astype(BF)
    return jnp.concatenate([scaled, jnp.broadcast_to(row, scaled.shape)], 0), wide


def pack(q, csum, moments, message):
    columns = q.shape[1]
    half = csum.shape[0]
    message[:, :columns] = q.astype(BF)
    high = csum.astype(BF)
    low = (csum - high.astype(F32)).astype(BF)
    message[:, columns : columns + LANES] = jnp.concatenate([high, low], 0)
    high = moments.astype(BF).astype(F32)
    low = moments - high
    lanes = lane_ids(q.shape[0])
    both = jnp.where(lanes < 2, high, jnp.where(lanes < 4, pltpu.roll(low, 2, 1), 0.0))
    message[:, columns + LANES :] = both.astype(BF)
    assert 2 * half == q.shape[0]


def unpack_sum(state, messages):
    rows, total = state.shape
    columns = total - 2 * LANES
    half = rows // 2
    q = state[:, :columns]
    csum = state[:half, columns : columns + LANES]
    moments = state[:, columns + LANES :]
    for m in messages:
        q = q + m[:, :columns].astype(F32)
        c = m[:, columns : columns + LANES].astype(F32)
        csum = csum + c[:half] + c[half:]
        v = m[:, columns + LANES :].astype(F32)
        moments = moments + v + pltpu.roll(v, LANES - 2, 1)
    return q, csum, jnp.where(lane_ids(rows) < 2, moments, 0.0)


def store_state(q, csum, moments, state):
    columns = q.shape[1]
    state[:, :columns] = q
    state[:, columns : columns + LANES] = jnp.concatenate([csum, jnp.zeros_like(csum)], 0)
    state[:, columns + LANES :] = moments


def query_kernel(first, second, gain, w_query, state, message):
    lhs, wide = projection_rows(first, second, gain)
    rows = wide.shape[0]
    product = jnp.dot(lhs, w_query[...], preferred_element_type=F32)
    half = rows // 2
    ids = row_ids(half)
    csum = jnp.zeros((half, LANES), F32)
    for i in range(product.shape[1] // LANES):
        csum = jnp.where(
            ids == i, product[rows : rows + half, i * LANES : (i + 1) * LANES], csum
        )
    lanes = lane_ids(rows)
    first_sum = jnp.sum(wide, 1, keepdims=True)
    second_sum = jnp.sum(wide * wide, 1, keepdims=True)
    moments = jnp.where(lanes == 0, first_sum, jnp.where(lanes == 1, second_sum, 0.0))
    store_state(product[:rows], csum, moments, state)
    pack(product[:rows], csum, moments, message)


def middle_kernel(old, m1, m2, m3, state, message):
    q, csum, moments = unpack_sum(old, (m1, m2, m3))
    store_state(q, csum, moments, state)
    pack(q, csum, moments, message)


def other_kernel(lengths, first, second, gain, w_key, w_value, w_gate, k_out, v_out, g_out, turn):
    lhs, wide = projection_rows(first, second, gain)
    rows = wide.shape[0]
    for w, out in ((w_key, k_out), (w_value, v_out), (w_gate, g_out)):
        product = jnp.dot(lhs, w[...], preferred_element_type=F32)
        out[...] = product[: rows + 8]
    half = HEAD_KEY // 2
    entry = (lane_ids(rows) % half).astype(F32)
    inverse = jnp.exp(entry * (-math.log(THETA) / half))
    angle = column_of(lengths, rows, F32) * inverse
    turn[0] = jnp.cos(angle)
    turn[1] = jnp.sin(angle)


def attend_kernel(
    width,
    lengths,
    decay,
    old,
    m1,
    m2,
    m3,
    k_part,
    v_part,
    g_part,
    turn,
    keys,
    values,
    out,
    key_buffer,
    value_buffer,
    query_rows,
    cached,
    key_sem,
    value_sem,
):
    rows, span, key_columns = keys.shape
    heads = key_columns // HEAD_KEY

    def copies(s):
        return (
            pltpu.make_async_copy(keys.at[s], key_buffer.at[s], key_sem.at[s]),
            pltpu.make_async_copy(values.at[s], value_buffer.at[s], value_sem.at[s]),
        )

    for s in range(rows):
        for copy in copies(s):
            copy.start()

    q, csum, moments = unpack_sum(old, (m1, m2, m3))
    average = moments[:, 0:1] / width
    inverse = lax.rsqrt(moments[:, 1:2] / width - average * average + EPS)
    lanes = lane_ids(rows)
    in_first = lanes % HEAD_KEY < HEAD_KEY // 2
    low_head = lanes < HEAD_KEY
    cosine, sine = turn[0], turn[1]
    for i in range(key_columns // LANES):
        cut = slice(i * LANES, (i + 1) * LANES)
        plain = inverse * (q[:, cut] - average * csum[i : i + 1])
        partner = jnp.where(
            in_first,
            -pltpu.roll(plain, LANES - HEAD_KEY // 2, 1),
            pltpu.roll(plain, HEAD_KEY // 2, 1),
        )
        turned = plain * cosine + partner * sine
        query_rows[:, cut] = turned.astype(BF).astype(F32)
        part = inverse * (k_part[:rows, cut] - average * k_part[rows : rows + 1, cut])
        both = plain * part * HEAD_KEY ** (-0.5)
        for j in range(2):
            picked = jnp.where(low_head == (j == 0), both, 0.0)
            score = jnp.sum(picked, 1, keepdims=True)
            high = score.astype(BF).astype(F32)
            out[2 * i + j, :, 3 * LANES :] = jnp.where(low_head, high, score - high).astype(BF)
    for h in range(heads):
        cut = slice(h * LANES, (h + 1) * LANES)
        for place, part in ((1, v_part), (2, g_part)):
            normed = inverse * (part[:rows, cut] - average * part[rows : rows + 1, cut])
            out[h, :, place * LANES : (place + 1) * LANES] = normed.astype(BF)

    base = lax.axis_index("kv") * span
    places = base + lax.broadcasted_iota(jnp.int32, (heads, span), 1)
    rate = column_of(decay, heads, F32)
    if span != LANES:
        rate = jnp.broadcast_to(rate[:, :1], (heads, span))
    head_of_key = lax.broadcasted_iota(jnp.int32, (heads, key_columns), 1) // HEAD_KEY
    own_key = head_of_key == row_ids(heads, key_columns)
    value_columns = heads * HEAD_VALUE
    head_of_value = lax.broadcasted_iota(jnp.int32, (heads, value_columns), 1) // HEAD_VALUE
    own_value = head_of_value == row_ids(heads, value_columns)
    for s in range(rows):
        for copy in copies(s):
            copy.wait()
        spread = jnp.broadcast_to(query_rows[s : s + 1, :], (heads, key_columns))
        query = jnp.where(own_key, spread, 0.0).astype(BF)
        scores = lax.dot_general(
            query, key_buffer[s], (((1,), (1,)), ((), ())), preferred_element_type=F32
        )
        distance = lengths[s] - places
        weight = jnp.exp(-rate * jnp.maximum(distance, 0).astype(F32))
        weight = jnp.where(distance > 0, weight, 0.0)
        coefficients = (scores * HEAD_KEY ** (-0.5) * weight).astype(BF)
        product = jnp.dot(coefficients, value_buffer[s], preferred_element_type=F32)
        cached[s : s + 1, :] = jnp.sum(
            jnp.where(own_value, product, 0.0), 0, keepdims=True
        )
    for h in range(heads):
        out[h, :, :LANES] = cached[:, h * LANES : (h + 1) * LANES].astype(BF)


def gate_kernel(pieces, head_gain, out):
    total = jnp.sum(pieces[...].astype(F32), 0)
    cached, value, gate, score = (total[:, i * LANES : (i + 1) * LANES] for i in range(4))
    score = score[:, 0:1] + score[:, HEAD_KEY : HEAD_KEY + 1]
    retained = cached + score * value
    centered = retained - jnp.mean(retained, -1, keepdims=True)
    spread = lax.rsqrt(jnp.mean(centered * centered, -1, keepdims=True) + EPS)
    gains = head_gain[...].astype(F32)
    mine = row_ids(gains.shape[0]) == lax.axis_index("kv")
    gain = jnp.sum(jnp.where(mine, gains, 0.0), 0, keepdims=True)
    normed = centered * spread * gain
    gated = (gate * jax.nn.sigmoid(gate) * normed).astype(BF)
    out[...] = jnp.broadcast_to(gated[None], out.shape)


def output_kernel(gated, w_output, keep, send):
    heads = gated.shape[0]
    lhs = jnp.concatenate([gated[h] for h in range(heads)], 1)
    part = jnp.dot(lhs, w_output[...], preferred_element_type=F32)
    t = lax.axis_index("tp")
    half = keep.shape[1]
    low, high = part[:, :half], part[:, half:]
    keep[...] = jnp.where(t == 0, low, high).astype(BF)
    send[...] = jnp.where(t == 0, high, low).astype(BF)


def residual_kernel(tokens, keep, got, own, out):
    branch = keep[...].astype(F32) + got[...].astype(F32)
    residual = (tokens[...].astype(F32) + branch).astype(BF)
    own[...] = residual
    out[...] = jnp.broadcast_to(residual[None], out.shape)


def mixer_kernel(residual, mlp_gain, w_up, w_down, out):
    blocks, rows, own = residual.shape
    width = blocks * own
    first = jnp.zeros((rows, own), F32)
    second = jnp.zeros((rows, own), F32)
    scaled = []
    for i in range(blocks):
        wide = residual[i].astype(F32)
        first = first + wide
        second = second + wide * wide
        row = mlp_gain[:, i * own : (i + 1) * own]
        scaled.append((wide * row.astype(F32)).astype(BF))
    scaled = jnp.concatenate(scaled, 1)
    lhs = jnp.concatenate([scaled, jnp.broadcast_to(mlp_gain[...], scaled.shape)], 0)
    up = jnp.dot(lhs, w_up[...], preferred_element_type=F32)
    average = jnp.sum(first, 1, keepdims=True) / width
    inverse = lax.rsqrt(jnp.sum(second, 1, keepdims=True) / width - average * average + EPS)
    hidden = inverse * (up[:rows] - average * up[rows : rows + 1])
    hidden = jnp.square(jnp.maximum(hidden, 0.0)).astype(BF)
    down = jnp.dot(hidden, w_down[...], preferred_element_type=F32)
    for i in range(blocks):
        out[i] = down[:, i * own : (i + 1) * own].astype(BF)


def final_kernel(pieces, own, out):
    total = jnp.sum(pieces[...].astype(F32), 0)
    out[...] = (own[...].astype(F32) + total).astype(BF)


VMEM = pl.BlockSpec(memory_space=pltpu.VMEM)
SMEM = pl.BlockSpec(memory_space=pltpu.SMEM)
ANY = pl.BlockSpec(memory_space=pl.ANY)


def call(kernel, name, outs, in_specs, flops=0, bytes_accessed=0, scratch=(), limit=None):
    return pl.pallas_call(
        kernel,
        name=name,
        out_shape=outs,
        in_specs=in_specs,
        out_specs=jax.tree.map(lambda _: VMEM, outs),
        scratch_shapes=list(scratch),
        cost_estimate=pl.CostEstimate(
            flops=flops, bytes_accessed=bytes_accessed, transcendentals=0
        ),
        compiler_params=pltpu.CompilerParams(vmem_limit_bytes=limit),
    )


def make_kernels_on_device(kv, tp):
    def on_device(
        tokens,
        lengths,
        attn_gain,
        w_query,
        w_key,
        w_value,
        w_gate,
        decay_rate,
        key_cache,
        value_cache,
        head_gain,
        w_output,
        mlp_gain,
        w_up,
        w_down,
    ):
        S, own = tokens.shape
        H = decay_rate.shape[0]
        span = key_cache.shape[1]
        width = own * kv * tp
        qc, vc = H * HEAD_KEY, H * HEAD_VALUE
        swap = [(0, 1), (1, 0)]
        mib = 1 << 20
        sds = jax.ShapeDtypeStruct

        other = lax.ppermute(tokens, "tp", swap)
        gain = attn_gain[None, :]
        columns = qc + 2 * LANES
        message_types = (sds((S, columns), F32), sds((S, columns), BF))
        state, message = call(
            query_kernel, "query", message_types, [VMEM] * 4, limit=4 * mib
        )(tokens, other, gain, w_query)

        def exchange(message, stride):
            return [
                lax.ppermute(message, "kv", [(i, i ^ (j * stride)) for i in range(kv)])
                for j in range(1, 4)
            ]

        k_part, v_part, g_part, turn = call(
            other_kernel,
            "other",
            (
                sds((S + 8, qc), F32),
                sds((S + 8, vc), F32),
                sds((S + 8, vc), F32),
                sds((2, S, LANES), F32),
            ),
            [SMEM] + [VMEM] * 6,
            flops=10**9,
            bytes_accessed=4 * mib,
            limit=8 * mib,
        )(lengths, tokens, other, gain, w_key, w_value, w_gate)

        got = exchange(message, 1)
        stride = 4
        while stride < kv:
            state, message = call(
                middle_kernel, "middle", message_types, [VMEM] * 4, limit=2 * mib
            )(state, *got)
            got = exchange(message, stride)
            stride *= 4

        pieces = call(
            functools.partial(attend_kernel, width),
            "attend",
            sds((H, S, 4 * LANES), BF),
            [SMEM] * 2 + [VMEM] * 8 + [ANY] * 2,
            scratch=[
                pltpu.VMEM(key_cache.shape, BF),
                pltpu.VMEM(value_cache.shape, BF),
                pltpu.VMEM((S, qc), F32),
                pltpu.VMEM((S, vc), F32),
                pltpu.SemaphoreType.DMA((S,)),
                pltpu.SemaphoreType.DMA((S,)),
            ],
            limit=20 * mib,
        )(lengths, decay_rate, state, *got, k_part, v_part, g_part, turn, key_cache, value_cache)

        pieces = lax.all_to_all(pieces, "kv", 0, 0, tiled=True)
        spread = call(gate_kernel, "gate", sds((kv, S, LANES), BF), [VMEM] * 2, limit=2 * mib)(
            pieces, head_gain.reshape(H, HEAD_VALUE)
        )
        gated = lax.all_to_all(spread, "kv", 0, 0, tiled=True)
        keep, send = call(
            output_kernel, "output", (sds((S, own), BF),) * 2, [VMEM] * 2, limit=4 * mib
        )(gated, w_output)
        got = lax.ppermute(send, "tp", swap)
        residual, spread = call(
            residual_kernel,
            "residual",
            (sds((S, own), BF), sds((kv * tp, S, own), BF)),
            [VMEM] * 3,
            limit=2 * mib,
        )(tokens, keep, got)
        spread = lax.all_to_all(spread, ("kv", "tp"), 0, 0, tiled=True)
        down = call(
            mixer_kernel, "mixer", sds((kv * tp, S, own), BF), [VMEM] * 4, limit=16 * mib
        )(spread, mlp_gain[None, :], w_up, w_down)
        down = lax.all_to_all(down, ("kv", "tp"), 0, 0, tiled=True)
        return call(final_kernel, "final", sds((S, own), BF), [VMEM] * 2, limit=2 * mib)(
            down, residual
        )

    return on_device


def solution(mesh):
    in_specs = (
        P(None, ("kv", "tp")),
        P(),
        P("kv"),
        P("kv", "tp"),
        P("kv", "tp"),
        P("kv", "tp"),
        P("kv", "tp"),
        P("tp"),
        P(None, "kv", "tp"),
        P(None, "kv", "tp"),
        P("tp"),
        P("tp", "kv"),
        P(),
        P(None, ("kv", "tp")),
        P(("kv", "tp"), None),
    )
    kv, tp = mesh.shape["kv"], mesh.shape["tp"]

    def on_device(*arrays):
        fits = tp == 2 and arrays[7].shape[0] == kv and arrays[0].shape[1] == LANES
        make = make_kernels_on_device if fits else make_on_device
        return make(kv, tp)(*arrays)

    return jax.shard_map(
        on_device,
        mesh=mesh,
        in_specs=in_specs,
        out_specs=P(None, ("kv", "tp")),
        check_vma=False,
    )
```

```python
import functools
import math

import jax
import jax.numpy as jnp
from jax import lax
from jax.experimental import pallas as pl
from jax.experimental.pallas import tpu as pltpu
from jax.sharding import PartitionSpec as P

HEAD_KEY = 64
HEAD_VALUE = 128
EPS = 1e-05
THETA = 10000.0
LANES = 128

BF = jnp.bfloat16
F32 = jnp.float32


def split_two(x):
    high = x.astype(BF)
    return high, (x - high.astype(F32)).astype(BF)


def rotate(flat, cosine, sine):
    rows = flat.shape[0]
    grouped = flat.reshape(rows, -1, HEAD_KEY)
    half = HEAD_KEY // 2
    a, b = grouped[..., :half], grouped[..., half:]
    c, s = cosine[:, None, :], sine[:, None, :]
    return jnp.concatenate([a * c - b * s, b * c + a * s], -1).reshape(rows, -1)


def broadcast_gather(x, axes, size):
    spread = jnp.broadcast_to(x[None], (size,) + x.shape)
    return lax.all_to_all(spread, axes, 0, 0, tiled=True)


def make_on_device(kv, tp):
    def on_device(
        tokens,
        lengths,
        attn_gain,
        w_query,
        w_key,
        w_value,
        w_gate,
        decay_rate,
        key_cache,
        value_cache,
        head_gain,
        w_output,
        mlp_gain,
        w_up,
        w_down,
    ):
        S = tokens.shape[0]
        H = decay_rate.shape[0]
        span = key_cache.shape[1]
        width = tokens.shape[1] * kv * tp
        own = tokens.shape[1]
        kvi = lax.axis_index("kv")
        tpi = lax.axis_index("tp")
        groups = kv // H
        rows = S // groups

        if tp == 2:
            other = lax.ppermute(tokens, "tp", [(0, 1), (1, 0)])
            low = jnp.where(tpi == 0, tokens, other)
            high = jnp.where(tpi == 0, other, tokens)
            block = jnp.concatenate([low, high], 1)
        else:
            block = lax.all_gather(tokens, "tp", axis=1, tiled=True)
        wide = block.astype(F32)
        scaled = (wide * attn_gain.astype(F32)).astype(BF)
        lhs = jnp.concatenate([scaled, attn_gain[None, :]], 0)
        part_q = jnp.dot(lhs, w_query, preferred_element_type=F32)
        moments = jnp.stack([jnp.sum(wide, -1), jnp.sum(wide * wide, -1)], -1)

        small = jnp.concatenate([part_q[S], moments.reshape(-1)])
        q_sum = part_q[:S]
        stride = 1
        while stride < kv:
            count = 4 if kv % (stride * 4) == 0 else 2
            high, low = split_two(small)
            tail = jnp.concatenate([high, low])
            pad = -tail.shape[0] % S
            tail = jnp.pad(tail, (0, pad)).reshape(S, -1)
            message = jnp.concatenate([q_sum.astype(BF), tail], 1)
            for j in range(1, count):
                got = lax.ppermute(message, "kv", [(i, i ^ (j * stride)) for i in range(kv)])
                got = got.astype(F32)
                q_sum = q_sum + got[:, : q_sum.shape[1]]
                flat = got[:, q_sum.shape[1] :].reshape(-1)
                n = small.shape[0]
                small = small + flat[:n] + flat[n : 2 * n]
            stride *= count
        csum_q = small[: q_sum.shape[1]]
        moments = small[q_sum.shape[1] :].reshape(S, 2)
        average = moments[:, 0] / width
        inverse = lax.rsqrt(moments[:, 1] / width - average * average + EPS)

        half = HEAD_KEY // 2
        turn = jnp.power(THETA, -jnp.arange(half, dtype=F32) / half)
        angles = lengths.astype(F32)[:, None] * turn[None, :]
        q_plain = inverse[:, None] * (q_sum - average[:, None] * csum_q[None, :])
        queries = rotate(q_plain, jnp.cos(angles), jnp.sin(angles)).astype(BF)
        queries = queries.reshape(S, H, HEAD_KEY)

        def partial(w):
            p = jnp.dot(lhs, w, preferred_element_type=F32)
            return inverse[:, None] * (p[:S] - average[:, None] * p[S:])

        part_k = partial(w_key).reshape(S, H, HEAD_KEY)
        part_v = partial(w_value).reshape(S, H, HEAD_VALUE)
        part_g = partial(w_gate).reshape(S, H, HEAD_VALUE)
        part_score = jnp.sum(q_plain.reshape(S, H, HEAD_KEY) * part_k, -1) * HEAD_KEY ** (-0.5)

        keys = key_cache.reshape(S, span, H, HEAD_KEY)
        values = value_cache.reshape(S, span, H, HEAD_VALUE)
        scores = jnp.einsum("bhd,bjhd->bhj", queries, keys, preferred_element_type=F32)
        places = kvi * span + jnp.arange(span, dtype=jnp.int32)
        distance = jnp.maximum(lengths[:, None] - places[None, :], 0).astype(F32)
        live = (places[None, :] < lengths[:, None])[:, None, :]
        decays = jnp.where(
            live, jnp.exp(-decay_rate[None, :, None] * distance[:, None, :]), 0.0
        )
        coefficients = (scores * HEAD_KEY ** (-0.5) * decays).astype(BF)
        part_c = jnp.einsum("bhj,bjhe->bhe", coefficients, values, preferred_element_type=F32)

        high, low = split_two(part_score)
        pieces = jnp.concatenate(
            [
                part_c.astype(BF),
                part_v.astype(BF),
                part_g.astype(BF),
                high[..., None],
                low[..., None],
                jnp.zeros((S, H, 126), BF),
            ],
            -1,
        )
        pieces = pieces.transpose(1, 0, 2).reshape(kv, rows, 4 * HEAD_VALUE)
        mine = jnp.sum(
            lax.all_to_all(pieces, "kv", 0, 0, tiled=True).astype(F32), 0
        )
        cached, value, gate = (
            mine[:, i * HEAD_VALUE : (i + 1) * HEAD_VALUE] for i in range(3)
        )
        score = mine[:, 3 * HEAD_VALUE] + mine[:, 3 * HEAD_VALUE + 1]
        retained = cached + score[:, None] * value
        centered = retained - jnp.mean(retained, -1, keepdims=True)
        gain = lax.dynamic_slice(head_gain, ((kvi // groups) * HEAD_VALUE,), (HEAD_VALUE,))
        normed = (
            centered
            * lax.rsqrt(jnp.mean(centered * centered, -1, keepdims=True) + EPS)
            * gain.astype(F32)
        )
        gated = (jax.nn.silu(gate) * normed).astype(BF)
        gathered = broadcast_gather(gated, "kv", kv).reshape(H, S, HEAD_VALUE)
        gathered = gathered.transpose(1, 0, 2).reshape(S, H * HEAD_VALUE)
        part_b = jnp.dot(gathered, w_output, preferred_element_type=F32).astype(BF)
        part_b = part_b.reshape(S, tp, own).transpose(1, 0, 2)
        if tp == 2:
            keep = jnp.where(tpi == 0, part_b[0], part_b[1])
            send = jnp.where(tpi == 0, part_b[1], part_b[0])
            got = lax.ppermute(send, "tp", [(0, 1), (1, 0)])
            branch = keep.astype(F32) + got.astype(F32)
        else:
            branch = jnp.sum(
                lax.all_to_all(part_b, "tp", 0, 0, tiled=True).astype(F32), 0
            )
        own_residual = (tokens.astype(F32) + branch).astype(BF)

        residual = broadcast_gather(own_residual, ("kv", "tp"), kv * tp)
        residual = residual.transpose(1, 0, 2).reshape(S, width)
        wide = residual.astype(F32)
        scaled = (wide * mlp_gain.astype(F32)).astype(BF)
        lhs = jnp.concatenate([scaled, mlp_gain[None, :]], 0)
        up = jnp.dot(lhs, w_up, preferred_element_type=F32)
        average = jnp.sum(wide, -1) / width
        inverse = lax.rsqrt(jnp.sum(wide * wide, -1) / width - average * average + EPS)
        hidden = inverse[:, None] * (up[:S] - average[:, None] * up[S:])
        hidden = jnp.square(jax.nn.relu(hidden)).astype(BF)
        down = jnp.dot(hidden, w_down, preferred_element_type=F32).astype(BF)
        down = down.reshape(S, kv * tp, own).transpose(1, 0, 2)
        mixer = jnp.sum(
            lax.all_to_all(down, ("kv", "tp"), 0, 0, tiled=True).astype(F32), 0
        )
        return (own_residual.astype(F32) + mixer).astype(BF)

    return on_device


def lane_ids(rows):
    return lax.broadcasted_iota(jnp.int32, (rows, LANES), 1)


def row_ids(rows, columns=LANES):
    return lax.broadcasted_iota(jnp.int32, (rows, columns), 0)


def column_of(scalars, rows, dtype):
    ids = row_ids(rows)
    out = jnp.zeros((rows, LANES), dtype)
    for i in range(rows):
        out = jnp.where(ids == i, scalars[i].astype(dtype), out)
    return out


def gain_row(gain, rows):
    wide = gain[...].astype(F32)
    return jnp.concatenate(
        [jnp.broadcast_to(wide[i : i + 1], (rows, LANES)) for i in range(wide.shape[0])], 1
    )


def projection_rows(first, second, gain):
    t = lax.axis_index("tp")
    a, b = first[...].astype(F32), second[...].astype(F32)
    wide = jnp.concatenate([jnp.where(t == 0, a, b), jnp.where(t == 0, b, a)], 1)
    row = gain_row(gain, wide.shape[0])
    return jnp.concatenate([(wide * row).astype(BF), row.astype(BF)], 0), wide


def pack(q, csum, moments, message):
    columns = q.shape[1]
    half = csum.shape[0]
    message[:, :columns] = q.astype(BF)
    high = csum.astype(BF)
    low = (csum - high.astype(F32)).astype(BF)
    message[:, columns : columns + LANES] = jnp.concatenate([high, low], 0)
    high = moments.astype(BF).astype(F32)
    low = moments - high
    lanes = lane_ids(q.shape[0])
    both = jnp.where(lanes < 2, high, jnp.where(lanes < 4, pltpu.roll(low, 2, 1), 0.0))
    message[:, columns + LANES :] = both.astype(BF)
    assert 2 * half == q.shape[0]


def unpack_sum(state, messages):
    rows, total = state.shape
    columns = total - 2 * LANES
    half = rows // 2
    q = state[:, :columns]
    csum = state[:half, columns : columns + LANES]
    moments = state[:, columns + LANES :]
    for m in messages:
        q = q + m[:, :columns].astype(F32)
        c = m[:, columns : columns + LANES].astype(F32)
        csum = csum + c[:half] + c[half:]
        v = m[:, columns + LANES :].astype(F32)
        moments = moments + v + pltpu.roll(v, LANES - 2, 1)
    return q, csum, jnp.where(lane_ids(rows) < 2, moments, 0.0)


def store_state(q, csum, moments, state):
    columns = q.shape[1]
    state[:, :columns] = q
    state[:, columns : columns + LANES] = jnp.concatenate([csum, jnp.zeros_like(csum)], 0)
    state[:, columns + LANES :] = moments


def first_load_kernel(
    w_query,
    tokens,
    gain,
    lengths,
    decay,
    w_out,
    tokens_out,
    gain_out,
    length_out,
    rate_out,
    length_scalars,
    decay_scalars,
    sems,
):
    pairs = (
        (lengths, length_scalars),
        (decay, decay_scalars),
        (tokens, tokens_out),
        (gain, gain_out),
        (w_query, w_out),
    )
    copies = [pltpu.make_async_copy(a, b, sems.at[i]) for i, (a, b) in enumerate(pairs)]
    for copy in copies:
        copy.start()
    copies[0].wait()
    length_out[...] = column_of(length_scalars, length_out.shape[0], jnp.int32)
    copies[1].wait()
    rate_out[...] = column_of(decay_scalars, rate_out.shape[0], F32)
    for copy in copies[2:]:
        copy.wait()


def cache_load_kernel(after, keys, values, keys_out, values_out, sems):
    copies = (
        pltpu.make_async_copy(keys, keys_out, sems.at[0]),
        pltpu.make_async_copy(values, values_out, sems.at[1]),
    )
    for copy in copies:
        copy.start()
    for copy in copies:
        copy.wait()


def query_kernel(first, second, gain, w_query, state, message):
    lhs, wide = projection_rows(first, second, gain)
    rows = wide.shape[0]
    product = jnp.dot(lhs, w_query[...], preferred_element_type=F32)
    half = rows // 2
    ids = row_ids(half)
    csum = jnp.zeros((half, LANES), F32)
    for i in range(product.shape[1] // LANES):
        csum = jnp.where(
            ids == i, product[rows : rows + half, i * LANES : (i + 1) * LANES], csum
        )
    lanes = lane_ids(rows)
    first_sum = jnp.sum(wide, 1, keepdims=True)
    second_sum = jnp.sum(wide * wide, 1, keepdims=True)
    moments = jnp.where(lanes == 0, first_sum, jnp.where(lanes == 1, second_sum, 0.0))
    store_state(product[:rows], csum, moments, state)
    pack(product[:rows], csum, moments, message)


def middle_kernel(old, m1, m2, m3, state, message):
    q, csum, moments = unpack_sum(old, (m1, m2, m3))
    store_state(q, csum, moments, state)
    pack(q, csum, moments, message)


def other_kernel(
    after,
    lengths,
    rates,
    first,
    second,
    gain,
    w_key,
    w_value,
    w_gate,
    k_out,
    v_out,
    g_out,
    turn,
    weights,
    key_buffer,
    value_buffer,
    gate_buffer,
    sems,
):
    sources = (w_key, w_value, w_gate)
    buffers = (key_buffer, value_buffer, gate_buffer)
    copies = [
        pltpu.make_async_copy(source, buffer, sems.at[i])
        for i, (source, buffer) in enumerate(zip(sources, buffers))
    ]
    for copy in copies:
        copy.start()
    lhs, wide = projection_rows(first, second, gain)
    rows = wide.shape[0]
    half = HEAD_KEY // 2
    entry = (lane_ids(rows) % half).astype(F32)
    inverse = jnp.exp(entry * (-math.log(THETA) / half))
    angle = lengths[...].astype(F32) * inverse
    turn[0] = jnp.cos(angle)
    turn[1] = jnp.sin(angle)
    heads = rates.shape[0]
    places = lax.axis_index("kv") * LANES + lane_ids(heads)
    rate = rates[...]
    for s in range(rows):
        distance = jnp.broadcast_to(lengths[s : s + 1, :], (heads, LANES)) - places
        weight = jnp.exp(-rate * jnp.maximum(distance, 0).astype(F32)) * HEAD_KEY ** (-0.5)
        weights[s] = jnp.where(distance > 0, weight, 0.0)
    for copy, buffer, out in zip(copies, buffers, (k_out, v_out, g_out)):
        copy.wait()
        product = jnp.dot(lhs, buffer[...], preferred_element_type=F32)
        out[...] = product[: rows + 8]


def attend_kernel(
    width,
    old,
    m1,
    m2,
    m3,
    k_part,
    v_part,
    g_part,
    turn,
    weights,
    keys,
    values,
    out,
    query_rows,
    cached,
):
    rows, span, key_columns = keys.shape
    heads = key_columns // HEAD_KEY
    q, csum, moments = unpack_sum(old, (m1, m2, m3))
    average = moments[:, 0:1] / width
    inverse = lax.rsqrt(moments[:, 1:2] / width - average * average + EPS)
    lanes = lane_ids(rows)
    in_first = lanes % HEAD_KEY < HEAD_KEY // 2
    low_head = lanes < HEAD_KEY
    top = rows // 2
    cosine, sine = turn[0], turn[1]
    for i in range(key_columns // LANES):
        cut = slice(i * LANES, (i + 1) * LANES)
        plain = inverse * (q[:, cut] - average * csum[i : i + 1])
        partner = jnp.where(
            in_first,
            -pltpu.roll(plain, LANES - HEAD_KEY // 2, 1),
            pltpu.roll(plain, HEAD_KEY // 2, 1),
        )
        turned = plain * cosine + partner * sine
        query_rows[:, cut] = turned.astype(BF).astype(F32)
        part = inverse * (k_part[:rows, cut] - average * k_part[rows : rows + 1, cut])
        both = plain * part * HEAD_KEY ** (-0.5)
        for j in range(2):
            picked = jnp.where(low_head == (j == 0), both, 0.0)
            score = jnp.sum(picked, 1, keepdims=True)
            high = score.astype(BF).astype(F32)
            low = score - high
            folded = jnp.where(
                lanes[:top] < HEAD_KEY,
                jnp.where(in_first[:top], high[:top], low[:top]),
                jnp.where(in_first[:top], high[top:], low[top:]),
            )
            out[2 * i + j, 3 * rows :, :] = folded.astype(BF)
    for h in range(heads):
        cut = slice(h * LANES, (h + 1) * LANES)
        for place, part in ((1, v_part), (2, g_part)):
            normed = inverse * (part[:rows, cut] - average * part[rows : rows + 1, cut])
            out[h, place * rows : (place + 1) * rows, :] = normed.astype(BF)

    head_of_key = lax.broadcasted_iota(jnp.int32, (heads, key_columns), 1) // HEAD_KEY
    own_key = head_of_key == row_ids(heads, key_columns)
    value_columns = heads * HEAD_VALUE
    head_of_value = lax.broadcasted_iota(jnp.int32, (heads, value_columns), 1) // HEAD_VALUE
    own_value = head_of_value == row_ids(heads, value_columns)
    for s in range(rows):
        spread = jnp.broadcast_to(query_rows[s : s + 1, :], (heads, key_columns))
        query = jnp.where(own_key, spread, 0.0).astype(BF)
        scores = lax.dot_general(
            query, keys[s], (((1,), (1,)), ((), ())), preferred_element_type=F32
        )
        coefficients = (scores * weights[s]).astype(BF)
        product = jnp.dot(coefficients, values[s], preferred_element_type=F32)
        cached[s : s + 1, :] = jnp.sum(
            jnp.where(own_value, product, 0.0), 0, keepdims=True
        )
    for h in range(heads):
        out[h, :rows, :] = cached[:, h * LANES : (h + 1) * LANES].astype(BF)


def gate_kernel(pieces, head_gain, out):
    rows = out.shape[1]
    total = jnp.sum(pieces[...].astype(F32), 0)
    cached, value, gate = (total[i * rows : (i + 1) * rows] for i in range(3))
    folded = total[3 * rows :]
    half = HEAD_KEY // 2
    score = jnp.concatenate(
        [folded[:, i : i + 1] + folded[:, i + half : i + half + 1] for i in (0, HEAD_KEY)], 0
    )
    retained = cached + score * value
    centered = retained - jnp.mean(retained, -1, keepdims=True)
    spread = lax.rsqrt(jnp.mean(centered * centered, -1, keepdims=True) + EPS)
    gains = head_gain[...].astype(F32)
    mine = row_ids(gains.shape[0]) == lax.axis_index("kv")
    gain = jnp.sum(jnp.where(mine, gains, 0.0), 0, keepdims=True)
    normed = centered * spread * gain
    gated = (gate * jax.nn.sigmoid(gate) * normed).astype(BF)
    out[...] = jnp.broadcast_to(gated[None], out.shape)


def output_kernel(gated, w_output, keep, send):
    heads = gated.shape[0]
    lhs = jnp.concatenate([gated[h] for h in range(heads)], 1)
    part = jnp.dot(lhs, w_output[...], preferred_element_type=F32)
    t = lax.axis_index("tp")
    half = keep.shape[1]
    low, high = part[:, :half], part[:, half:]
    keep[...] = jnp.where(t == 0, low, high).astype(BF)
    send[...] = jnp.where(t == 0, high, low).astype(BF)


def residual_kernel(tokens, keep, got, own, out):
    branch = keep[...].astype(F32) + got[...].astype(F32)
    residual = (tokens[...].astype(F32) + branch).astype(BF)
    own[...] = residual
    out[...] = jnp.broadcast_to(residual[None], out.shape)


def mixer_kernel(residual, mlp_gain, w_up, w_down, out):
    blocks, rows, own = residual.shape
    width = blocks * own
    first = jnp.zeros((rows, own), F32)
    second = jnp.zeros((rows, own), F32)
    scaled, gain = [], []
    gains = mlp_gain[...].astype(F32)
    for i in range(blocks):
        wide = residual[i].astype(F32)
        first = first + wide
        second = second + wide * wide
        row = gains[i : i + 1]
        scaled.append((wide * row).astype(BF))
        gain.append(jnp.broadcast_to(row, wide.shape).astype(BF))
    lhs = jnp.concatenate([jnp.concatenate(scaled, 1), jnp.concatenate(gain, 1)], 0)
    up = jnp.dot(lhs, w_up[...], preferred_element_type=F32)
    average = jnp.sum(first, 1, keepdims=True) / width
    inverse = lax.rsqrt(jnp.sum(second, 1, keepdims=True) / width - average * average + EPS)
    hidden = inverse * (up[:rows] - average * up[rows : rows + 1])
    hidden = jnp.square(jnp.maximum(hidden, 0.0)).astype(BF)
    down = jnp.dot(hidden, w_down[...], preferred_element_type=F32)
    for i in range(blocks):
        out[i] = down[:, i * own : (i + 1) * own].astype(BF)


def final_kernel(pieces, own, out):
    total = jnp.sum(pieces[...].astype(F32), 0)
    out[...] = (own[...].astype(F32) + total).astype(BF)


VMEM = pl.BlockSpec(memory_space=pltpu.VMEM)
HBM = pl.BlockSpec(memory_space=pltpu.HBM)
ANY = pl.BlockSpec(memory_space=pl.ANY)


def in_hbm(*arrays):
    return [pltpu.with_memory_space_constraint(x, pltpu.HBM) for x in arrays]


def call(kernel, name, outs, in_specs, flops=0, bytes_accessed=0, scratch=(), limit=None):
    return pl.pallas_call(
        kernel,
        name=name,
        out_shape=outs,
        in_specs=in_specs,
        out_specs=jax.tree.map(lambda _: VMEM, outs),
        scratch_shapes=list(scratch),
        cost_estimate=pl.CostEstimate(
            flops=flops, bytes_accessed=bytes_accessed, transcendentals=0
        ),
        compiler_params=pltpu.CompilerParams(vmem_limit_bytes=limit),
    )


def make_kernels_on_device(kv, tp):
    def on_device(
        tokens,
        lengths,
        attn_gain,
        w_query,
        w_key,
        w_value,
        w_gate,
        decay_rate,
        key_cache,
        value_cache,
        head_gain,
        w_output,
        mlp_gain,
        w_up,
        w_down,
    ):
        S, own = tokens.shape
        H = decay_rate.shape[0]
        span = key_cache.shape[1]
        width = own * kv * tp
        qc, vc = H * HEAD_KEY, H * HEAD_VALUE
        swap = [(0, 1), (1, 0)]
        mib = 1 << 20
        sds = jax.ShapeDtypeStruct

        other = lax.ppermute(tokens, "tp", swap)
        gain = attn_gain.reshape(-1, LANES)
        w_query, tokens, gain, length_rows, rates = call(
            first_load_kernel,
            "first_load",
            (
                sds(w_query.shape, BF),
                sds(tokens.shape, BF),
                sds(gain.shape, BF),
                sds((S, LANES), jnp.int32),
                sds((H, LANES), F32),
            ),
            [HBM] * 5,
            flops=10**9,
            scratch=[
                pltpu.SMEM((S,), jnp.int32),
                pltpu.SMEM((H,), F32),
                pltpu.SemaphoreType.DMA((5,)),
            ],
            limit=2 * mib,
        )(*in_hbm(w_query, tokens, gain, lengths, decay_rate))
        columns = qc + 2 * LANES
        message_types = (sds((S, columns), F32), sds((S, columns), BF))
        state, message = call(
            query_kernel, "query", message_types, [VMEM] * 4, limit=2 * mib
        )(tokens, other, gain, w_query)

        def exchange(message, stride):
            return [
                lax.ppermute(message, "kv", [(i, i ^ (j * stride)) for i in range(kv)])
                for j in range(1, 4)
            ]

        got = exchange(message, 1)
        k_part, v_part, g_part, turn, weights = call(
            other_kernel,
            "other",
            (
                sds((S + 8, qc), F32),
                sds((S + 8, vc), F32),
                sds((S + 8, vc), F32),
                sds((2, S, LANES), F32),
                sds((S, H, LANES), F32),
            ),
            [ANY] + [VMEM] * 5 + [HBM] * 3,
            flops=10**9,
            scratch=[pltpu.VMEM(w.shape, BF) for w in (w_key, w_value, w_gate)]
            + [pltpu.SemaphoreType.DMA((3,))],
            limit=6 * mib,
        )(message, length_rows, rates, tokens, other, gain, *in_hbm(w_key, w_value, w_gate))

        stride = 4
        while stride < kv:
            state, message = call(
                middle_kernel, "middle", message_types, [VMEM] * 4, limit=2 * mib
            )(state, *got)
            got = exchange(message, stride)
            stride *= 4
        keys, values = call(
            cache_load_kernel,
            "cache_load",
            (sds(key_cache.shape, BF), sds(value_cache.shape, BF)),
            [ANY] + [HBM] * 2,
            flops=10**9,
            scratch=[pltpu.SemaphoreType.DMA((2,))],
            limit=2 * mib,
        )(message, *in_hbm(key_cache, value_cache))

        pieces = call(
            functools.partial(attend_kernel, width),
            "attend",
            sds((H, 3 * S + S // 2, LANES), BF),
            [VMEM] * 11,
            scratch=[pltpu.VMEM((S, qc), F32), pltpu.VMEM((S, vc), F32)],
            limit=4 * mib,
        )(state, *got, k_part, v_part, g_part, turn, weights, keys, values)

        pieces = lax.all_to_all(pieces, "kv", 0, 0, tiled=True)
        spread = call(gate_kernel, "gate", sds((kv, S, LANES), BF), [VMEM] * 2, limit=2 * mib)(
            pieces, head_gain.reshape(H, HEAD_VALUE)
        )
        gated = lax.all_to_all(spread, "kv", 0, 0, tiled=True)
        keep, send = call(
            output_kernel, "output", (sds((S, own), BF),) * 2, [VMEM] * 2, limit=4 * mib
        )(gated, w_output)
        got = lax.ppermute(send, "tp", swap)
        residual, spread = call(
            residual_kernel,
            "residual",
            (sds((S, own), BF), sds((kv * tp, S, own), BF)),
            [VMEM] * 3,
            limit=2 * mib,
        )(tokens, keep, got)
        spread = lax.all_to_all(spread, ("kv", "tp"), 0, 0, tiled=True)
        down = call(
            mixer_kernel, "mixer", sds((kv * tp, S, own), BF), [VMEM] * 4, limit=16 * mib
        )(spread, mlp_gain.reshape(-1, LANES), w_up, w_down)
        down = lax.all_to_all(down, ("kv", "tp"), 0, 0, tiled=True)
        return call(final_kernel, "final", sds((S, own), BF), [VMEM] * 2, limit=2 * mib)(
            down, residual
        )

    return on_device


def solution(mesh):
    in_specs = (
        P(None, ("kv", "tp")),
        P(),
        P("kv"),
        P("kv", "tp"),
        P("kv", "tp"),
        P("kv", "tp"),
        P("kv", "tp"),
        P("tp"),
        P(None, "kv", "tp"),
        P(None, "kv", "tp"),
        P("tp"),
        P("tp", "kv"),
        P(),
        P(None, ("kv", "tp")),
        P(("kv", "tp"), None),
    )
    kv, tp = mesh.shape["kv"], mesh.shape["tp"]

    def on_device(*arrays):
        fits = tp == 2 and arrays[7].shape[0] == kv
        fits = fits and arrays[0].shape[1] == LANES == arrays[8].shape[1]
        make = make_kernels_on_device if fits else make_on_device
        return make(kv, tp)(*arrays)

    return jax.shard_map(
        on_device,
        mesh=mesh,
        in_specs=in_specs,
        out_specs=P(None, ("kv", "tp")),
        check_vma=False,
    )
```

```python
import functools
import math

import jax
import jax.numpy as jnp
from jax import lax
from jax.experimental import pallas as pl
from jax.experimental.pallas import tpu as pltpu
from jax.sharding import PartitionSpec as P


HEAD_KEY = 64
HEAD_VALUE = 128
EPS = 1e-05
THETA = 10000.0
LANES = 128

BF = jnp.bfloat16
F32 = jnp.float32


def split_two(x):
    high = x.astype(BF)
    return high, (x - high.astype(F32)).astype(BF)


def rotate(flat, cosine, sine):
    rows = flat.shape[0]
    grouped = flat.reshape(rows, -1, HEAD_KEY)
    half = HEAD_KEY // 2
    a, b = grouped[..., :half], grouped[..., half:]
    c, s = cosine[:, None, :], sine[:, None, :]
    return jnp.concatenate([a * c - b * s, b * c + a * s], -1).reshape(rows, -1)


def broadcast_gather(x, axes, size):
    spread = jnp.broadcast_to(x[None], (size,) + x.shape)
    return lax.all_to_all(spread, axes, 0, 0, tiled=True)


def make_on_device(kv, tp):
    def on_device(
        tokens,
        lengths,
        attn_gain,
        w_query,
        w_key,
        w_value,
        w_gate,
        decay_rate,
        key_cache,
        value_cache,
        head_gain,
        w_output,
        mlp_gain,
        w_up,
        w_down,
    ):
        S = tokens.shape[0]
        H = decay_rate.shape[0]
        span = key_cache.shape[1]
        width = tokens.shape[1] * kv * tp
        own = tokens.shape[1]
        kvi = lax.axis_index("kv")
        tpi = lax.axis_index("tp")
        groups = kv // H
        rows = S // groups

        if tp == 2:
            other = lax.ppermute(tokens, "tp", [(0, 1), (1, 0)])
            low = jnp.where(tpi == 0, tokens, other)
            high = jnp.where(tpi == 0, other, tokens)
            block = jnp.concatenate([low, high], 1)
        else:
            block = lax.all_gather(tokens, "tp", axis=1, tiled=True)
        wide = block.astype(F32)
        scaled = (wide * attn_gain.astype(F32)).astype(BF)
        lhs = jnp.concatenate([scaled, attn_gain[None, :]], 0)
        part_q = jnp.dot(lhs, w_query, preferred_element_type=F32)
        moments = jnp.stack([jnp.sum(wide, -1), jnp.sum(wide * wide, -1)], -1)

        small = jnp.concatenate([part_q[S], moments.reshape(-1)])
        q_sum = part_q[:S]
        stride = 1
        while stride < kv:
            count = 4 if kv % (stride * 4) == 0 else 2
            high, low = split_two(small)
            tail = jnp.concatenate([high, low])
            pad = -tail.shape[0] % S
            tail = jnp.pad(tail, (0, pad)).reshape(S, -1)
            message = jnp.concatenate([q_sum.astype(BF), tail], 1)
            for j in range(1, count):
                got = lax.ppermute(message, "kv", [(i, i ^ (j * stride)) for i in range(kv)])
                got = got.astype(F32)
                q_sum = q_sum + got[:, : q_sum.shape[1]]
                flat = got[:, q_sum.shape[1] :].reshape(-1)
                n = small.shape[0]
                small = small + flat[:n] + flat[n : 2 * n]
            stride *= count
        csum_q = small[: q_sum.shape[1]]
        moments = small[q_sum.shape[1] :].reshape(S, 2)
        average = moments[:, 0] / width
        inverse = lax.rsqrt(moments[:, 1] / width - average * average + EPS)

        half = HEAD_KEY // 2
        turn = jnp.power(THETA, -jnp.arange(half, dtype=F32) / half)
        angles = lengths.astype(F32)[:, None] * turn[None, :]
        q_plain = inverse[:, None] * (q_sum - average[:, None] * csum_q[None, :])
        queries = rotate(q_plain, jnp.cos(angles), jnp.sin(angles)).astype(BF)
        queries = queries.reshape(S, H, HEAD_KEY)

        def partial(w):
            p = jnp.dot(lhs, w, preferred_element_type=F32)
            return inverse[:, None] * (p[:S] - average[:, None] * p[S:])

        part_k = partial(w_key).reshape(S, H, HEAD_KEY)
        part_v = partial(w_value).reshape(S, H, HEAD_VALUE)
        part_g = partial(w_gate).reshape(S, H, HEAD_VALUE)
        part_score = jnp.sum(q_plain.reshape(S, H, HEAD_KEY) * part_k, -1) * HEAD_KEY ** (-0.5)

        keys = key_cache.reshape(S, span, H, HEAD_KEY)
        values = value_cache.reshape(S, span, H, HEAD_VALUE)
        scores = jnp.einsum("bhd,bjhd->bhj", queries, keys, preferred_element_type=F32)
        places = kvi * span + jnp.arange(span, dtype=jnp.int32)
        distance = jnp.maximum(lengths[:, None] - places[None, :], 0).astype(F32)
        live = (places[None, :] < lengths[:, None])[:, None, :]
        decays = jnp.where(
            live, jnp.exp(-decay_rate[None, :, None] * distance[:, None, :]), 0.0
        )
        coefficients = (scores * HEAD_KEY ** (-0.5) * decays).astype(BF)
        part_c = jnp.einsum("bhj,bjhe->bhe", coefficients, values, preferred_element_type=F32)

        high, low = split_two(part_score)
        pieces = jnp.concatenate(
            [
                part_c.astype(BF),
                part_v.astype(BF),
                part_g.astype(BF),
                high[..., None],
                low[..., None],
                jnp.zeros((S, H, 126), BF),
            ],
            -1,
        )
        pieces = pieces.transpose(1, 0, 2).reshape(kv, rows, 4 * HEAD_VALUE)
        mine = jnp.sum(
            lax.all_to_all(pieces, "kv", 0, 0, tiled=True).astype(F32), 0
        )
        cached, value, gate = (
            mine[:, i * HEAD_VALUE : (i + 1) * HEAD_VALUE] for i in range(3)
        )
        score = mine[:, 3 * HEAD_VALUE] + mine[:, 3 * HEAD_VALUE + 1]
        retained = cached + score[:, None] * value
        centered = retained - jnp.mean(retained, -1, keepdims=True)
        gain = lax.dynamic_slice(head_gain, ((kvi // groups) * HEAD_VALUE,), (HEAD_VALUE,))
        normed = (
            centered
            * lax.rsqrt(jnp.mean(centered * centered, -1, keepdims=True) + EPS)
            * gain.astype(F32)
        )
        gated = (jax.nn.silu(gate) * normed).astype(BF)
        gathered = broadcast_gather(gated, "kv", kv).reshape(H, S, HEAD_VALUE)
        gathered = gathered.transpose(1, 0, 2).reshape(S, H * HEAD_VALUE)
        part_b = jnp.dot(gathered, w_output, preferred_element_type=F32).astype(BF)
        part_b = part_b.reshape(S, tp, own).transpose(1, 0, 2)
        if tp == 2:
            keep = jnp.where(tpi == 0, part_b[0], part_b[1])
            send = jnp.where(tpi == 0, part_b[1], part_b[0])
            got = lax.ppermute(send, "tp", [(0, 1), (1, 0)])
            branch = keep.astype(F32) + got.astype(F32)
        else:
            branch = jnp.sum(
                lax.all_to_all(part_b, "tp", 0, 0, tiled=True).astype(F32), 0
            )
        own_residual = (tokens.astype(F32) + branch).astype(BF)

        residual = broadcast_gather(own_residual, ("kv", "tp"), kv * tp)
        residual = residual.transpose(1, 0, 2).reshape(S, width)
        wide = residual.astype(F32)
        scaled = (wide * mlp_gain.astype(F32)).astype(BF)
        lhs = jnp.concatenate([scaled, mlp_gain[None, :]], 0)
        up = jnp.dot(lhs, w_up, preferred_element_type=F32)
        average = jnp.sum(wide, -1) / width
        inverse = lax.rsqrt(jnp.sum(wide * wide, -1) / width - average * average + EPS)
        hidden = inverse[:, None] * (up[:S] - average[:, None] * up[S:])
        hidden = jnp.square(jax.nn.relu(hidden)).astype(BF)
        down = jnp.dot(hidden, w_down, preferred_element_type=F32).astype(BF)
        down = down.reshape(S, kv * tp, own).transpose(1, 0, 2)
        mixer = jnp.sum(
            lax.all_to_all(down, ("kv", "tp"), 0, 0, tiled=True).astype(F32), 0
        )
        return (own_residual.astype(F32) + mixer).astype(BF)

    return on_device


def lane_ids(rows):
    return lax.broadcasted_iota(jnp.int32, (rows, LANES), 1)


def row_ids(rows, columns=LANES):
    return lax.broadcasted_iota(jnp.int32, (rows, columns), 0)


def column_of(scalars, rows, dtype):
    ids = row_ids(rows)
    out = jnp.zeros((rows, LANES), dtype)
    for i in range(rows):
        out = jnp.where(ids == i, scalars[i].astype(dtype), out)
    return out


def gain_row(gain, rows):
    wide = gain[...].astype(F32)
    return jnp.concatenate(
        [jnp.broadcast_to(wide[i : i + 1], (rows, LANES)) for i in range(wide.shape[0])], 1
    )


def projection_rows(first, second, gain):
    t = lax.axis_index("tp")
    a, b = first[...].astype(F32), second[...].astype(F32)
    wide = jnp.concatenate([jnp.where(t == 0, a, b), jnp.where(t == 0, b, a)], 1)
    row = gain_row(gain, wide.shape[0])
    return jnp.concatenate([(wide * row).astype(BF), row.astype(BF)], 0), wide


def pack(q, csum, moments, message):
    columns = q.shape[1]
    half = csum.shape[0]
    message[:, :columns] = q.astype(BF)
    high = csum.astype(BF)
    low = (csum - high.astype(F32)).astype(BF)
    message[:, columns : columns + LANES] = jnp.concatenate([high, low], 0)
    high = moments.astype(BF).astype(F32)
    low = moments - high
    lanes = lane_ids(q.shape[0])
    both = jnp.where(lanes < 2, high, jnp.where(lanes < 4, pltpu.roll(low, 2, 1), 0.0))
    message[:, columns + LANES :] = both.astype(BF)
    assert 2 * half == q.shape[0]


def unpack_sum(state, messages):
    rows, total = state.shape
    columns = total - 2 * LANES
    half = rows // 2
    q = state[:, :columns]
    csum = state[:half, columns : columns + LANES]
    moments = state[:, columns + LANES :]
    for m in messages:
        q = q + m[:, :columns].astype(F32)
        c = m[:, columns : columns + LANES].astype(F32)
        csum = csum + c[:half] + c[half:]
        v = m[:, columns + LANES :].astype(F32)
        moments = moments + v + pltpu.roll(v, LANES - 2, 1)
    return q, csum, jnp.where(lane_ids(rows) < 2, moments, 0.0)


def store_state(q, csum, moments, state):
    columns = q.shape[1]
    state[:, :columns] = q
    state[:, columns : columns + LANES] = jnp.concatenate([csum, jnp.zeros_like(csum)], 0)
    state[:, columns + LANES :] = moments


def first_load_kernel(
    w_query,
    tokens,
    gain,
    lengths,
    decay,
    w_out,
    tokens_out,
    gain_out,
    length_out,
    rate_out,
    length_scalars,
    decay_scalars,
    sems,
):
    pairs = (
        (lengths, length_scalars),
        (decay, decay_scalars),
        (tokens, tokens_out),
        (gain, gain_out),
        (w_query, w_out),
    )
    copies = [pltpu.make_async_copy(a, b, sems.at[i]) for i, (a, b) in enumerate(pairs)]
    for copy in copies:
        copy.start()
    copies[0].wait()
    length_out[...] = column_of(length_scalars, length_out.shape[0], jnp.int32)
    copies[1].wait()
    rate_out[...] = column_of(decay_scalars, rate_out.shape[0], F32)
    for copy in copies[2:]:
        copy.wait()


def cache_load_kernel(after, values, values_out, sem):
    copy = pltpu.make_async_copy(values, values_out, sem)
    copy.start()
    copy.wait()


def query_kernel(first, second, gain, w_query, state, message):
    lhs, wide = projection_rows(first, second, gain)
    rows = wide.shape[0]
    product = jnp.dot(lhs, w_query[...], preferred_element_type=F32)
    half = rows // 2
    ids = row_ids(half)
    csum = jnp.zeros((half, LANES), F32)
    for i in range(product.shape[1] // LANES):
        csum = jnp.where(
            ids == i, product[rows : rows + half, i * LANES : (i + 1) * LANES], csum
        )
    lanes = lane_ids(rows)
    first_sum = jnp.sum(wide, 1, keepdims=True)
    second_sum = jnp.sum(wide * wide, 1, keepdims=True)
    moments = jnp.where(lanes == 0, first_sum, jnp.where(lanes == 1, second_sum, 0.0))
    store_state(product[:rows], csum, moments, state)
    pack(product[:rows], csum, moments, message)


def middle_kernel(old, m1, m2, m3, state, message):
    q, csum, moments = unpack_sum(old, (m1, m2, m3))
    store_state(q, csum, moments, state)
    pack(q, csum, moments, message)


def other_kernel(
    after,
    lengths,
    rates,
    first,
    second,
    gain,
    w_key,
    w_value,
    w_gate,
    w_output,
    keys,
    k_out,
    v_out,
    g_out,
    turn,
    weights,
    w_keep,
    w_send,
    keys_out,
    key_buffer,
    value_buffer,
    gate_buffer,
    sems,
):
    own = w_keep.shape[1]
    t = lax.axis_index("tp")
    kept = pl.ds(pl.multiple_of(t * own, own), own)
    sent = pl.ds(pl.multiple_of((1 - t) * own, own), own)
    buffers = (key_buffer, value_buffer, gate_buffer)
    pairs = (
        (w_key, key_buffer),
        (w_value, value_buffer),
        (w_gate, gate_buffer),
        (w_output.at[:, sent], w_send),
        (w_output.at[:, kept], w_keep),
        (keys, keys_out),
    )
    copies = [pltpu.make_async_copy(a, b, sems.at[i]) for i, (a, b) in enumerate(pairs)]
    for copy in copies:
        copy.start()
    lhs, wide = projection_rows(first, second, gain)
    rows = wide.shape[0]
    half = HEAD_KEY // 2
    entry = (lane_ids(rows) % half).astype(F32)
    inverse = jnp.exp(entry * (-math.log(THETA) / half))
    angle = lengths[...].astype(F32) * inverse
    turn[0] = jnp.cos(angle)
    turn[1] = jnp.sin(angle)
    heads = rates.shape[0]
    places = lax.axis_index("kv") * LANES + lane_ids(heads)
    rate = rates[...]
    for s in range(rows):
        distance = jnp.broadcast_to(lengths[s : s + 1, :], (heads, LANES)) - places
        weight = jnp.exp(-rate * jnp.maximum(distance, 0).astype(F32)) * HEAD_KEY ** (-0.5)
        weights[s] = jnp.where(distance > 0, weight, 0.0)
    for copy, buffer, out in zip(copies, buffers, (k_out, v_out, g_out)):
        copy.wait()
        product = jnp.dot(lhs, buffer[...], preferred_element_type=F32)
        out[...] = product[: rows + 8]
    for copy in copies[len(buffers) :]:
        copy.wait()


def attend_kernel(
    width,
    after,
    old,
    m1,
    m2,
    m3,
    k_part,
    v_part,
    g_part,
    turn,
    weights,
    keys,
    values,
    out,
    query_rows,
    cached,
):
    rows, _, key_columns = keys.shape
    heads = key_columns // HEAD_KEY
    q, csum, moments = unpack_sum(old, (m1, m2, m3))
    average = moments[:, 0:1] / width
    inverse = lax.rsqrt(moments[:, 1:2] / width - average * average + EPS)
    lanes = lane_ids(rows)
    in_first = lanes % HEAD_KEY < HEAD_KEY // 2
    low_head = lanes < HEAD_KEY
    top = rows // 2
    cosine, sine = turn[0], turn[1]
    for i in range(key_columns // LANES):
        cut = slice(i * LANES, (i + 1) * LANES)
        plain = inverse * (q[:, cut] - average * csum[i : i + 1])
        partner = jnp.where(
            in_first,
            -pltpu.roll(plain, LANES - HEAD_KEY // 2, 1),
            pltpu.roll(plain, HEAD_KEY // 2, 1),
        )
        turned = plain * cosine + partner * sine
        query_rows[:, cut] = turned.astype(BF).astype(F32)
        part = inverse * (k_part[:rows, cut] - average * k_part[rows : rows + 1, cut])
        both = plain * part * HEAD_KEY ** (-0.5)
        for j in range(2):
            picked = jnp.where(low_head == (j == 0), both, 0.0)
            score = jnp.sum(picked, 1, keepdims=True)
            high = score.astype(BF).astype(F32)
            low = score - high
            folded = jnp.where(
                lanes[:top] < HEAD_KEY,
                jnp.where(in_first[:top], high[:top], low[:top]),
                jnp.where(in_first[:top], high[top:], low[top:]),
            )
            out[2 * i + j, 3 * rows :, :] = folded.astype(BF)
    for h in range(heads):
        cut = slice(h * LANES, (h + 1) * LANES)
        for place, part in ((1, v_part), (2, g_part)):
            normed = inverse * (part[:rows, cut] - average * part[rows : rows + 1, cut])
            out[h, place * rows : (place + 1) * rows, :] = normed.astype(BF)

    head_of_key = lax.broadcasted_iota(jnp.int32, (heads, key_columns), 1) // HEAD_KEY
    own_key = head_of_key == row_ids(heads, key_columns)
    value_columns = heads * HEAD_VALUE
    head_of_value = lax.broadcasted_iota(jnp.int32, (heads, value_columns), 1) // HEAD_VALUE
    own_value = head_of_value == row_ids(heads, value_columns)
    for s in range(rows):
        spread = jnp.broadcast_to(query_rows[s : s + 1, :], (heads, key_columns))
        query = jnp.where(own_key, spread, 0.0).astype(BF)
        scores = lax.dot_general(
            query, keys[s], (((1,), (1,)), ((), ())), preferred_element_type=F32
        )
        coefficients = (scores * weights[s]).astype(BF)
        product = jnp.dot(coefficients, values[s], preferred_element_type=F32)
        cached[s : s + 1, :] = jnp.sum(
            jnp.where(own_value, product, 0.0), 0, keepdims=True
        )
    for h in range(heads):
        out[h, :rows, :] = cached[:, h * LANES : (h + 1) * LANES].astype(BF)


def gate_kernel(pieces, head_gain, out):
    rows = out.shape[1]
    total = jnp.sum(pieces[...].astype(F32), 0)
    cached, value, gate = (total[i * rows : (i + 1) * rows] for i in range(3))
    folded = total[3 * rows :]
    half = HEAD_KEY // 2
    score = jnp.concatenate(
        [folded[:, i : i + 1] + folded[:, i + half : i + half + 1] for i in (0, HEAD_KEY)], 0
    )
    retained = cached + score * value
    centered = retained - jnp.mean(retained, -1, keepdims=True)
    spread = lax.rsqrt(jnp.mean(centered * centered, -1, keepdims=True) + EPS)
    gains = head_gain[...].astype(F32)
    mine = row_ids(gains.shape[0]) == lax.axis_index("kv")
    gain = jnp.sum(jnp.where(mine, gains, 0.0), 0, keepdims=True)
    normed = centered * spread * gain
    gated = (gate * jax.nn.sigmoid(gate) * normed).astype(BF)
    out[...] = jnp.broadcast_to(gated[None], out.shape)


def output_kernel(gated, w_keep, w_got, tokens, own, out):
    heads = gated.shape[0] // 2
    t = lax.axis_index("tp")
    branch = 0.0
    for group, w in ((t, w_keep), (1 - t, w_got)):
        lhs = jnp.concatenate([gated[2 * h + group] for h in range(heads)], 1)
        part = jnp.dot(lhs, w[...], preferred_element_type=F32)
        branch = branch + part.astype(BF).astype(F32)
    residual = (tokens[...].astype(F32) + branch).astype(BF)
    own[...] = residual
    out[...] = jnp.broadcast_to(residual[None], out.shape)


def mixer_kernel(residual, mlp_gain, w_up, w_down, out):
    blocks, rows, own = residual.shape
    width = blocks * own
    first = jnp.zeros((rows, own), F32)
    second = jnp.zeros((rows, own), F32)
    scaled, gain = [], []
    gains = mlp_gain[...].astype(F32)
    for i in range(blocks):
        wide = residual[i].astype(F32)
        first = first + wide
        second = second + wide * wide
        row = gains[i : i + 1]
        scaled.append((wide * row).astype(BF))
        gain.append(jnp.broadcast_to(row, wide.shape).astype(BF))
    lhs = jnp.concatenate([jnp.concatenate(scaled, 1), jnp.concatenate(gain, 1)], 0)
    up = jnp.dot(lhs, w_up[...], preferred_element_type=F32)
    average = jnp.sum(first, 1, keepdims=True) / width
    inverse = lax.rsqrt(jnp.sum(second, 1, keepdims=True) / width - average * average + EPS)
    hidden = inverse * (up[:rows] - average * up[rows : rows + 1])
    hidden = jnp.square(jnp.maximum(hidden, 0.0)).astype(BF)
    down = jnp.dot(hidden, w_down[...], preferred_element_type=F32)
    for i in range(blocks):
        out[i] = down[:, i * own : (i + 1) * own].astype(BF)


def final_kernel(pieces, own, out):
    total = jnp.sum(pieces[...].astype(F32), 0)
    out[...] = (own[...].astype(F32) + total).astype(BF)


VMEM = pl.BlockSpec(memory_space=pltpu.VMEM)
HBM = pl.BlockSpec(memory_space=pltpu.HBM)
ANY = pl.BlockSpec(memory_space=pl.ANY)


def in_hbm(*arrays):
    return [pltpu.with_memory_space_constraint(x, pltpu.HBM) for x in arrays]


def call(kernel, outs, in_specs, flops=0, bytes_accessed=0, scratch=(), limit=None):
    return pl.pallas_call(
        kernel,
        out_shape=outs,
        in_specs=in_specs,
        out_specs=jax.tree.map(lambda _: VMEM, outs),
        scratch_shapes=list(scratch),
        cost_estimate=pl.CostEstimate(
            flops=flops, bytes_accessed=bytes_accessed, transcendentals=0
        ),
        compiler_params=pltpu.CompilerParams(vmem_limit_bytes=limit),
    )


def make_kernels_on_device(kv, tp):
    def on_device(
        tokens,
        lengths,
        attn_gain,
        w_query,
        w_key,
        w_value,
        w_gate,
        decay_rate,
        key_cache,
        value_cache,
        head_gain,
        w_output,
        mlp_gain,
        w_up,
        w_down,
    ):
        S, own = tokens.shape
        H = decay_rate.shape[0]
        width = own * kv * tp
        qc, vc = H * HEAD_KEY, H * HEAD_VALUE
        swap = [(0, 1), (1, 0)]
        mib = 1 << 20
        sds = jax.ShapeDtypeStruct

        other = lax.ppermute(tokens, "tp", swap)
        gain = attn_gain.reshape(-1, LANES)
        w_query, tokens, gain, length_rows, rates = call(
            first_load_kernel,
            (
                sds(w_query.shape, BF),
                sds(tokens.shape, BF),
                sds(gain.shape, BF),
                sds((S, LANES), jnp.int32),
                sds((H, LANES), F32),
            ),
            [HBM] * 5,
            flops=10**9,
            scratch=[
                pltpu.SMEM((S,), jnp.int32),
                pltpu.SMEM((H,), F32),
                pltpu.SemaphoreType.DMA((5,)),
            ],
            limit=2 * mib,
        )(*in_hbm(w_query, tokens, gain, lengths, decay_rate))
        columns = qc + 2 * LANES
        message_types = (sds((S, columns), F32), sds((S, columns), BF))
        state, message = call(
            query_kernel, message_types, [VMEM] * 4, limit=2 * mib
        )(tokens, other, gain, w_query)

        def exchange(message, stride):
            return [
                lax.ppermute(message, "kv", [(i, i ^ (j * stride)) for i in range(kv)])
                for j in range(1, 4)
            ]

        got = exchange(message, 1)
        k_part, v_part, g_part, turn, weights, w_keep, w_send, keys = call(
            other_kernel,
            (
                sds((S + 8, qc), F32),
                sds((S + 8, vc), F32),
                sds((S + 8, vc), F32),
                sds((2, S, LANES), F32),
                sds((S, H, LANES), F32),
                sds((w_output.shape[0], own), BF),
                sds((w_output.shape[0], own), BF),
                sds(key_cache.shape, BF),
            ),
            [ANY] + [VMEM] * 5 + [HBM] * 5,
            flops=10**9,
            scratch=[pltpu.VMEM(w.shape, BF) for w in (w_key, w_value, w_gate)]
            + [pltpu.SemaphoreType.DMA((6,))],
            limit=6 * mib,
        )(
            message,
            length_rows,
            rates,
            tokens,
            other,
            gain,
            *in_hbm(w_key, w_value, w_gate, w_output, key_cache),
        )
        w_got = lax.ppermute(w_send, "tp", swap)

        stride = 4
        while stride < kv:
            state, message = call(
                middle_kernel, message_types, [VMEM] * 4, limit=2 * mib
            )(state, *got)
            got = exchange(message, stride)
            stride *= 4
        values = call(
            cache_load_kernel,
            sds(value_cache.shape, BF),
            [ANY, HBM],
            flops=10**9,
            scratch=[pltpu.SemaphoreType.DMA],
            limit=2 * mib,
        )(message, *in_hbm(value_cache))

        pieces = call(
            functools.partial(attend_kernel, width),
            sds((H, 3 * S + S // 2, LANES), BF),
            [ANY] + [VMEM] * 11,
            scratch=[pltpu.VMEM((S, qc), F32), pltpu.VMEM((S, vc), F32)],
            limit=4 * mib,
        )(w_got, state, *got, k_part, v_part, g_part, turn, weights, keys, values)

        pieces = lax.all_to_all(pieces, "kv", 0, 0, tiled=True)
        gated = call(
            gate_kernel, sds((kv * tp, S, LANES), BF), [VMEM] * 2, limit=2 * mib
        )(pieces, head_gain.reshape(H, HEAD_VALUE))
        gated = lax.all_to_all(gated, ("kv", "tp"), 0, 0, tiled=True)
        residual, spread = call(
            output_kernel,
            (sds((S, own), BF), sds((kv * tp, S, own), BF)),
            [VMEM] * 4,
            limit=4 * mib,
        )(gated, w_keep, w_got, tokens)
        spread = lax.all_to_all(spread, ("kv", "tp"), 0, 0, tiled=True)
        down = call(
            mixer_kernel, sds((kv * tp, S, own), BF), [VMEM] * 4, limit=16 * mib
        )(spread, mlp_gain.reshape(-1, LANES), w_up, w_down)
        down = lax.all_to_all(down, ("kv", "tp"), 0, 0, tiled=True)
        return call(final_kernel, sds((S, own), BF), [VMEM] * 2, limit=2 * mib)(down, residual)

    return on_device


def solution(mesh):
    in_specs = (
        P(None, ("kv", "tp")),
        P(),
        P("kv"),
        P("kv", "tp"),
        P("kv", "tp"),
        P("kv", "tp"),
        P("kv", "tp"),
        P("tp"),
        P(None, "kv", "tp"),
        P(None, "kv", "tp"),
        P("tp"),
        P("tp", "kv"),
        P(),
        P(None, ("kv", "tp")),
        P(("kv", "tp"), None),
    )
    kv, tp = mesh.shape["kv"], mesh.shape["tp"]

    def on_device(*arrays):
        fits = tp == 2 and arrays[7].shape[0] == kv
        fits = fits and arrays[0].shape[1] == LANES == arrays[8].shape[1]
        make = make_kernels_on_device if fits else make_on_device
        return make(kv, tp)(*arrays)

    return jax.shard_map(
        on_device,
        mesh=mesh,
        in_specs=in_specs,
        out_specs=P(None, ("kv", "tp")),
        check_vma=False,
    )
```

```python
import functools
import math

import jax
import jax.numpy as jnp
from jax import lax
from jax.experimental import pallas as pl
from jax.experimental.pallas import tpu as pltpu
from jax.sharding import PartitionSpec as P


HEAD_KEY = 64
HEAD_VALUE = 128
EPS = 1e-05
THETA = 10000.0
LANES = 128

BF = jnp.bfloat16
F32 = jnp.float32


def split_two(x):
    high = x.astype(BF)
    return high, (x - high.astype(F32)).astype(BF)


def rotate(flat, cosine, sine):
    rows = flat.shape[0]
    grouped = flat.reshape(rows, -1, HEAD_KEY)
    half = HEAD_KEY // 2
    a, b = grouped[..., :half], grouped[..., half:]
    c, s = cosine[:, None, :], sine[:, None, :]
    return jnp.concatenate([a * c - b * s, b * c + a * s], -1).reshape(rows, -1)


def broadcast_gather(x, axes, size):
    spread = jnp.broadcast_to(x[None], (size,) + x.shape)
    return lax.all_to_all(spread, axes, 0, 0, tiled=True)


def make_on_device(kv, tp):
    def on_device(
        tokens,
        lengths,
        attn_gain,
        w_query,
        w_key,
        w_value,
        w_gate,
        decay_rate,
        key_cache,
        value_cache,
        head_gain,
        w_output,
        mlp_gain,
        w_up,
        w_down,
    ):
        S = tokens.shape[0]
        H = decay_rate.shape[0]
        span = key_cache.shape[1]
        width = tokens.shape[1] * kv * tp
        own = tokens.shape[1]
        kvi = lax.axis_index("kv")
        tpi = lax.axis_index("tp")
        groups = kv // H
        rows = S // groups

        if tp == 2:
            other = lax.ppermute(tokens, "tp", [(0, 1), (1, 0)])
            low = jnp.where(tpi == 0, tokens, other)
            high = jnp.where(tpi == 0, other, tokens)
            block = jnp.concatenate([low, high], 1)
        else:
            block = lax.all_gather(tokens, "tp", axis=1, tiled=True)
        wide = block.astype(F32)
        scaled = (wide * attn_gain.astype(F32)).astype(BF)
        lhs = jnp.concatenate([scaled, attn_gain[None, :]], 0)
        part_q = jnp.dot(lhs, w_query, preferred_element_type=F32)
        moments = jnp.stack([jnp.sum(wide, -1), jnp.sum(wide * wide, -1)], -1)

        small = jnp.concatenate([part_q[S], moments.reshape(-1)])
        q_sum = part_q[:S]
        stride = 1
        while stride < kv:
            count = 4 if kv % (stride * 4) == 0 else 2
            high, low = split_two(small)
            tail = jnp.concatenate([high, low])
            pad = -tail.shape[0] % S
            tail = jnp.pad(tail, (0, pad)).reshape(S, -1)
            message = jnp.concatenate([q_sum.astype(BF), tail], 1)
            for j in range(1, count):
                got = lax.ppermute(message, "kv", [(i, i ^ (j * stride)) for i in range(kv)])
                got = got.astype(F32)
                q_sum = q_sum + got[:, : q_sum.shape[1]]
                flat = got[:, q_sum.shape[1] :].reshape(-1)
                n = small.shape[0]
                small = small + flat[:n] + flat[n : 2 * n]
            stride *= count
        csum_q = small[: q_sum.shape[1]]
        moments = small[q_sum.shape[1] :].reshape(S, 2)
        average = moments[:, 0] / width
        inverse = lax.rsqrt(moments[:, 1] / width - average * average + EPS)

        half = HEAD_KEY // 2
        turn = jnp.power(THETA, -jnp.arange(half, dtype=F32) / half)
        angles = lengths.astype(F32)[:, None] * turn[None, :]
        q_plain = inverse[:, None] * (q_sum - average[:, None] * csum_q[None, :])
        queries = rotate(q_plain, jnp.cos(angles), jnp.sin(angles)).astype(BF)
        queries = queries.reshape(S, H, HEAD_KEY)

        def partial(w):
            p = jnp.dot(lhs, w, preferred_element_type=F32)
            return inverse[:, None] * (p[:S] - average[:, None] * p[S:])

        part_k = partial(w_key).reshape(S, H, HEAD_KEY)
        part_v = partial(w_value).reshape(S, H, HEAD_VALUE)
        part_g = partial(w_gate).reshape(S, H, HEAD_VALUE)
        part_score = jnp.sum(q_plain.reshape(S, H, HEAD_KEY) * part_k, -1) * HEAD_KEY ** (-0.5)

        keys = key_cache.reshape(S, span, H, HEAD_KEY)
        values = value_cache.reshape(S, span, H, HEAD_VALUE)
        scores = jnp.einsum("bhd,bjhd->bhj", queries, keys, preferred_element_type=F32)
        places = kvi * span + jnp.arange(span, dtype=jnp.int32)
        distance = jnp.maximum(lengths[:, None] - places[None, :], 0).astype(F32)
        live = (places[None, :] < lengths[:, None])[:, None, :]
        decays = jnp.where(
            live, jnp.exp(-decay_rate[None, :, None] * distance[:, None, :]), 0.0
        )
        coefficients = (scores * HEAD_KEY ** (-0.5) * decays).astype(BF)
        part_c = jnp.einsum("bhj,bjhe->bhe", coefficients, values, preferred_element_type=F32)

        high, low = split_two(part_score)
        pieces = jnp.concatenate(
            [
                part_c.astype(BF),
                part_v.astype(BF),
                part_g.astype(BF),
                high[..., None],
                low[..., None],
                jnp.zeros((S, H, 126), BF),
            ],
            -1,
        )
        pieces = pieces.transpose(1, 0, 2).reshape(kv, rows, 4 * HEAD_VALUE)
        mine = jnp.sum(
            lax.all_to_all(pieces, "kv", 0, 0, tiled=True).astype(F32), 0
        )
        cached, value, gate = (
            mine[:, i * HEAD_VALUE : (i + 1) * HEAD_VALUE] for i in range(3)
        )
        score = mine[:, 3 * HEAD_VALUE] + mine[:, 3 * HEAD_VALUE + 1]
        retained = cached + score[:, None] * value
        centered = retained - jnp.mean(retained, -1, keepdims=True)
        gain = lax.dynamic_slice(head_gain, ((kvi // groups) * HEAD_VALUE,), (HEAD_VALUE,))
        normed = (
            centered
            * lax.rsqrt(jnp.mean(centered * centered, -1, keepdims=True) + EPS)
            * gain.astype(F32)
        )
        gated = (jax.nn.silu(gate) * normed).astype(BF)
        gathered = broadcast_gather(gated, "kv", kv).reshape(H, S, HEAD_VALUE)
        gathered = gathered.transpose(1, 0, 2).reshape(S, H * HEAD_VALUE)
        part_b = jnp.dot(gathered, w_output, preferred_element_type=F32).astype(BF)
        part_b = part_b.reshape(S, tp, own).transpose(1, 0, 2)
        if tp == 2:
            keep = jnp.where(tpi == 0, part_b[0], part_b[1])
            send = jnp.where(tpi == 0, part_b[1], part_b[0])
            got = lax.ppermute(send, "tp", [(0, 1), (1, 0)])
            branch = keep.astype(F32) + got.astype(F32)
        else:
            branch = jnp.sum(
                lax.all_to_all(part_b, "tp", 0, 0, tiled=True).astype(F32), 0
            )
        own_residual = (tokens.astype(F32) + branch).astype(BF)

        residual = broadcast_gather(own_residual, ("kv", "tp"), kv * tp)
        residual = residual.transpose(1, 0, 2).reshape(S, width)
        wide = residual.astype(F32)
        scaled = (wide * mlp_gain.astype(F32)).astype(BF)
        lhs = jnp.concatenate([scaled, mlp_gain[None, :]], 0)
        up = jnp.dot(lhs, w_up, preferred_element_type=F32)
        average = jnp.sum(wide, -1) / width
        inverse = lax.rsqrt(jnp.sum(wide * wide, -1) / width - average * average + EPS)
        hidden = inverse[:, None] * (up[:S] - average[:, None] * up[S:])
        hidden = jnp.square(jax.nn.relu(hidden)).astype(BF)
        down = jnp.dot(hidden, w_down, preferred_element_type=F32).astype(BF)
        down = down.reshape(S, kv * tp, own).transpose(1, 0, 2)
        mixer = jnp.sum(
            lax.all_to_all(down, ("kv", "tp"), 0, 0, tiled=True).astype(F32), 0
        )
        return (own_residual.astype(F32) + mixer).astype(BF)

    return on_device


def lane_ids(rows):
    return lax.broadcasted_iota(jnp.int32, (rows, LANES), 1)


def row_ids(rows, columns=LANES):
    return lax.broadcasted_iota(jnp.int32, (rows, columns), 0)


def column_of(scalars, rows, dtype):
    ids = row_ids(rows)
    out = jnp.zeros((rows, LANES), dtype)
    for i in range(rows):
        out = jnp.where(ids == i, scalars[i].astype(dtype), out)
    return out


def gain_row(gain, rows):
    wide = gain[...].astype(F32)
    return jnp.concatenate(
        [jnp.broadcast_to(wide[i : i + 1], (rows, LANES)) for i in range(wide.shape[0])], 1
    )


def projection_rows(first, second, gain):
    t = lax.axis_index("tp")
    a, b = first[...].astype(F32), second[...].astype(F32)
    wide = jnp.concatenate([jnp.where(t == 0, a, b), jnp.where(t == 0, b, a)], 1)
    row = gain_row(gain, wide.shape[0])
    return jnp.concatenate([(wide * row).astype(BF), row.astype(BF)], 0), wide


def pack(q, csum, moments, message):
    columns = q.shape[1]
    half = csum.shape[0]
    message[:, :columns] = q.astype(BF)
    high = csum.astype(BF)
    low = (csum - high.astype(F32)).astype(BF)
    message[:, columns : columns + LANES] = jnp.concatenate([high, low], 0)
    high = moments.astype(BF).astype(F32)
    low = moments - high
    lanes = lane_ids(q.shape[0])
    both = jnp.where(lanes < 2, high, jnp.where(lanes < 4, pltpu.roll(low, 2, 1), 0.0))
    message[:, columns + LANES :] = both.astype(BF)
    assert 2 * half == q.shape[0]


def unpack_sum(state, messages):
    rows, total = state.shape
    columns = total - 2 * LANES
    half = rows // 2
    q = state[:, :columns]
    csum = state[:half, columns : columns + LANES]
    moments = state[:, columns + LANES :]
    for m in messages:
        q = q + m[:, :columns].astype(F32)
        c = m[:, columns : columns + LANES].astype(F32)
        csum = csum + c[:half] + c[half:]
        v = m[:, columns + LANES :].astype(F32)
        moments = moments + v + pltpu.roll(v, LANES - 2, 1)
    return q, csum, jnp.where(lane_ids(rows) < 2, moments, 0.0)


def store_state(q, csum, moments, state):
    columns = q.shape[1]
    state[:, :columns] = q
    state[:, columns : columns + LANES] = jnp.concatenate([csum, jnp.zeros_like(csum)], 0)
    state[:, columns + LANES :] = moments


def first_load_kernel(
    w_query,
    tokens,
    gain,
    lengths,
    decay,
    w_out,
    tokens_out,
    gain_out,
    length_out,
    rate_out,
    length_scalars,
    decay_scalars,
    sems,
):
    pairs = (
        (lengths, length_scalars),
        (decay, decay_scalars),
        (tokens, tokens_out),
        (gain, gain_out),
        (w_query, w_out),
    )
    copies = [pltpu.make_async_copy(a, b, sems.at[i]) for i, (a, b) in enumerate(pairs)]
    for copy in copies:
        copy.start()
    copies[0].wait()
    length_out[...] = column_of(length_scalars, length_out.shape[0], jnp.int32)
    copies[1].wait()
    rate_out[...] = column_of(decay_scalars, rate_out.shape[0], F32)
    for copy in copies[2:]:
        copy.wait()


def live_scalars(lengths, base):
    values = lengths[...]
    return [values[s, 0] > base for s in range(values.shape[0])]


def cache_load_kernel(
    after, lengths, keys, values, keys_out, values_out, key_sems, value_sems
):
    live = live_scalars(lengths, lax.axis_index("kv") * keys.shape[1])

    def copies(s):
        return (
            pltpu.make_async_copy(keys.at[s], keys_out.at[s], key_sems.at[s]),
            pltpu.make_async_copy(values.at[s], values_out.at[s], value_sems.at[s]),
        )

    for s in range(keys.shape[0]):

        @pl.when(live[s])
        def _():
            for copy in copies(s):
                copy.start()

    for s in range(keys.shape[0]):

        @pl.when(live[s])
        def _():
            for copy in copies(s):
                copy.wait()


def query_kernel(first, second, gain, w_query, state, message):
    lhs, wide = projection_rows(first, second, gain)
    rows = wide.shape[0]
    product = jnp.dot(lhs, w_query[...], preferred_element_type=F32)
    half = rows // 2
    ids = row_ids(half)
    csum = jnp.zeros((half, LANES), F32)
    for i in range(product.shape[1] // LANES):
        csum = jnp.where(
            ids == i, product[rows : rows + half, i * LANES : (i + 1) * LANES], csum
        )
    lanes = lane_ids(rows)
    first_sum = jnp.sum(wide, 1, keepdims=True)
    second_sum = jnp.sum(wide * wide, 1, keepdims=True)
    moments = jnp.where(lanes == 0, first_sum, jnp.where(lanes == 1, second_sum, 0.0))
    store_state(product[:rows], csum, moments, state)
    pack(product[:rows], csum, moments, message)


def middle_kernel(old, m1, m2, m3, state, message):
    q, csum, moments = unpack_sum(old, (m1, m2, m3))
    store_state(q, csum, moments, state)
    pack(q, csum, moments, message)


def other_kernel(
    after,
    lengths,
    rates,
    first,
    second,
    gain,
    w_key,
    w_value,
    w_gate,
    w_output,
    k_out,
    v_out,
    g_out,
    turn,
    weights,
    w_keep,
    w_send,
    key_buffer,
    value_buffer,
    gate_buffer,
    sems,
):
    own = w_keep.shape[1]
    t = lax.axis_index("tp")
    kept = pl.ds(pl.multiple_of(t * own, own), own)
    sent = pl.ds(pl.multiple_of((1 - t) * own, own), own)
    buffers = (key_buffer, value_buffer, gate_buffer)
    pairs = (
        (w_key, key_buffer),
        (w_value, value_buffer),
        (w_gate, gate_buffer),
        (w_output.at[:, sent], w_send),
        (w_output.at[:, kept], w_keep),
    )
    copies = [pltpu.make_async_copy(a, b, sems.at[i]) for i, (a, b) in enumerate(pairs)]
    for copy in copies:
        copy.start()
    lhs, wide = projection_rows(first, second, gain)
    rows = wide.shape[0]
    half = HEAD_KEY // 2
    entry = (lane_ids(rows) % half).astype(F32)
    inverse = jnp.exp(entry * (-math.log(THETA) / half))
    angle = lengths[...].astype(F32) * inverse
    turn[0] = jnp.cos(angle)
    turn[1] = jnp.sin(angle)
    heads = rates.shape[0]
    places = lax.axis_index("kv") * LANES + lane_ids(heads)
    rate = rates[...]
    for s in range(rows):
        distance = jnp.broadcast_to(lengths[s : s + 1, :], (heads, LANES)) - places
        weight = jnp.exp(-rate * jnp.maximum(distance, 0).astype(F32)) * HEAD_KEY ** (-0.5)
        weights[s] = jnp.where(distance > 0, weight, 0.0)
    for copy, buffer, out in zip(copies, buffers, (k_out, v_out, g_out)):
        copy.wait()
        product = jnp.dot(lhs, buffer[...], preferred_element_type=F32)
        out[...] = product[: rows + 8]
    for copy in copies[len(buffers) :]:
        copy.wait()


def attend_kernel(
    width,
    after,
    lengths,
    old,
    m1,
    m2,
    m3,
    k_part,
    v_part,
    g_part,
    turn,
    weights,
    keys,
    values,
    out,
    query_rows,
    cached,
    order,
):
    rows, span, key_columns = keys.shape
    heads = key_columns // HEAD_KEY
    q, csum, moments = unpack_sum(old, (m1, m2, m3))
    average = moments[:, 0:1] / width
    inverse = lax.rsqrt(moments[:, 1:2] / width - average * average + EPS)
    lanes = lane_ids(rows)
    in_first = lanes % HEAD_KEY < HEAD_KEY // 2
    low_head = lanes < HEAD_KEY
    top = rows // 2
    cosine, sine = turn[0], turn[1]
    for i in range(key_columns // LANES):
        cut = slice(i * LANES, (i + 1) * LANES)
        plain = inverse * (q[:, cut] - average * csum[i : i + 1])
        partner = jnp.where(
            in_first,
            -pltpu.roll(plain, LANES - HEAD_KEY // 2, 1),
            pltpu.roll(plain, HEAD_KEY // 2, 1),
        )
        turned = plain * cosine + partner * sine
        query_rows[:, cut] = turned.astype(BF).astype(F32)
        part = inverse * (k_part[:rows, cut] - average * k_part[rows : rows + 1, cut])
        both = plain * part * HEAD_KEY ** (-0.5)
        for j in range(2):
            picked = jnp.where(low_head == (j == 0), both, 0.0)
            score = jnp.sum(picked, 1, keepdims=True)
            high = score.astype(BF).astype(F32)
            low = score - high
            folded = jnp.where(
                lanes[:top] < HEAD_KEY,
                jnp.where(in_first[:top], high[:top], low[:top]),
                jnp.where(in_first[:top], high[top:], low[top:]),
            )
            out[2 * i + j, 3 * rows :, :] = folded.astype(BF)
    for h in range(heads):
        cut = slice(h * LANES, (h + 1) * LANES)
        for place, part in ((1, v_part), (2, g_part)):
            normed = inverse * (part[:rows, cut] - average * part[rows : rows + 1, cut])
            out[h, place * rows : (place + 1) * rows, :] = normed.astype(BF)

    head_of_key = lax.broadcasted_iota(jnp.int32, (heads, key_columns), 1) // HEAD_KEY
    own_key = head_of_key == row_ids(heads, key_columns)
    value_columns = heads * HEAD_VALUE
    head_of_value = lax.broadcasted_iota(jnp.int32, (heads, value_columns), 1) // HEAD_VALUE
    own_value = head_of_value == row_ids(heads, value_columns)
    live = live_scalars(lengths, lax.axis_index("kv") * span)
    count = jnp.int32(0)
    for s in range(rows):
        order[count] = s
        count = count + live[s].astype(jnp.int32)

    def one(s, is_live):
        row = pl.ds(s, 1)
        spread = jnp.broadcast_to(query_rows[row, :], (heads, key_columns))
        query = jnp.where(own_key, spread, 0.0).astype(BF)
        scores = lax.dot_general(
            query, keys[s], (((1,), (1,)), ((), ())), preferred_element_type=F32
        )
        weight = weights[s]
        coefficients = jnp.where(weight > 0.0, scores * weight, 0.0).astype(BF)
        product = jnp.dot(coefficients, values[s], preferred_element_type=F32)
        kept = jnp.logical_and(own_value, is_live)
        cached[row, :] = jnp.sum(jnp.where(kept, product, 0.0), 0, keepdims=True)

    steps = [n for n in (4, 8) if n < rows] + [rows]
    for least, most in zip([-1] + steps[:-1], steps):

        @pl.when(jnp.logical_and(count > least, count <= most))
        def _():
            if most == rows:
                for s in range(rows):
                    one(s, live[s])
            else:
                cached[...] = jnp.zeros_like(cached)
                for i in range(most):
                    one(order[jnp.minimum(i, jnp.maximum(count - 1, 0))], count > 0)

    for h in range(heads):
        out[h, :rows, :] = cached[:, h * LANES : (h + 1) * LANES].astype(BF)


def gate_kernel(pieces, head_gain, out):
    rows = out.shape[1]
    total = jnp.sum(pieces[...].astype(F32), 0)
    cached, value, gate = (total[i * rows : (i + 1) * rows] for i in range(3))
    folded = total[3 * rows :]
    half = HEAD_KEY // 2
    score = jnp.concatenate(
        [folded[:, i : i + 1] + folded[:, i + half : i + half + 1] for i in (0, HEAD_KEY)], 0
    )
    retained = cached + score * value
    centered = retained - jnp.mean(retained, -1, keepdims=True)
    spread = lax.rsqrt(jnp.mean(centered * centered, -1, keepdims=True) + EPS)
    gains = head_gain[...].astype(F32)
    mine = row_ids(gains.shape[0]) == lax.axis_index("kv")
    gain = jnp.sum(jnp.where(mine, gains, 0.0), 0, keepdims=True)
    normed = centered * spread * gain
    gated = (gate * jax.nn.sigmoid(gate) * normed).astype(BF)
    out[...] = jnp.broadcast_to(gated[None], out.shape)


def output_kernel(gated, w_keep, w_got, tokens, own, out):
    heads = gated.shape[0] // 2
    t = lax.axis_index("tp")
    branch = 0.0
    for group, w in ((t, w_keep), (1 - t, w_got)):
        lhs = jnp.concatenate([gated[2 * h + group] for h in range(heads)], 1)
        part = jnp.dot(lhs, w[...], preferred_element_type=F32)
        branch = branch + part.astype(BF).astype(F32)
    residual = (tokens[...].astype(F32) + branch).astype(BF)
    own[...] = residual
    out[...] = jnp.broadcast_to(residual[None], out.shape)


def mixer_kernel(residual, mlp_gain, w_up, w_down, out):
    blocks, rows, own = residual.shape
    width = blocks * own
    first = jnp.zeros((rows, own), F32)
    second = jnp.zeros((rows, own), F32)
    scaled, gain = [], []
    gains = mlp_gain[...].astype(F32)
    for i in range(blocks):
        wide = residual[i].astype(F32)
        first = first + wide
        second = second + wide * wide
        row = gains[i : i + 1]
        scaled.append((wide * row).astype(BF))
        gain.append(jnp.broadcast_to(row, wide.shape).astype(BF))
    lhs = jnp.concatenate([jnp.concatenate(scaled, 1), jnp.concatenate(gain, 1)], 0)
    up = jnp.dot(lhs, w_up[...], preferred_element_type=F32)
    average = jnp.sum(first, 1, keepdims=True) / width
    inverse = lax.rsqrt(jnp.sum(second, 1, keepdims=True) / width - average * average + EPS)
    hidden = inverse * (up[:rows] - average * up[rows : rows + 1])
    hidden = jnp.square(jnp.maximum(hidden, 0.0)).astype(BF)
    down = jnp.dot(hidden, w_down[...], preferred_element_type=F32)
    for i in range(blocks):
        out[i] = down[:, i * own : (i + 1) * own].astype(BF)


def final_kernel(pieces, own, out):
    total = jnp.sum(pieces[...].astype(F32), 0)
    out[...] = (own[...].astype(F32) + total).astype(BF)


VMEM = pl.BlockSpec(memory_space=pltpu.VMEM)
HBM = pl.BlockSpec(memory_space=pltpu.HBM)
ANY = pl.BlockSpec(memory_space=pl.ANY)


def in_hbm(*arrays):
    return [pltpu.with_memory_space_constraint(x, pltpu.HBM) for x in arrays]


def call(kernel, outs, in_specs, flops=0, bytes_accessed=0, scratch=(), limit=None):
    return pl.pallas_call(
        kernel,
        out_shape=outs,
        in_specs=in_specs,
        out_specs=jax.tree.map(lambda _: VMEM, outs),
        scratch_shapes=list(scratch),
        cost_estimate=pl.CostEstimate(
            flops=flops, bytes_accessed=bytes_accessed, transcendentals=0
        ),
        compiler_params=pltpu.CompilerParams(vmem_limit_bytes=limit),
    )


def make_kernels_on_device(kv, tp):
    def on_device(
        tokens,
        lengths,
        attn_gain,
        w_query,
        w_key,
        w_value,
        w_gate,
        decay_rate,
        key_cache,
        value_cache,
        head_gain,
        w_output,
        mlp_gain,
        w_up,
        w_down,
    ):
        S, own = tokens.shape
        H = decay_rate.shape[0]
        width = own * kv * tp
        qc, vc = H * HEAD_KEY, H * HEAD_VALUE
        swap = [(0, 1), (1, 0)]
        mib = 1 << 20
        sds = jax.ShapeDtypeStruct

        other = lax.ppermute(tokens, "tp", swap)
        gain = attn_gain.reshape(-1, LANES)
        w_query, tokens, gain, length_rows, rates = call(
            first_load_kernel,
            (
                sds(w_query.shape, BF),
                sds(tokens.shape, BF),
                sds(gain.shape, BF),
                sds((S, LANES), jnp.int32),
                sds((H, LANES), F32),
            ),
            [HBM] * 5,
            flops=10**9,
            scratch=[
                pltpu.SMEM((S,), jnp.int32),
                pltpu.SMEM((H,), F32),
                pltpu.SemaphoreType.DMA((5,)),
            ],
            limit=2 * mib,
        )(*in_hbm(w_query, tokens, gain, lengths, decay_rate))
        columns = qc + 2 * LANES
        message_types = (sds((S, columns), F32), sds((S, columns), BF))
        state, message = call(
            query_kernel, message_types, [VMEM] * 4, limit=2 * mib
        )(tokens, other, gain, w_query)

        def exchange(message, stride):
            return [
                lax.ppermute(message, "kv", [(i, i ^ (j * stride)) for i in range(kv)])
                for j in range(1, 4)
            ]

        got = exchange(message, 1)
        k_part, v_part, g_part, turn, weights, w_keep, w_send = call(
            other_kernel,
            (
                sds((S + 8, qc), F32),
                sds((S + 8, vc), F32),
                sds((S + 8, vc), F32),
                sds((2, S, LANES), F32),
                sds((S, H, LANES), F32),
                sds((w_output.shape[0], own), BF),
                sds((w_output.shape[0], own), BF),
            ),
            [ANY] + [VMEM] * 5 + [HBM] * 4,
            flops=10**9,
            scratch=[pltpu.VMEM(w.shape, BF) for w in (w_key, w_value, w_gate)]
            + [pltpu.SemaphoreType.DMA((5,))],
            limit=6 * mib,
        )(
            message,
            length_rows,
            rates,
            tokens,
            other,
            gain,
            *in_hbm(w_key, w_value, w_gate, w_output),
        )
        w_got = lax.ppermute(w_send, "tp", swap)

        stride = 4
        while stride < kv:
            state, message = call(
                middle_kernel, message_types, [VMEM] * 4, limit=2 * mib
            )(state, *got)
            got = exchange(message, stride)
            stride *= 4
        keys, values = call(
            cache_load_kernel,
            (sds(key_cache.shape, BF), sds(value_cache.shape, BF)),
            [ANY, VMEM] + [HBM] * 2,
            flops=10**9,
            scratch=[pltpu.SemaphoreType.DMA((S,))] * 2,
            limit=2 * mib,
        )(message, length_rows, *in_hbm(key_cache, value_cache))

        pieces = call(
            functools.partial(attend_kernel, width),
            sds((H, 3 * S + S // 2, LANES), BF),
            [ANY] + [VMEM] * 12,
            scratch=[
                pltpu.VMEM((S, qc), F32),
                pltpu.VMEM((S, vc), F32),
                pltpu.SMEM((S,), jnp.int32),
            ],
            limit=4 * mib,
        )(w_got, length_rows, state, *got, k_part, v_part, g_part, turn, weights, keys, values)

        pieces = lax.all_to_all(pieces, "kv", 0, 0, tiled=True)
        gated = call(
            gate_kernel, sds((kv * tp, S, LANES), BF), [VMEM] * 2, limit=2 * mib
        )(pieces, head_gain.reshape(H, HEAD_VALUE))
        gated = lax.all_to_all(gated, ("kv", "tp"), 0, 0, tiled=True)
        residual, spread = call(
            output_kernel,
            (sds((S, own), BF), sds((kv * tp, S, own), BF)),
            [VMEM] * 4,
            limit=4 * mib,
        )(gated, w_keep, w_got, tokens)
        spread = lax.all_to_all(spread, ("kv", "tp"), 0, 0, tiled=True)
        down = call(
            mixer_kernel, sds((kv * tp, S, own), BF), [VMEM] * 4, limit=16 * mib
        )(spread, mlp_gain.reshape(-1, LANES), w_up, w_down)
        down = lax.all_to_all(down, ("kv", "tp"), 0, 0, tiled=True)
        return call(final_kernel, sds((S, own), BF), [VMEM] * 2, limit=2 * mib)(down, residual)

    return on_device


def solution(mesh):
    in_specs = (
        P(None, ("kv", "tp")),
        P(),
        P("kv"),
        P("kv", "tp"),
        P("kv", "tp"),
        P("kv", "tp"),
        P("kv", "tp"),
        P("tp"),
        P(None, "kv", "tp"),
        P(None, "kv", "tp"),
        P("tp"),
        P("tp", "kv"),
        P(),
        P(None, ("kv", "tp")),
        P(("kv", "tp"), None),
    )
    kv, tp = mesh.shape["kv"], mesh.shape["tp"]

    def on_device(*arrays):
        fits = tp == 2 and arrays[7].shape[0] == kv
        fits = fits and arrays[0].shape[1] == LANES == arrays[8].shape[1]
        make = make_kernels_on_device if fits else make_on_device
        return make(kv, tp)(*arrays)

    return jax.shard_map(
        on_device,
        mesh=mesh,
        in_specs=in_specs,
        out_specs=P(None, ("kv", "tp")),
        check_vma=False,
    )
```

```python
import functools
import math

import jax
import jax.numpy as jnp
from jax import lax
from jax.experimental import pallas as pl
from jax.experimental.pallas import tpu as pltpu
from jax.sharding import PartitionSpec as P


HEAD_KEY = 64
HEAD_VALUE = 128
EPS = 1e-05
THETA = 10000.0
LANES = 128

BF = jnp.bfloat16
F32 = jnp.float32


def split_two(x):
    high = x.astype(BF)
    return high, (x - high.astype(F32)).astype(BF)


def rotate(flat, cosine, sine):
    rows = flat.shape[0]
    grouped = flat.reshape(rows, -1, HEAD_KEY)
    half = HEAD_KEY // 2
    a, b = grouped[..., :half], grouped[..., half:]
    c, s = cosine[:, None, :], sine[:, None, :]
    return jnp.concatenate([a * c - b * s, b * c + a * s], -1).reshape(rows, -1)


def broadcast_gather(x, axes, size):
    spread = jnp.broadcast_to(x[None], (size,) + x.shape)
    return lax.all_to_all(spread, axes, 0, 0, tiled=True)


def make_on_device(kv, tp):
    def on_device(
        tokens,
        lengths,
        attn_gain,
        w_query,
        w_key,
        w_value,
        w_gate,
        decay_rate,
        key_cache,
        value_cache,
        head_gain,
        w_output,
        mlp_gain,
        w_up,
        w_down,
    ):
        S = tokens.shape[0]
        H = decay_rate.shape[0]
        span = key_cache.shape[1]
        width = tokens.shape[1] * kv * tp
        own = tokens.shape[1]
        kvi = lax.axis_index("kv")
        tpi = lax.axis_index("tp")
        groups = kv // H
        rows = S // groups

        if tp == 2:
            other = lax.ppermute(tokens, "tp", [(0, 1), (1, 0)])
            low = jnp.where(tpi == 0, tokens, other)
            high = jnp.where(tpi == 0, other, tokens)
            block = jnp.concatenate([low, high], 1)
        else:
            block = lax.all_gather(tokens, "tp", axis=1, tiled=True)
        wide = block.astype(F32)
        scaled = (wide * attn_gain.astype(F32)).astype(BF)
        lhs = jnp.concatenate([scaled, attn_gain[None, :]], 0)
        part_q = jnp.dot(lhs, w_query, preferred_element_type=F32)
        moments = jnp.stack([jnp.sum(wide, -1), jnp.sum(wide * wide, -1)], -1)

        small = jnp.concatenate([part_q[S], moments.reshape(-1)])
        q_sum = part_q[:S]
        stride = 1
        while stride < kv:
            count = 4 if kv % (stride * 4) == 0 else 2
            high, low = split_two(small)
            tail = jnp.concatenate([high, low])
            pad = -tail.shape[0] % S
            tail = jnp.pad(tail, (0, pad)).reshape(S, -1)
            message = jnp.concatenate([q_sum.astype(BF), tail], 1)
            for j in range(1, count):
                got = lax.ppermute(message, "kv", [(i, i ^ (j * stride)) for i in range(kv)])
                got = got.astype(F32)
                q_sum = q_sum + got[:, : q_sum.shape[1]]
                flat = got[:, q_sum.shape[1] :].reshape(-1)
                n = small.shape[0]
                small = small + flat[:n] + flat[n : 2 * n]
            stride *= count
        csum_q = small[: q_sum.shape[1]]
        moments = small[q_sum.shape[1] :].reshape(S, 2)
        average = moments[:, 0] / width
        inverse = lax.rsqrt(moments[:, 1] / width - average * average + EPS)

        half = HEAD_KEY // 2
        turn = jnp.power(THETA, -jnp.arange(half, dtype=F32) / half)
        angles = lengths.astype(F32)[:, None] * turn[None, :]
        q_plain = inverse[:, None] * (q_sum - average[:, None] * csum_q[None, :])
        queries = rotate(q_plain, jnp.cos(angles), jnp.sin(angles)).astype(BF)
        queries = queries.reshape(S, H, HEAD_KEY)

        def partial(w):
            p = jnp.dot(lhs, w, preferred_element_type=F32)
            return inverse[:, None] * (p[:S] - average[:, None] * p[S:])

        part_k = partial(w_key).reshape(S, H, HEAD_KEY)
        part_v = partial(w_value).reshape(S, H, HEAD_VALUE)
        part_g = partial(w_gate).reshape(S, H, HEAD_VALUE)
        part_score = jnp.sum(q_plain.reshape(S, H, HEAD_KEY) * part_k, -1) * HEAD_KEY ** (-0.5)

        keys = key_cache.reshape(S, span, H, HEAD_KEY)
        values = value_cache.reshape(S, span, H, HEAD_VALUE)
        scores = jnp.einsum("bhd,bjhd->bhj", queries, keys, preferred_element_type=F32)
        places = kvi * span + jnp.arange(span, dtype=jnp.int32)
        distance = jnp.maximum(lengths[:, None] - places[None, :], 0).astype(F32)
        live = (places[None, :] < lengths[:, None])[:, None, :]
        decays = jnp.where(
            live, jnp.exp(-decay_rate[None, :, None] * distance[:, None, :]), 0.0
        )
        coefficients = (scores * HEAD_KEY ** (-0.5) * decays).astype(BF)
        part_c = jnp.einsum("bhj,bjhe->bhe", coefficients, values, preferred_element_type=F32)

        high, low = split_two(part_score)
        pieces = jnp.concatenate(
            [
                part_c.astype(BF),
                part_v.astype(BF),
                part_g.astype(BF),
                high[..., None],
                low[..., None],
                jnp.zeros((S, H, 126), BF),
            ],
            -1,
        )
        pieces = pieces.transpose(1, 0, 2).reshape(kv, rows, 4 * HEAD_VALUE)
        mine = jnp.sum(
            lax.all_to_all(pieces, "kv", 0, 0, tiled=True).astype(F32), 0
        )
        cached, value, gate = (
            mine[:, i * HEAD_VALUE : (i + 1) * HEAD_VALUE] for i in range(3)
        )
        score = mine[:, 3 * HEAD_VALUE] + mine[:, 3 * HEAD_VALUE + 1]
        retained = cached + score[:, None] * value
        centered = retained - jnp.mean(retained, -1, keepdims=True)
        gain = lax.dynamic_slice(head_gain, ((kvi // groups) * HEAD_VALUE,), (HEAD_VALUE,))
        normed = (
            centered
            * lax.rsqrt(jnp.mean(centered * centered, -1, keepdims=True) + EPS)
            * gain.astype(F32)
        )
        gated = (jax.nn.silu(gate) * normed).astype(BF)
        gathered = broadcast_gather(gated, "kv", kv).reshape(H, S, HEAD_VALUE)
        gathered = gathered.transpose(1, 0, 2).reshape(S, H * HEAD_VALUE)
        part_b = jnp.dot(gathered, w_output, preferred_element_type=F32).astype(BF)
        part_b = part_b.reshape(S, tp, own).transpose(1, 0, 2)
        if tp == 2:
            keep = jnp.where(tpi == 0, part_b[0], part_b[1])
            send = jnp.where(tpi == 0, part_b[1], part_b[0])
            got = lax.ppermute(send, "tp", [(0, 1), (1, 0)])
            branch = keep.astype(F32) + got.astype(F32)
        else:
            branch = jnp.sum(
                lax.all_to_all(part_b, "tp", 0, 0, tiled=True).astype(F32), 0
            )
        own_residual = (tokens.astype(F32) + branch).astype(BF)

        residual = broadcast_gather(own_residual, ("kv", "tp"), kv * tp)
        residual = residual.transpose(1, 0, 2).reshape(S, width)
        wide = residual.astype(F32)
        scaled = (wide * mlp_gain.astype(F32)).astype(BF)
        lhs = jnp.concatenate([scaled, mlp_gain[None, :]], 0)
        up = jnp.dot(lhs, w_up, preferred_element_type=F32)
        average = jnp.sum(wide, -1) / width
        inverse = lax.rsqrt(jnp.sum(wide * wide, -1) / width - average * average + EPS)
        hidden = inverse[:, None] * (up[:S] - average[:, None] * up[S:])
        hidden = jnp.square(jax.nn.relu(hidden)).astype(BF)
        down = jnp.dot(hidden, w_down, preferred_element_type=F32).astype(BF)
        down = down.reshape(S, kv * tp, own).transpose(1, 0, 2)
        mixer = jnp.sum(
            lax.all_to_all(down, ("kv", "tp"), 0, 0, tiled=True).astype(F32), 0
        )
        return (own_residual.astype(F32) + mixer).astype(BF)

    return on_device


def lane_ids(rows):
    return lax.broadcasted_iota(jnp.int32, (rows, LANES), 1)


def row_ids(rows, columns=LANES):
    return lax.broadcasted_iota(jnp.int32, (rows, columns), 0)


def column_of(scalars, rows, dtype):
    ids = row_ids(rows)
    out = jnp.zeros((rows, LANES), dtype)
    for i in range(rows):
        out = jnp.where(ids == i, scalars[i].astype(dtype), out)
    return out


def gain_row(gain, rows):
    wide = gain[...].astype(F32)
    return jnp.concatenate(
        [jnp.broadcast_to(wide[i : i + 1], (rows, LANES)) for i in range(wide.shape[0])], 1
    )


def projection_rows(first, second, gain):
    t = lax.axis_index("tp")
    a, b = first[...].astype(F32), second[...].astype(F32)
    wide = jnp.concatenate([jnp.where(t == 0, a, b), jnp.where(t == 0, b, a)], 1)
    row = gain_row(gain, wide.shape[0])
    return jnp.concatenate([(wide * row).astype(BF), row.astype(BF)], 0), wide


def pack(q, csum, moments, message):
    columns = q.shape[1]
    half = csum.shape[0]
    message[:, :columns] = q.astype(BF)
    high = csum.astype(BF)
    low = (csum - high.astype(F32)).astype(BF)
    message[:, columns : columns + LANES] = jnp.concatenate([high, low], 0)
    high = moments.astype(BF).astype(F32)
    low = moments - high
    lanes = lane_ids(q.shape[0])
    both = jnp.where(lanes < 2, high, jnp.where(lanes < 4, pltpu.roll(low, 2, 1), 0.0))
    message[:, columns + LANES :] = both.astype(BF)
    assert 2 * half == q.shape[0]


def unpack_sum(state, messages):
    rows, total = state.shape
    columns = total - 2 * LANES
    half = rows // 2
    q = state[:, :columns]
    csum = state[:half, columns : columns + LANES]
    moments = state[:, columns + LANES :]
    for m in messages:
        q = q + m[:, :columns].astype(F32)
        c = m[:, columns : columns + LANES].astype(F32)
        csum = csum + c[:half] + c[half:]
        v = m[:, columns + LANES :].astype(F32)
        moments = moments + v + pltpu.roll(v, LANES - 2, 1)
    return q, csum, jnp.where(lane_ids(rows) < 2, moments, 0.0)


def store_state(q, csum, moments, state):
    columns = q.shape[1]
    state[:, :columns] = q
    state[:, columns : columns + LANES] = jnp.concatenate([csum, jnp.zeros_like(csum)], 0)
    state[:, columns + LANES :] = moments


def first_load_kernel(
    w_query,
    tokens,
    gain,
    lengths,
    decay,
    w_out,
    tokens_out,
    gain_out,
    length_out,
    rate_out,
    length_scalars,
    decay_scalars,
    sems,
):
    pairs = (
        (lengths, length_scalars),
        (decay, decay_scalars),
        (tokens, tokens_out),
        (gain, gain_out),
        (w_query, w_out),
    )
    copies = [pltpu.make_async_copy(a, b, sems.at[i]) for i, (a, b) in enumerate(pairs)]
    for copy in copies:
        copy.start()
    copies[0].wait()
    length_out[...] = column_of(length_scalars, length_out.shape[0], jnp.int32)
    copies[1].wait()
    rate_out[...] = column_of(decay_scalars, rate_out.shape[0], F32)
    for copy in copies[2:]:
        copy.wait()


def live_scalars(lengths, base):
    values = lengths[...]
    live = [values[s, 0] > base for s in range(values.shape[0])]
    count = jnp.int32(0)
    for flag in live:
        count = count + flag.astype(jnp.int32)
    return live, count


def few_rows(rows):
    return rows // 2


def late_rows(rows):
    return rows * 3 // 8


def cache_load_kernel(
    after, lengths, keys, values, keys_out, values_out, key_sems, value_sems
):
    rows = keys.shape[0]
    live, count = live_scalars(lengths, lax.axis_index("kv") * keys.shape[1])
    few = count <= few_rows(rows)

    def each_copy(act):
        for s in range(rows):
            key = pltpu.make_async_copy(keys.at[s], keys_out.at[s], key_sems.at[s])
            value = pltpu.make_async_copy(values.at[s], values_out.at[s], value_sems.at[s])
            late = s >= rows - late_rows(rows)

            @pl.when(live[s])
            def _():
                act(key)
                if not late:
                    act(value)

            if late:

                @pl.when(jnp.logical_and(live[s], few))
                def _():
                    act(value)

    each_copy(lambda copy: copy.start())
    each_copy(lambda copy: copy.wait())


def query_kernel(first, second, gain, w_query, state, message):
    lhs, wide = projection_rows(first, second, gain)
    rows = wide.shape[0]
    product = jnp.dot(lhs, w_query[...], preferred_element_type=F32)
    half = rows // 2
    ids = row_ids(half)
    csum = jnp.zeros((half, LANES), F32)
    for i in range(product.shape[1] // LANES):
        csum = jnp.where(
            ids == i, product[rows : rows + half, i * LANES : (i + 1) * LANES], csum
        )
    lanes = lane_ids(rows)
    first_sum = jnp.sum(wide, 1, keepdims=True)
    second_sum = jnp.sum(wide * wide, 1, keepdims=True)
    moments = jnp.where(lanes == 0, first_sum, jnp.where(lanes == 1, second_sum, 0.0))
    store_state(product[:rows], csum, moments, state)
    pack(product[:rows], csum, moments, message)


def middle_kernel(old, m1, m2, m3, state, message):
    q, csum, moments = unpack_sum(old, (m1, m2, m3))
    store_state(q, csum, moments, state)
    pack(q, csum, moments, message)


def other_kernel(
    after,
    lengths,
    rates,
    first,
    second,
    gain,
    w_key,
    w_value,
    w_gate,
    w_output,
    k_out,
    v_out,
    g_out,
    turn,
    weights,
    w_keep,
    w_send,
    key_buffer,
    value_buffer,
    gate_buffer,
    sems,
):
    own = w_keep.shape[1]
    t = lax.axis_index("tp")
    kept = pl.ds(pl.multiple_of(t * own, own), own)
    sent = pl.ds(pl.multiple_of((1 - t) * own, own), own)
    buffers = (key_buffer, value_buffer, gate_buffer)
    pairs = (
        (w_key, key_buffer),
        (w_value, value_buffer),
        (w_gate, gate_buffer),
        (w_output.at[:, sent], w_send),
        (w_output.at[:, kept], w_keep),
    )
    copies = [pltpu.make_async_copy(a, b, sems.at[i]) for i, (a, b) in enumerate(pairs)]
    for copy in copies:
        copy.start()
    lhs, wide = projection_rows(first, second, gain)
    rows = wide.shape[0]
    half = HEAD_KEY // 2
    entry = (lane_ids(rows) % half).astype(F32)
    inverse = jnp.exp(entry * (-math.log(THETA) / half))
    angle = lengths[...].astype(F32) * inverse
    turn[0] = jnp.cos(angle)
    turn[1] = jnp.sin(angle)
    heads = rates.shape[0]
    places = lax.axis_index("kv") * LANES + lane_ids(heads)
    rate = rates[...]
    for s in range(rows):
        distance = jnp.broadcast_to(lengths[s : s + 1, :], (heads, LANES)) - places
        weight = jnp.exp(-rate * jnp.maximum(distance, 0).astype(F32)) * HEAD_KEY ** (-0.5)
        weights[s] = jnp.where(distance > 0, weight, 0.0)
    for copy, buffer, out in zip(copies, buffers, (k_out, v_out, g_out)):
        copy.wait()
        product = jnp.dot(lhs, buffer[...], preferred_element_type=F32)
        out[...] = product[: rows + 8]
    for copy in copies[len(buffers) :]:
        copy.wait()


def attend_kernel(
    width,
    after,
    lengths,
    old,
    m1,
    m2,
    m3,
    k_part,
    v_part,
    g_part,
    turn,
    weights,
    keys,
    values,
    values_far,
    out,
    query_rows,
    cached,
    order,
    late_values,
    late_sems,
):
    rows, span, key_columns = keys.shape
    heads = key_columns // HEAD_KEY
    live, live_count = live_scalars(lengths, lax.axis_index("kv") * span)
    late = late_values.shape[0]
    late_copies = [
        pltpu.make_async_copy(values_far.at[rows - late + i], late_values.at[i], late_sems.at[i])
        for i in range(late)
    ]

    @pl.when(live_count > few_rows(rows))
    def _():
        for copy in late_copies:
            copy.start()

    q, csum, moments = unpack_sum(old, (m1, m2, m3))
    average = moments[:, 0:1] / width
    inverse = lax.rsqrt(moments[:, 1:2] / width - average * average + EPS)
    lanes = lane_ids(rows)
    in_first = lanes % HEAD_KEY < HEAD_KEY // 2
    low_head = lanes < HEAD_KEY
    top = rows // 2
    cosine, sine = turn[0], turn[1]
    for i in range(key_columns // LANES):
        cut = slice(i * LANES, (i + 1) * LANES)
        plain = inverse * (q[:, cut] - average * csum[i : i + 1])
        partner = jnp.where(
            in_first,
            -pltpu.roll(plain, LANES - HEAD_KEY // 2, 1),
            pltpu.roll(plain, HEAD_KEY // 2, 1),
        )
        turned = plain * cosine + partner * sine
        query_rows[:, cut] = turned.astype(BF).astype(F32)
        part = inverse * (k_part[:rows, cut] - average * k_part[rows : rows + 1, cut])
        both = plain * part * HEAD_KEY ** (-0.5)
        for j in range(2):
            picked = jnp.where(low_head == (j == 0), both, 0.0)
            score = jnp.sum(picked, 1, keepdims=True)
            high = score.astype(BF).astype(F32)
            low = score - high
            folded = jnp.where(
                lanes[:top] < HEAD_KEY,
                jnp.where(in_first[:top], high[:top], low[:top]),
                jnp.where(in_first[:top], high[top:], low[top:]),
            )
            out[2 * i + j, 3 * rows :, :] = folded.astype(BF)
    for h in range(heads):
        cut = slice(h * LANES, (h + 1) * LANES)
        for place, part in ((1, v_part), (2, g_part)):
            normed = inverse * (part[:rows, cut] - average * part[rows : rows + 1, cut])
            out[h, place * rows : (place + 1) * rows, :] = normed.astype(BF)

    head_of_key = lax.broadcasted_iota(jnp.int32, (heads, key_columns), 1) // HEAD_KEY
    own_key = head_of_key == row_ids(heads, key_columns)
    value_columns = heads * HEAD_VALUE
    head_of_value = lax.broadcasted_iota(jnp.int32, (heads, value_columns), 1) // HEAD_VALUE
    own_value = head_of_value == row_ids(heads, value_columns)
    count = jnp.int32(0)
    for s in range(rows):
        order[count] = s
        count = count + live[s].astype(jnp.int32)

    def one(s, is_live, value=None):
        row = pl.ds(s, 1)
        spread = jnp.broadcast_to(query_rows[row, :], (heads, key_columns))
        query = jnp.where(own_key, spread, 0.0).astype(BF)
        scores = lax.dot_general(
            query, keys[s], (((1,), (1,)), ((), ())), preferred_element_type=F32
        )
        weight = weights[s]
        coefficients = jnp.where(weight > 0.0, scores * weight, 0.0).astype(BF)
        value = values[s] if value is None else value
        product = jnp.dot(coefficients, value, preferred_element_type=F32)
        kept = jnp.logical_and(own_value, is_live)
        cached[row, :] = jnp.sum(jnp.where(kept, product, 0.0), 0, keepdims=True)

    steps = [few_rows(rows) // 2, few_rows(rows), rows]
    for least, most in zip([-1] + steps[:-1], steps):

        @pl.when(jnp.logical_and(count > least, count <= most))
        def _():
            if most == rows:
                for s in range(rows - late):
                    one(s, live[s])
                for copy in late_copies:
                    copy.wait()
                for i in range(late):
                    one(rows - late + i, live[rows - late + i], late_values[i])
            else:
                cached[...] = jnp.zeros_like(cached)
                for i in range(most):
                    one(order[jnp.minimum(i, jnp.maximum(count - 1, 0))], count > 0)

    for h in range(heads):
        out[h, :rows, :] = cached[:, h * LANES : (h + 1) * LANES].astype(BF)


def gate_kernel(pieces, head_gain, out):
    rows = out.shape[1]
    total = jnp.sum(pieces[...].astype(F32), 0)
    cached, value, gate = (total[i * rows : (i + 1) * rows] for i in range(3))
    folded = total[3 * rows :]
    half = HEAD_KEY // 2
    score = jnp.concatenate(
        [folded[:, i : i + 1] + folded[:, i + half : i + half + 1] for i in (0, HEAD_KEY)], 0
    )
    retained = cached + score * value
    centered = retained - jnp.mean(retained, -1, keepdims=True)
    spread = lax.rsqrt(jnp.mean(centered * centered, -1, keepdims=True) + EPS)
    gains = head_gain[...].astype(F32)
    mine = row_ids(gains.shape[0]) == lax.axis_index("kv")
    gain = jnp.sum(jnp.where(mine, gains, 0.0), 0, keepdims=True)
    normed = centered * spread * gain
    gated = (gate * jax.nn.sigmoid(gate) * normed).astype(BF)
    out[...] = jnp.broadcast_to(gated[None], out.shape)


def output_kernel(gated, w_keep, w_got, tokens, own, out):
    heads = gated.shape[0] // 2
    t = lax.axis_index("tp")
    branch = 0.0
    for group, w in ((t, w_keep), (1 - t, w_got)):
        lhs = jnp.concatenate([gated[2 * h + group] for h in range(heads)], 1)
        part = jnp.dot(lhs, w[...], preferred_element_type=F32)
        branch = branch + part.astype(BF).astype(F32)
    residual = (tokens[...].astype(F32) + branch).astype(BF)
    own[...] = residual
    out[...] = jnp.broadcast_to(residual[None], out.shape)


def mixer_kernel(residual, mlp_gain, w_up, w_down, out):
    blocks, rows, own = residual.shape
    width = blocks * own
    first = jnp.zeros((rows, own), F32)
    second = jnp.zeros((rows, own), F32)
    scaled, gain = [], []
    gains = mlp_gain[...].astype(F32)
    for i in range(blocks):
        wide = residual[i].astype(F32)
        first = first + wide
        second = second + wide * wide
        row = gains[i : i + 1]
        scaled.append((wide * row).astype(BF))
        gain.append(jnp.broadcast_to(row, wide.shape).astype(BF))
    lhs = jnp.concatenate([jnp.concatenate(scaled, 1), jnp.concatenate(gain, 1)], 0)
    up = jnp.dot(lhs, w_up[...], preferred_element_type=F32)
    average = jnp.sum(first, 1, keepdims=True) / width
    inverse = lax.rsqrt(jnp.sum(second, 1, keepdims=True) / width - average * average + EPS)
    hidden = inverse * (up[:rows] - average * up[rows : rows + 1])
    hidden = jnp.square(jnp.maximum(hidden, 0.0)).astype(BF)
    down = jnp.dot(hidden, w_down[...], preferred_element_type=F32)
    for i in range(blocks):
        out[i] = down[:, i * own : (i + 1) * own].astype(BF)


def final_kernel(pieces, own, out):
    total = jnp.sum(pieces[...].astype(F32), 0)
    out[...] = (own[...].astype(F32) + total).astype(BF)


VMEM = pl.BlockSpec(memory_space=pltpu.VMEM)
HBM = pl.BlockSpec(memory_space=pltpu.HBM)
ANY = pl.BlockSpec(memory_space=pl.ANY)


def in_hbm(*arrays):
    return [pltpu.with_memory_space_constraint(x, pltpu.HBM) for x in arrays]


def call(kernel, outs, in_specs, flops=0, bytes_accessed=0, scratch=(), limit=None):
    return pl.pallas_call(
        kernel,
        out_shape=outs,
        in_specs=in_specs,
        out_specs=jax.tree.map(lambda _: VMEM, outs),
        scratch_shapes=list(scratch),
        cost_estimate=pl.CostEstimate(
            flops=flops, bytes_accessed=bytes_accessed, transcendentals=0
        ),
        compiler_params=pltpu.CompilerParams(vmem_limit_bytes=limit),
    )


def make_kernels_on_device(kv, tp):
    def on_device(
        tokens,
        lengths,
        attn_gain,
        w_query,
        w_key,
        w_value,
        w_gate,
        decay_rate,
        key_cache,
        value_cache,
        head_gain,
        w_output,
        mlp_gain,
        w_up,
        w_down,
    ):
        S, own = tokens.shape
        H = decay_rate.shape[0]
        width = own * kv * tp
        qc, vc = H * HEAD_KEY, H * HEAD_VALUE
        swap = [(0, 1), (1, 0)]
        mib = 1 << 20
        sds = jax.ShapeDtypeStruct

        other = lax.ppermute(tokens, "tp", swap)
        gain = attn_gain.reshape(-1, LANES)
        w_query, tokens, gain, length_rows, rates = call(
            first_load_kernel,
            (
                sds(w_query.shape, BF),
                sds(tokens.shape, BF),
                sds(gain.shape, BF),
                sds((S, LANES), jnp.int32),
                sds((H, LANES), F32),
            ),
            [HBM] * 5,
            flops=10**9,
            scratch=[
                pltpu.SMEM((S,), jnp.int32),
                pltpu.SMEM((H,), F32),
                pltpu.SemaphoreType.DMA((5,)),
            ],
            limit=2 * mib,
        )(*in_hbm(w_query, tokens, gain, lengths, decay_rate))
        columns = qc + 2 * LANES
        message_types = (sds((S, columns), F32), sds((S, columns), BF))
        state, message = call(
            query_kernel, message_types, [VMEM] * 4, limit=2 * mib
        )(tokens, other, gain, w_query)

        def exchange(message, stride):
            return [
                lax.ppermute(message, "kv", [(i, i ^ (j * stride)) for i in range(kv)])
                for j in range(1, 4)
            ]

        got = exchange(message, 1)
        k_part, v_part, g_part, turn, weights, w_keep, w_send = call(
            other_kernel,
            (
                sds((S + 8, qc), F32),
                sds((S + 8, vc), F32),
                sds((S + 8, vc), F32),
                sds((2, S, LANES), F32),
                sds((S, H, LANES), F32),
                sds((w_output.shape[0], own), BF),
                sds((w_output.shape[0], own), BF),
            ),
            [ANY] + [VMEM] * 5 + [HBM] * 4,
            flops=10**9,
            scratch=[pltpu.VMEM(w.shape, BF) for w in (w_key, w_value, w_gate)]
            + [pltpu.SemaphoreType.DMA((5,))],
            limit=6 * mib,
        )(
            message,
            length_rows,
            rates,
            tokens,
            other,
            gain,
            *in_hbm(w_key, w_value, w_gate, w_output),
        )
        w_got = lax.ppermute(w_send, "tp", swap)

        stride = 4
        while stride < kv:
            state, message = call(
                middle_kernel, message_types, [VMEM] * 4, limit=2 * mib
            )(state, *got)
            got = exchange(message, stride)
            stride *= 4
        keys, values = call(
            cache_load_kernel,
            (sds(key_cache.shape, BF), sds(value_cache.shape, BF)),
            [ANY, VMEM] + [HBM] * 2,
            flops=10**9,
            scratch=[pltpu.SemaphoreType.DMA((S,))] * 2,
            limit=2 * mib,
        )(message, length_rows, *in_hbm(key_cache, value_cache))

        pieces = call(
            functools.partial(attend_kernel, width),
            sds((H, 3 * S + S // 2, LANES), BF),
            [ANY] + [VMEM] * 12 + [HBM],
            scratch=[
                pltpu.VMEM((S, qc), F32),
                pltpu.VMEM((S, vc), F32),
                pltpu.SMEM((S,), jnp.int32),
                pltpu.VMEM((late_rows(S),) + value_cache.shape[1:], BF),
                pltpu.SemaphoreType.DMA((late_rows(S),)),
            ],
            limit=8 * mib,
        )(
            w_got,
            length_rows,
            state,
            *got,
            k_part,
            v_part,
            g_part,
            turn,
            weights,
            keys,
            values,
            *in_hbm(value_cache),
        )

        pieces = lax.all_to_all(pieces, "kv", 0, 0, tiled=True)
        gated = call(
            gate_kernel, sds((kv * tp, S, LANES), BF), [VMEM] * 2, limit=2 * mib
        )(pieces, head_gain.reshape(H, HEAD_VALUE))
        gated = lax.all_to_all(gated, ("kv", "tp"), 0, 0, tiled=True)
        residual, spread = call(
            output_kernel,
            (sds((S, own), BF), sds((kv * tp, S, own), BF)),
            [VMEM] * 4,
            limit=4 * mib,
        )(gated, w_keep, w_got, tokens)
        spread = lax.all_to_all(spread, ("kv", "tp"), 0, 0, tiled=True)
        down = call(
            mixer_kernel, sds((kv * tp, S, own), BF), [VMEM] * 4, limit=16 * mib
        )(spread, mlp_gain.reshape(-1, LANES), w_up, w_down)
        down = lax.all_to_all(down, ("kv", "tp"), 0, 0, tiled=True)
        return call(final_kernel, sds((S, own), BF), [VMEM] * 2, limit=2 * mib)(down, residual)

    return on_device


def solution(mesh):
    in_specs = (
        P(None, ("kv", "tp")),
        P(),
        P("kv"),
        P("kv", "tp"),
        P("kv", "tp"),
        P("kv", "tp"),
        P("kv", "tp"),
        P("tp"),
        P(None, "kv", "tp"),
        P(None, "kv", "tp"),
        P("tp"),
        P("tp", "kv"),
        P(),
        P(None, ("kv", "tp")),
        P(("kv", "tp"), None),
    )
    kv, tp = mesh.shape["kv"], mesh.shape["tp"]

    def on_device(*arrays):
        fits = tp == 2 and arrays[7].shape[0] == kv
        fits = fits and arrays[0].shape[1] == LANES == arrays[8].shape[1]
        make = make_kernels_on_device if fits else make_on_device
        return make(kv, tp)(*arrays)

    return jax.shard_map(
        on_device,
        mesh=mesh,
        in_specs=in_specs,
        out_specs=P(None, ("kv", "tp")),
        check_vma=False,
    )
```

```python
import functools
import math

import jax
import jax.numpy as jnp
from jax import lax
from jax.experimental import pallas as pl
from jax.experimental.pallas import tpu as pltpu
from jax.sharding import PartitionSpec as P


HEAD_KEY = 64
HEAD_VALUE = 128
EPS = 1e-05
THETA = 10000.0
LANES = 128

BF = jnp.bfloat16
F32 = jnp.float32


def split_two(x):
    high = x.astype(BF)
    return high, (x - high.astype(F32)).astype(BF)


def rotate(flat, cosine, sine):
    rows = flat.shape[0]
    grouped = flat.reshape(rows, -1, HEAD_KEY)
    half = HEAD_KEY // 2
    a, b = grouped[..., :half], grouped[..., half:]
    c, s = cosine[:, None, :], sine[:, None, :]
    return jnp.concatenate([a * c - b * s, b * c + a * s], -1).reshape(rows, -1)


def broadcast_gather(x, axes, size):
    spread = jnp.broadcast_to(x[None], (size,) + x.shape)
    return lax.all_to_all(spread, axes, 0, 0, tiled=True)


def make_on_device(kv, tp):
    def on_device(
        tokens,
        lengths,
        attn_gain,
        w_query,
        w_key,
        w_value,
        w_gate,
        decay_rate,
        key_cache,
        value_cache,
        head_gain,
        w_output,
        mlp_gain,
        w_up,
        w_down,
    ):
        S = tokens.shape[0]
        H = decay_rate.shape[0]
        span = key_cache.shape[1]
        width = tokens.shape[1] * kv * tp
        own = tokens.shape[1]
        kvi = lax.axis_index("kv")
        tpi = lax.axis_index("tp")
        groups = kv // H
        rows = S // groups

        if tp == 2:
            other = lax.ppermute(tokens, "tp", [(0, 1), (1, 0)])
            low = jnp.where(tpi == 0, tokens, other)
            high = jnp.where(tpi == 0, other, tokens)
            block = jnp.concatenate([low, high], 1)
        else:
            block = lax.all_gather(tokens, "tp", axis=1, tiled=True)
        wide = block.astype(F32)
        scaled = (wide * attn_gain.astype(F32)).astype(BF)
        lhs = jnp.concatenate([scaled, attn_gain[None, :]], 0)
        part_q = jnp.dot(lhs, w_query, preferred_element_type=F32)
        moments = jnp.stack([jnp.sum(wide, -1), jnp.sum(wide * wide, -1)], -1)

        small = jnp.concatenate([part_q[S], moments.reshape(-1)])
        q_sum = part_q[:S]
        stride = 1
        while stride < kv:
            count = 4 if kv % (stride * 4) == 0 else 2
            high, low = split_two(small)
            tail = jnp.concatenate([high, low])
            pad = -tail.shape[0] % S
            tail = jnp.pad(tail, (0, pad)).reshape(S, -1)
            message = jnp.concatenate([q_sum.astype(BF), tail], 1)
            for j in range(1, count):
                got = lax.ppermute(message, "kv", [(i, i ^ (j * stride)) for i in range(kv)])
                got = got.astype(F32)
                q_sum = q_sum + got[:, : q_sum.shape[1]]
                flat = got[:, q_sum.shape[1] :].reshape(-1)
                n = small.shape[0]
                small = small + flat[:n] + flat[n : 2 * n]
            stride *= count
        csum_q = small[: q_sum.shape[1]]
        moments = small[q_sum.shape[1] :].reshape(S, 2)
        average = moments[:, 0] / width
        inverse = lax.rsqrt(moments[:, 1] / width - average * average + EPS)

        half = HEAD_KEY // 2
        turn = jnp.power(THETA, -jnp.arange(half, dtype=F32) / half)
        angles = lengths.astype(F32)[:, None] * turn[None, :]
        q_plain = inverse[:, None] * (q_sum - average[:, None] * csum_q[None, :])
        queries = rotate(q_plain, jnp.cos(angles), jnp.sin(angles)).astype(BF)
        queries = queries.reshape(S, H, HEAD_KEY)

        def partial(w):
            p = jnp.dot(lhs, w, preferred_element_type=F32)
            return inverse[:, None] * (p[:S] - average[:, None] * p[S:])

        part_k = partial(w_key).reshape(S, H, HEAD_KEY)
        part_v = partial(w_value).reshape(S, H, HEAD_VALUE)
        part_g = partial(w_gate).reshape(S, H, HEAD_VALUE)
        part_score = jnp.sum(q_plain.reshape(S, H, HEAD_KEY) * part_k, -1) * HEAD_KEY ** (-0.5)

        keys = key_cache.reshape(S, span, H, HEAD_KEY)
        values = value_cache.reshape(S, span, H, HEAD_VALUE)
        scores = jnp.einsum("bhd,bjhd->bhj", queries, keys, preferred_element_type=F32)
        places = kvi * span + jnp.arange(span, dtype=jnp.int32)
        distance = jnp.maximum(lengths[:, None] - places[None, :], 0).astype(F32)
        live = (places[None, :] < lengths[:, None])[:, None, :]
        decays = jnp.where(
            live, jnp.exp(-decay_rate[None, :, None] * distance[:, None, :]), 0.0
        )
        coefficients = (scores * HEAD_KEY ** (-0.5) * decays).astype(BF)
        part_c = jnp.einsum("bhj,bjhe->bhe", coefficients, values, preferred_element_type=F32)

        high, low = split_two(part_score)
        pieces = jnp.concatenate(
            [
                part_c.astype(BF),
                part_v.astype(BF),
                part_g.astype(BF),
                high[..., None],
                low[..., None],
                jnp.zeros((S, H, 126), BF),
            ],
            -1,
        )
        pieces = pieces.transpose(1, 0, 2).reshape(kv, rows, 4 * HEAD_VALUE)
        mine = jnp.sum(
            lax.all_to_all(pieces, "kv", 0, 0, tiled=True).astype(F32), 0
        )
        cached, value, gate = (
            mine[:, i * HEAD_VALUE : (i + 1) * HEAD_VALUE] for i in range(3)
        )
        score = mine[:, 3 * HEAD_VALUE] + mine[:, 3 * HEAD_VALUE + 1]
        retained = cached + score[:, None] * value
        centered = retained - jnp.mean(retained, -1, keepdims=True)
        gain = lax.dynamic_slice(head_gain, ((kvi // groups) * HEAD_VALUE,), (HEAD_VALUE,))
        normed = (
            centered
            * lax.rsqrt(jnp.mean(centered * centered, -1, keepdims=True) + EPS)
            * gain.astype(F32)
        )
        gated = (jax.nn.silu(gate) * normed).astype(BF)
        gathered = broadcast_gather(gated, "kv", kv).reshape(H, S, HEAD_VALUE)
        gathered = gathered.transpose(1, 0, 2).reshape(S, H * HEAD_VALUE)
        part_b = jnp.dot(gathered, w_output, preferred_element_type=F32).astype(BF)
        part_b = part_b.reshape(S, tp, own).transpose(1, 0, 2)
        if tp == 2:
            keep = jnp.where(tpi == 0, part_b[0], part_b[1])
            send = jnp.where(tpi == 0, part_b[1], part_b[0])
            got = lax.ppermute(send, "tp", [(0, 1), (1, 0)])
            branch = keep.astype(F32) + got.astype(F32)
        else:
            branch = jnp.sum(
                lax.all_to_all(part_b, "tp", 0, 0, tiled=True).astype(F32), 0
            )
        own_residual = (tokens.astype(F32) + branch).astype(BF)

        residual = broadcast_gather(own_residual, ("kv", "tp"), kv * tp)
        residual = residual.transpose(1, 0, 2).reshape(S, width)
        wide = residual.astype(F32)
        scaled = (wide * mlp_gain.astype(F32)).astype(BF)
        lhs = jnp.concatenate([scaled, mlp_gain[None, :]], 0)
        up = jnp.dot(lhs, w_up, preferred_element_type=F32)
        average = jnp.sum(wide, -1) / width
        inverse = lax.rsqrt(jnp.sum(wide * wide, -1) / width - average * average + EPS)
        hidden = inverse[:, None] * (up[:S] - average[:, None] * up[S:])
        hidden = jnp.square(jax.nn.relu(hidden)).astype(BF)
        down = jnp.dot(hidden, w_down, preferred_element_type=F32).astype(BF)
        down = down.reshape(S, kv * tp, own).transpose(1, 0, 2)
        mixer = jnp.sum(
            lax.all_to_all(down, ("kv", "tp"), 0, 0, tiled=True).astype(F32), 0
        )
        return (own_residual.astype(F32) + mixer).astype(BF)

    return on_device


def lane_ids(rows):
    return lax.broadcasted_iota(jnp.int32, (rows, LANES), 1)


def row_ids(rows, columns=LANES):
    return lax.broadcasted_iota(jnp.int32, (rows, columns), 0)


def column_of(scalars, rows, dtype):
    ids = row_ids(rows)
    out = jnp.zeros((rows, LANES), dtype)
    for i in range(rows):
        out = jnp.where(ids == i, scalars[i].astype(dtype), out)
    return out


def gain_row(gain, rows):
    wide = gain[...].astype(F32)
    return jnp.concatenate(
        [jnp.broadcast_to(wide[i : i + 1], (rows, LANES)) for i in range(wide.shape[0])], 1
    )


def projection_rows(first, second, gain):
    t = lax.axis_index("tp")
    a, b = first[...].astype(F32), second[...].astype(F32)
    wide = jnp.concatenate([jnp.where(t == 0, a, b), jnp.where(t == 0, b, a)], 1)
    row = gain_row(gain, wide.shape[0])
    return jnp.concatenate([(wide * row).astype(BF), row.astype(BF)], 0), wide


def pack(q, csum, moments, message):
    columns = q.shape[1]
    half = csum.shape[0]
    message[:, :columns] = q.astype(BF)
    high = csum.astype(BF)
    low = (csum - high.astype(F32)).astype(BF)
    message[:, columns : columns + LANES] = jnp.concatenate([high, low], 0)
    high = moments.astype(BF).astype(F32)
    low = moments - high
    lanes = lane_ids(q.shape[0])
    both = jnp.where(lanes < 2, high, jnp.where(lanes < 4, pltpu.roll(low, 2, 1), 0.0))
    message[:, columns + LANES :] = both.astype(BF)
    assert 2 * half == q.shape[0]


def unpack_sum(state, messages):
    rows, total = state.shape
    columns = total - 2 * LANES
    half = rows // 2
    q = state[:, :columns]
    csum = state[:half, columns : columns + LANES]
    moments = state[:, columns + LANES :]
    for m in messages:
        q = q + m[:, :columns].astype(F32)
        c = m[:, columns : columns + LANES].astype(F32)
        csum = csum + c[:half] + c[half:]
        v = m[:, columns + LANES :].astype(F32)
        moments = moments + v + pltpu.roll(v, LANES - 2, 1)
    return q, csum, jnp.where(lane_ids(rows) < 2, moments, 0.0)


def store_state(q, csum, moments, state):
    columns = q.shape[1]
    state[:, :columns] = q
    state[:, columns : columns + LANES] = jnp.concatenate([csum, jnp.zeros_like(csum)], 0)
    state[:, columns + LANES :] = moments


def first_load_kernel(
    w_query,
    tokens,
    gain,
    lengths,
    decay,
    w_out,
    tokens_out,
    gain_out,
    length_out,
    rate_out,
    length_scalars,
    decay_scalars,
    sems,
):
    pairs = (
        (lengths, length_scalars),
        (decay, decay_scalars),
        (tokens, tokens_out),
        (gain, gain_out),
        (w_query, w_out),
    )
    copies = [pltpu.make_async_copy(a, b, sems.at[i]) for i, (a, b) in enumerate(pairs)]
    for copy in copies:
        copy.start()
    copies[0].wait()
    length_out[...] = column_of(length_scalars, length_out.shape[0], jnp.int32)
    copies[1].wait()
    rate_out[...] = column_of(decay_scalars, rate_out.shape[0], F32)
    for copy in copies[2:]:
        copy.wait()


def live_scalars(lengths, base):
    values = lengths[...]
    return [values[s, 0] > base for s in range(values.shape[0])]


def when_live(flags, copies, act):
    for flag, copy in zip(flags, copies):

        @pl.when(flag)
        def _():
            act(copy)


def copies_of(source, target, sems, first, count):
    return [
        pltpu.make_async_copy(source.at[s], target.at[s], sems.at[s - first])
        for s in range(first, first + count)
    ]


def cache_load_kernel(
    after, lengths, keys, values, keys_begun, keys_out, values_out, key_sems, value_sems
):
    rows, span = keys.shape[:2]
    live = live_scalars(lengths, lax.axis_index("kv") * span)
    half = rows // 2
    copies = copies_of(keys, keys_out, key_sems, half, rows - half)
    copies += copies_of(values, values_out, value_sems, 0, rows)
    when_live(live[half:] + live, copies, lambda copy: copy.start())
    when_live(live[half:] + live, copies, lambda copy: copy.wait())


def query_kernel(first, second, gain, w_query, state, message):
    lhs, wide = projection_rows(first, second, gain)
    rows = wide.shape[0]
    product = jnp.dot(lhs, w_query[...], preferred_element_type=F32)
    half = rows // 2
    ids = row_ids(half)
    csum = jnp.zeros((half, LANES), F32)
    for i in range(product.shape[1] // LANES):
        csum = jnp.where(
            ids == i, product[rows : rows + half, i * LANES : (i + 1) * LANES], csum
        )
    lanes = lane_ids(rows)
    first_sum = jnp.sum(wide, 1, keepdims=True)
    second_sum = jnp.sum(wide * wide, 1, keepdims=True)
    moments = jnp.where(lanes == 0, first_sum, jnp.where(lanes == 1, second_sum, 0.0))
    store_state(product[:rows], csum, moments, state)
    pack(product[:rows], csum, moments, message)


def middle_kernel(old, m1, m2, m3, state, message):
    q, csum, moments = unpack_sum(old, (m1, m2, m3))
    store_state(q, csum, moments, state)
    pack(q, csum, moments, message)


def other_kernel(
    after,
    lengths,
    rates,
    first,
    second,
    gain,
    w_key,
    w_value,
    w_gate,
    w_output,
    keys,
    k_out,
    v_out,
    g_out,
    turn,
    weights,
    w_keep,
    keys_out,
    key_buffer,
    value_buffer,
    gate_buffer,
    sems,
    cache_sems,
):
    own = w_keep.shape[1]
    kept = pl.ds(pl.multiple_of(lax.axis_index("tp") * own, own), own)
    buffers = (key_buffer, value_buffer, gate_buffer)
    pairs = (
        (w_key, key_buffer),
        (w_value, value_buffer),
        (w_gate, gate_buffer),
        (w_output.at[:, kept], w_keep),
    )
    copies = [pltpu.make_async_copy(a, b, sems.at[i]) for i, (a, b) in enumerate(pairs)]
    for copy in copies:
        copy.start()
    lhs, wide = projection_rows(first, second, gain)
    rows = wide.shape[0]
    live = live_scalars(lengths, lax.axis_index("kv") * keys.shape[1])[: rows // 2]
    caches = copies_of(keys, keys_out, cache_sems, 0, rows // 2)
    when_live(live, caches, lambda copy: copy.start())
    half = HEAD_KEY // 2
    entry = (lane_ids(rows) % half).astype(F32)
    inverse = jnp.exp(entry * (-math.log(THETA) / half))
    angle = lengths[...].astype(F32) * inverse
    turn[0] = jnp.cos(angle)
    turn[1] = jnp.sin(angle)
    heads = rates.shape[0]
    places = lax.axis_index("kv") * LANES + lane_ids(heads)
    rate = rates[...]
    for s in range(rows):
        distance = jnp.broadcast_to(lengths[s : s + 1, :], (heads, LANES)) - places
        weight = jnp.exp(-rate * jnp.maximum(distance, 0).astype(F32)) * HEAD_KEY ** (-0.5)
        weights[s] = jnp.where(distance > 0, weight, 0.0)
    for copy, buffer, out in zip(copies, buffers, (k_out, v_out, g_out)):
        copy.wait()
        product = jnp.dot(lhs, buffer[...], preferred_element_type=F32)
        out[...] = product[: rows + 8]
    for copy in copies[len(buffers) :]:
        copy.wait()
    when_live(live, caches, lambda copy: copy.wait())


def attend_kernel(
    width,
    after,
    lengths,
    old,
    m1,
    m2,
    m3,
    k_part,
    v_part,
    g_part,
    turn,
    weights,
    keys,
    values,
    out,
    query_rows,
    cached,
    order,
):
    rows, span, key_columns = keys.shape
    heads = key_columns // HEAD_KEY
    q, csum, moments = unpack_sum(old, (m1, m2, m3))
    average = moments[:, 0:1] / width
    inverse = lax.rsqrt(moments[:, 1:2] / width - average * average + EPS)
    lanes = lane_ids(rows)
    in_first = lanes % HEAD_KEY < HEAD_KEY // 2
    low_head = lanes < HEAD_KEY
    top = rows // 2
    cosine, sine = turn[0], turn[1]
    for i in range(key_columns // LANES):
        cut = slice(i * LANES, (i + 1) * LANES)
        plain = inverse * (q[:, cut] - average * csum[i : i + 1])
        partner = jnp.where(
            in_first,
            -pltpu.roll(plain, LANES - HEAD_KEY // 2, 1),
            pltpu.roll(plain, HEAD_KEY // 2, 1),
        )
        turned = plain * cosine + partner * sine
        query_rows[:, cut] = turned.astype(BF).astype(F32)
        part = inverse * (k_part[:rows, cut] - average * k_part[rows : rows + 1, cut])
        both = plain * part * HEAD_KEY ** (-0.5)
        for j in range(2):
            picked = jnp.where(low_head == (j == 0), both, 0.0)
            score = jnp.sum(picked, 1, keepdims=True)
            high = score.astype(BF).astype(F32)
            low = score - high
            folded = jnp.where(
                lanes[:top] < HEAD_KEY,
                jnp.where(in_first[:top], high[:top], low[:top]),
                jnp.where(in_first[:top], high[top:], low[top:]),
            )
            out[2 * i + j, 3 * rows :, :] = folded.astype(BF)
    for h in range(heads):
        cut = slice(h * LANES, (h + 1) * LANES)
        for place, part in ((1, v_part), (2, g_part)):
            normed = inverse * (part[:rows, cut] - average * part[rows : rows + 1, cut])
            out[h, place * rows : (place + 1) * rows, :] = normed.astype(BF)

    head_of_key = lax.broadcasted_iota(jnp.int32, (heads, key_columns), 1) // HEAD_KEY
    own_key = head_of_key == row_ids(heads, key_columns)
    value_columns = heads * HEAD_VALUE
    head_of_value = lax.broadcasted_iota(jnp.int32, (heads, value_columns), 1) // HEAD_VALUE
    own_value = head_of_value == row_ids(heads, value_columns)
    live = live_scalars(lengths, lax.axis_index("kv") * span)
    count = jnp.int32(0)
    for s in range(rows):
        order[count] = s
        count = count + live[s].astype(jnp.int32)

    def one(s, is_live):
        row = pl.ds(s, 1)
        spread = jnp.broadcast_to(query_rows[row, :], (heads, key_columns))
        query = jnp.where(own_key, spread, 0.0).astype(BF)
        scores = lax.dot_general(
            query, keys[s], (((1,), (1,)), ((), ())), preferred_element_type=F32
        )
        weight = weights[s]
        coefficients = jnp.where(weight > 0.0, scores * weight, 0.0).astype(BF)
        product = jnp.dot(coefficients, values[s], preferred_element_type=F32)
        kept = jnp.logical_and(own_value, is_live)
        cached[row, :] = jnp.sum(jnp.where(kept, product, 0.0), 0, keepdims=True)

    steps = [n for n in (4, 8) if n < rows] + [rows]
    for least, most in zip([-1] + steps[:-1], steps):

        @pl.when(jnp.logical_and(count > least, count <= most))
        def _():
            if most == rows:
                for s in range(rows):
                    one(s, live[s])
            else:
                cached[...] = jnp.zeros_like(cached)
                for i in range(most):
                    one(order[jnp.minimum(i, jnp.maximum(count - 1, 0))], count > 0)

    for h in range(heads):
        out[h, :rows, :] = cached[:, h * LANES : (h + 1) * LANES].astype(BF)


def gate_kernel(pieces, head_gain, out):
    rows = out.shape[1]
    total = jnp.sum(pieces[...].astype(F32), 0)
    cached, value, gate = (total[i * rows : (i + 1) * rows] for i in range(3))
    folded = total[3 * rows :]
    half = HEAD_KEY // 2
    score = jnp.concatenate(
        [folded[:, i : i + 1] + folded[:, i + half : i + half + 1] for i in (0, HEAD_KEY)], 0
    )
    retained = cached + score * value
    centered = retained - jnp.mean(retained, -1, keepdims=True)
    spread = lax.rsqrt(jnp.mean(centered * centered, -1, keepdims=True) + EPS)
    gains = head_gain[...].astype(F32)
    mine = row_ids(gains.shape[0]) == lax.axis_index("kv")
    gain = jnp.sum(jnp.where(mine, gains, 0.0), 0, keepdims=True)
    normed = centered * spread * gain
    gated = (gate * jax.nn.sigmoid(gate) * normed).astype(BF)
    out[...] = jnp.broadcast_to(gated[None], out.shape)


def output_kernel(gated, w_keep, w_got, tokens, own, out):
    heads = gated.shape[0] // 2
    t = lax.axis_index("tp")
    branch = 0.0
    width = own.shape[1]
    columns = pl.ds(pl.multiple_of(t * width, width), width)
    for group, w in ((t, w_keep[...]), (1 - t, w_got[:, columns])):
        lhs = jnp.concatenate([gated[2 * h + group] for h in range(heads)], 1)
        part = jnp.dot(lhs, w, preferred_element_type=F32)
        branch = branch + part.astype(BF).astype(F32)
    residual = (tokens[...].astype(F32) + branch).astype(BF)
    own[...] = residual
    out[...] = jnp.broadcast_to(residual[None], out.shape)


def mixer_kernel(residual, mlp_gain, w_up, w_down, out):
    blocks, rows, own = residual.shape
    width = blocks * own
    first = jnp.zeros((rows, own), F32)
    second = jnp.zeros((rows, own), F32)
    scaled, gain = [], []
    gains = mlp_gain[...].astype(F32)
    for i in range(blocks):
        wide = residual[i].astype(F32)
        first = first + wide
        second = second + wide * wide
        row = gains[i : i + 1]
        scaled.append((wide * row).astype(BF))
        gain.append(jnp.broadcast_to(row, wide.shape).astype(BF))
    lhs = jnp.concatenate([jnp.concatenate(scaled, 1), jnp.concatenate(gain, 1)], 0)
    up = jnp.dot(lhs, w_up[...], preferred_element_type=F32)
    average = jnp.sum(first, 1, keepdims=True) / width
    inverse = lax.rsqrt(jnp.sum(second, 1, keepdims=True) / width - average * average + EPS)
    hidden = inverse * (up[:rows] - average * up[rows : rows + 1])
    hidden = jnp.square(jnp.maximum(hidden, 0.0)).astype(BF)
    down = jnp.dot(hidden, w_down[...], preferred_element_type=F32)
    for i in range(blocks):
        out[i] = down[:, i * own : (i + 1) * own].astype(BF)


def final_kernel(pieces, own, out):
    total = jnp.sum(pieces[...].astype(F32), 0)
    out[...] = (own[...].astype(F32) + total).astype(BF)


VMEM = pl.BlockSpec(memory_space=pltpu.VMEM)
HBM = pl.BlockSpec(memory_space=pltpu.HBM)
ANY = pl.BlockSpec(memory_space=pl.ANY)


def in_hbm(*arrays):
    return [pltpu.with_memory_space_constraint(x, pltpu.HBM) for x in arrays]


def call(kernel, outs, in_specs, flops=0, bytes_accessed=0, scratch=(), limit=None, aliases={}):
    return pl.pallas_call(
        kernel,
        out_shape=outs,
        in_specs=in_specs,
        out_specs=jax.tree.map(lambda _: VMEM, outs),
        scratch_shapes=list(scratch),
        input_output_aliases=aliases,
        cost_estimate=pl.CostEstimate(
            flops=flops, bytes_accessed=bytes_accessed, transcendentals=0
        ),
        compiler_params=pltpu.CompilerParams(vmem_limit_bytes=limit),
    )


def make_kernels_on_device(kv, tp):
    def on_device(
        tokens,
        lengths,
        attn_gain,
        w_query,
        w_key,
        w_value,
        w_gate,
        decay_rate,
        key_cache,
        value_cache,
        head_gain,
        w_output,
        mlp_gain,
        w_up,
        w_down,
    ):
        S, own = tokens.shape
        H = decay_rate.shape[0]
        width = own * kv * tp
        qc, vc = H * HEAD_KEY, H * HEAD_VALUE
        swap = [(0, 1), (1, 0)]
        mib = 1 << 20
        sds = jax.ShapeDtypeStruct

        other = lax.ppermute(tokens, "tp", swap)
        w_got = lax.ppermute(w_output, "tp", swap)
        gain = attn_gain.reshape(-1, LANES)
        w_query, tokens, gain, length_rows, rates = call(
            first_load_kernel,
            (
                sds(w_query.shape, BF),
                sds(tokens.shape, BF),
                sds(gain.shape, BF),
                sds((S, LANES), jnp.int32),
                sds((H, LANES), F32),
            ),
            [HBM] * 5,
            flops=10**9,
            scratch=[
                pltpu.SMEM((S,), jnp.int32),
                pltpu.SMEM((H,), F32),
                pltpu.SemaphoreType.DMA((5,)),
            ],
            limit=2 * mib,
        )(*in_hbm(w_query, tokens, gain, lengths, decay_rate))
        columns = qc + 2 * LANES
        message_types = (sds((S, columns), F32), sds((S, columns), BF))
        state, message = call(
            query_kernel, message_types, [VMEM] * 4, limit=2 * mib
        )(tokens, other, gain, w_query)

        def exchange(message, stride):
            return [
                lax.ppermute(message, "kv", [(i, i ^ (j * stride)) for i in range(kv)])
                for j in range(1, 4)
            ]

        got = exchange(message, 1)
        k_part, v_part, g_part, turn, weights, w_keep, keys = call(
            other_kernel,
            (
                sds((S + 8, qc), F32),
                sds((S + 8, vc), F32),
                sds((S + 8, vc), F32),
                sds((2, S, LANES), F32),
                sds((S, H, LANES), F32),
                sds((w_output.shape[0], own), BF),
                sds(key_cache.shape, BF),
            ),
            [ANY] + [VMEM] * 5 + [HBM] * 5,
            flops=10**9,
            scratch=[pltpu.VMEM(w.shape, BF) for w in (w_key, w_value, w_gate)]
            + [pltpu.SemaphoreType.DMA((4,)), pltpu.SemaphoreType.DMA((S // 2,))],
            limit=6 * mib,
        )(
            message,
            length_rows,
            rates,
            tokens,
            other,
            gain,
            *in_hbm(w_key, w_value, w_gate, w_output, key_cache),
        )

        stride = 4
        while stride < kv:
            state, message = call(
                middle_kernel, message_types, [VMEM] * 4, limit=2 * mib
            )(state, *got)
            got = exchange(message, stride)
            stride *= 4
        keys, values = call(
            cache_load_kernel,
            (sds(key_cache.shape, BF), sds(value_cache.shape, BF)),
            [ANY, VMEM] + [HBM] * 2 + [VMEM],
            flops=10**9,
            scratch=[pltpu.SemaphoreType.DMA((S,))] * 2,
            limit=2 * mib,
            aliases={4: 0},
        )(message, length_rows, *in_hbm(key_cache, value_cache), keys)

        pieces = call(
            functools.partial(attend_kernel, width),
            sds((H, 3 * S + S // 2, LANES), BF),
            [ANY] + [VMEM] * 12,
            scratch=[
                pltpu.VMEM((S, qc), F32),
                pltpu.VMEM((S, vc), F32),
                pltpu.SMEM((S,), jnp.int32),
            ],
            limit=4 * mib,
        )(w_got, length_rows, state, *got, k_part, v_part, g_part, turn, weights, keys, values)

        pieces = lax.all_to_all(pieces, "kv", 0, 0, tiled=True)
        gated = call(
            gate_kernel, sds((kv * tp, S, LANES), BF), [VMEM] * 2, limit=2 * mib
        )(pieces, head_gain.reshape(H, HEAD_VALUE))
        gated = lax.all_to_all(gated, ("kv", "tp"), 0, 0, tiled=True)
        residual, spread = call(
            output_kernel,
            (sds((S, own), BF), sds((kv * tp, S, own), BF)),
            [VMEM] * 4,
            limit=4 * mib,
        )(gated, w_keep, w_got, tokens)
        spread = lax.all_to_all(spread, ("kv", "tp"), 0, 0, tiled=True)
        down = call(
            mixer_kernel, sds((kv * tp, S, own), BF), [VMEM] * 4, limit=16 * mib
        )(spread, mlp_gain.reshape(-1, LANES), w_up, w_down)
        down = lax.all_to_all(down, ("kv", "tp"), 0, 0, tiled=True)
        return call(final_kernel, sds((S, own), BF), [VMEM] * 2, limit=2 * mib)(down, residual)

    return on_device


def solution(mesh):
    in_specs = (
        P(None, ("kv", "tp")),
        P(),
        P("kv"),
        P("kv", "tp"),
        P("kv", "tp"),
        P("kv", "tp"),
        P("kv", "tp"),
        P("tp"),
        P(None, "kv", "tp"),
        P(None, "kv", "tp"),
        P("tp"),
        P("tp", "kv"),
        P(),
        P(None, ("kv", "tp")),
        P(("kv", "tp"), None),
    )
    kv, tp = mesh.shape["kv"], mesh.shape["tp"]

    def on_device(*arrays):
        fits = tp == 2 and arrays[7].shape[0] == kv
        fits = fits and arrays[0].shape[1] == LANES == arrays[8].shape[1]
        make = make_kernels_on_device if fits else make_on_device
        return make(kv, tp)(*arrays)

    return jax.shard_map(
        on_device,
        mesh=mesh,
        in_specs=in_specs,
        out_specs=P(None, ("kv", "tp")),
        check_vma=False,
    )
```

```python
import functools
import math

import jax
import jax.numpy as jnp
from jax import lax
from jax.experimental import pallas as pl
from jax.experimental.pallas import tpu as pltpu
from jax.sharding import PartitionSpec as P


HEAD_KEY = 64
HEAD_VALUE = 128
EPS = 1e-05
THETA = 10000.0
LANES = 128

BF = jnp.bfloat16
F32 = jnp.float32


def split_two(x):
    high = x.astype(BF)
    return high, (x - high.astype(F32)).astype(BF)


def rotate(flat, cosine, sine):
    rows = flat.shape[0]
    grouped = flat.reshape(rows, -1, HEAD_KEY)
    half = HEAD_KEY // 2
    a, b = grouped[..., :half], grouped[..., half:]
    c, s = cosine[:, None, :], sine[:, None, :]
    return jnp.concatenate([a * c - b * s, b * c + a * s], -1).reshape(rows, -1)


def broadcast_gather(x, axes, size):
    spread = jnp.broadcast_to(x[None], (size,) + x.shape)
    return lax.all_to_all(spread, axes, 0, 0, tiled=True)


def make_on_device(kv, tp):
    def on_device(
        tokens,
        lengths,
        attn_gain,
        w_query,
        w_key,
        w_value,
        w_gate,
        decay_rate,
        key_cache,
        value_cache,
        head_gain,
        w_output,
        mlp_gain,
        w_up,
        w_down,
    ):
        S = tokens.shape[0]
        H = decay_rate.shape[0]
        span = key_cache.shape[1]
        width = tokens.shape[1] * kv * tp
        own = tokens.shape[1]
        kvi = lax.axis_index("kv")
        tpi = lax.axis_index("tp")
        groups = kv // H
        rows = S // groups

        if tp == 2:
            other = lax.ppermute(tokens, "tp", [(0, 1), (1, 0)])
            low = jnp.where(tpi == 0, tokens, other)
            high = jnp.where(tpi == 0, other, tokens)
            block = jnp.concatenate([low, high], 1)
        else:
            block = lax.all_gather(tokens, "tp", axis=1, tiled=True)
        wide = block.astype(F32)
        scaled = (wide * attn_gain.astype(F32)).astype(BF)
        lhs = jnp.concatenate([scaled, attn_gain[None, :]], 0)
        part_q = jnp.dot(lhs, w_query, preferred_element_type=F32)
        moments = jnp.stack([jnp.sum(wide, -1), jnp.sum(wide * wide, -1)], -1)

        small = jnp.concatenate([part_q[S], moments.reshape(-1)])
        q_sum = part_q[:S]
        stride = 1
        while stride < kv:
            count = 4 if kv % (stride * 4) == 0 else 2
            high, low = split_two(small)
            tail = jnp.concatenate([high, low])
            pad = -tail.shape[0] % S
            tail = jnp.pad(tail, (0, pad)).reshape(S, -1)
            message = jnp.concatenate([q_sum.astype(BF), tail], 1)
            for j in range(1, count):
                got = lax.ppermute(message, "kv", [(i, i ^ (j * stride)) for i in range(kv)])
                got = got.astype(F32)
                q_sum = q_sum + got[:, : q_sum.shape[1]]
                flat = got[:, q_sum.shape[1] :].reshape(-1)
                n = small.shape[0]
                small = small + flat[:n] + flat[n : 2 * n]
            stride *= count
        csum_q = small[: q_sum.shape[1]]
        moments = small[q_sum.shape[1] :].reshape(S, 2)
        average = moments[:, 0] / width
        inverse = lax.rsqrt(moments[:, 1] / width - average * average + EPS)

        half = HEAD_KEY // 2
        turn = jnp.power(THETA, -jnp.arange(half, dtype=F32) / half)
        angles = lengths.astype(F32)[:, None] * turn[None, :]
        q_plain = inverse[:, None] * (q_sum - average[:, None] * csum_q[None, :])
        queries = rotate(q_plain, jnp.cos(angles), jnp.sin(angles)).astype(BF)
        queries = queries.reshape(S, H, HEAD_KEY)

        def partial(w):
            p = jnp.dot(lhs, w, preferred_element_type=F32)
            return inverse[:, None] * (p[:S] - average[:, None] * p[S:])

        part_k = partial(w_key).reshape(S, H, HEAD_KEY)
        part_v = partial(w_value).reshape(S, H, HEAD_VALUE)
        part_g = partial(w_gate).reshape(S, H, HEAD_VALUE)
        part_score = jnp.sum(q_plain.reshape(S, H, HEAD_KEY) * part_k, -1) * HEAD_KEY ** (-0.5)

        keys = key_cache.reshape(S, span, H, HEAD_KEY)
        values = value_cache.reshape(S, span, H, HEAD_VALUE)
        scores = jnp.einsum("bhd,bjhd->bhj", queries, keys, preferred_element_type=F32)
        places = kvi * span + jnp.arange(span, dtype=jnp.int32)
        distance = jnp.maximum(lengths[:, None] - places[None, :], 0).astype(F32)
        live = (places[None, :] < lengths[:, None])[:, None, :]
        decays = jnp.where(
            live, jnp.exp(-decay_rate[None, :, None] * distance[:, None, :]), 0.0
        )
        coefficients = (scores * HEAD_KEY ** (-0.5) * decays).astype(BF)
        part_c = jnp.einsum("bhj,bjhe->bhe", coefficients, values, preferred_element_type=F32)

        high, low = split_two(part_score)
        pieces = jnp.concatenate(
            [
                part_c.astype(BF),
                part_v.astype(BF),
                part_g.astype(BF),
                high[..., None],
                low[..., None],
                jnp.zeros((S, H, 126), BF),
            ],
            -1,
        )
        pieces = pieces.transpose(1, 0, 2).reshape(kv, rows, 4 * HEAD_VALUE)
        mine = jnp.sum(
            lax.all_to_all(pieces, "kv", 0, 0, tiled=True).astype(F32), 0
        )
        cached, value, gate = (
            mine[:, i * HEAD_VALUE : (i + 1) * HEAD_VALUE] for i in range(3)
        )
        score = mine[:, 3 * HEAD_VALUE] + mine[:, 3 * HEAD_VALUE + 1]
        retained = cached + score[:, None] * value
        centered = retained - jnp.mean(retained, -1, keepdims=True)
        gain = lax.dynamic_slice(head_gain, ((kvi // groups) * HEAD_VALUE,), (HEAD_VALUE,))
        normed = (
            centered
            * lax.rsqrt(jnp.mean(centered * centered, -1, keepdims=True) + EPS)
            * gain.astype(F32)
        )
        gated = (jax.nn.silu(gate) * normed).astype(BF)
        gathered = broadcast_gather(gated, "kv", kv).reshape(H, S, HEAD_VALUE)
        gathered = gathered.transpose(1, 0, 2).reshape(S, H * HEAD_VALUE)
        part_b = jnp.dot(gathered, w_output, preferred_element_type=F32).astype(BF)
        part_b = part_b.reshape(S, tp, own).transpose(1, 0, 2)
        if tp == 2:
            keep = jnp.where(tpi == 0, part_b[0], part_b[1])
            send = jnp.where(tpi == 0, part_b[1], part_b[0])
            got = lax.ppermute(send, "tp", [(0, 1), (1, 0)])
            branch = keep.astype(F32) + got.astype(F32)
        else:
            branch = jnp.sum(
                lax.all_to_all(part_b, "tp", 0, 0, tiled=True).astype(F32), 0
            )
        own_residual = (tokens.astype(F32) + branch).astype(BF)

        residual = broadcast_gather(own_residual, ("kv", "tp"), kv * tp)
        residual = residual.transpose(1, 0, 2).reshape(S, width)
        wide = residual.astype(F32)
        scaled = (wide * mlp_gain.astype(F32)).astype(BF)
        lhs = jnp.concatenate([scaled, mlp_gain[None, :]], 0)
        up = jnp.dot(lhs, w_up, preferred_element_type=F32)
        average = jnp.sum(wide, -1) / width
        inverse = lax.rsqrt(jnp.sum(wide * wide, -1) / width - average * average + EPS)
        hidden = inverse[:, None] * (up[:S] - average[:, None] * up[S:])
        hidden = jnp.square(jax.nn.relu(hidden)).astype(BF)
        down = jnp.dot(hidden, w_down, preferred_element_type=F32).astype(BF)
        down = down.reshape(S, kv * tp, own).transpose(1, 0, 2)
        mixer = jnp.sum(
            lax.all_to_all(down, ("kv", "tp"), 0, 0, tiled=True).astype(F32), 0
        )
        return (own_residual.astype(F32) + mixer).astype(BF)

    return on_device


def lane_ids(rows):
    return lax.broadcasted_iota(jnp.int32, (rows, LANES), 1)


def row_ids(rows, columns=LANES):
    return lax.broadcasted_iota(jnp.int32, (rows, columns), 0)


def column_of(scalars, rows, dtype):
    ids = row_ids(rows)
    out = jnp.zeros((rows, LANES), dtype)
    for i in range(rows):
        out = jnp.where(ids == i, scalars[i].astype(dtype), out)
    return out


def gain_row(gain, rows):
    wide = gain[...].astype(F32)
    return jnp.concatenate(
        [jnp.broadcast_to(wide[i : i + 1], (rows, LANES)) for i in range(wide.shape[0])], 1
    )


def projection_rows(first, second, gain):
    t = lax.axis_index("tp")
    a, b = first[...].astype(F32), second[...].astype(F32)
    wide = jnp.concatenate([jnp.where(t == 0, a, b), jnp.where(t == 0, b, a)], 1)
    row = gain_row(gain, wide.shape[0])
    return jnp.concatenate([(wide * row).astype(BF), row.astype(BF)], 0), wide


def pack(q, csum, moments, message):
    columns = q.shape[1]
    half = csum.shape[0]
    message[:, :columns] = q.astype(BF)
    high = csum.astype(BF)
    low = (csum - high.astype(F32)).astype(BF)
    message[:, columns : columns + LANES] = jnp.concatenate([high, low], 0)
    high = moments.astype(BF).astype(F32)
    low = moments - high
    lanes = lane_ids(q.shape[0])
    both = jnp.where(lanes < 2, high, jnp.where(lanes < 4, pltpu.roll(low, 2, 1), 0.0))
    message[:, columns + LANES :] = both.astype(BF)
    assert 2 * half == q.shape[0]


def unpack_sum(state, messages):
    rows, total = state.shape
    columns = total - 2 * LANES
    half = rows // 2
    q = state[:, :columns]
    csum = state[:half, columns : columns + LANES]
    moments = state[:, columns + LANES :]
    for m in messages:
        q = q + m[:, :columns].astype(F32)
        c = m[:, columns : columns + LANES].astype(F32)
        csum = csum + c[:half] + c[half:]
        v = m[:, columns + LANES :].astype(F32)
        moments = moments + v + pltpu.roll(v, LANES - 2, 1)
    return q, csum, jnp.where(lane_ids(rows) < 2, moments, 0.0)


def store_state(q, csum, moments, state):
    columns = q.shape[1]
    state[:, :columns] = q
    state[:, columns : columns + LANES] = jnp.concatenate([csum, jnp.zeros_like(csum)], 0)
    state[:, columns + LANES :] = moments


def first_load_kernel(
    w_query,
    tokens,
    gain,
    lengths,
    decay,
    w_out,
    tokens_out,
    gain_out,
    length_out,
    rate_out,
    length_scalars,
    decay_scalars,
    sems,
):
    pairs = (
        (lengths, length_scalars),
        (decay, decay_scalars),
        (tokens, tokens_out),
        (gain, gain_out),
        (w_query, w_out),
    )
    copies = [pltpu.make_async_copy(a, b, sems.at[i]) for i, (a, b) in enumerate(pairs)]
    for copy in copies:
        copy.start()
    copies[0].wait()
    length_out[...] = column_of(length_scalars, length_out.shape[0], jnp.int32)
    copies[1].wait()
    rate_out[...] = column_of(decay_scalars, rate_out.shape[0], F32)
    for copy in copies[2:]:
        copy.wait()


def live_scalars(lengths, base):
    values = lengths[...]
    return [values[s, 0] > base for s in range(values.shape[0])]


def when_live(flags, copies, act):
    for flag, copy in zip(flags, copies):

        @pl.when(flag)
        def _():
            act(copy)


def copies_of(source, target, sems, first, count):
    return [
        pltpu.make_async_copy(source.at[s], target.at[s], sems.at[s - first])
        for s in range(first, first + count)
    ]


def cache_load_kernel(
    after, lengths, keys, values, keys_begun, keys_out, values_out, key_sems, value_sems
):
    rows, span = keys.shape[:2]
    live = live_scalars(lengths, lax.axis_index("kv") * span)
    half = rows // 2
    copies = copies_of(keys, keys_out, key_sems, half, rows - half)
    copies += copies_of(values, values_out, value_sems, 0, rows)
    when_live(live[half:] + live, copies, lambda copy: copy.start())
    when_live(live[half:] + live, copies, lambda copy: copy.wait())


def query_kernel(first, second, gain, w_query, state, message):
    lhs, wide = projection_rows(first, second, gain)
    rows = wide.shape[0]
    product = jnp.dot(lhs, w_query[...], preferred_element_type=F32)
    half = rows // 2
    ids = row_ids(half)
    csum = jnp.zeros((half, LANES), F32)
    for i in range(product.shape[1] // LANES):
        csum = jnp.where(
            ids == i, product[rows : rows + half, i * LANES : (i + 1) * LANES], csum
        )
    lanes = lane_ids(rows)
    first_sum = jnp.sum(wide, 1, keepdims=True)
    second_sum = jnp.sum(wide * wide, 1, keepdims=True)
    moments = jnp.where(lanes == 0, first_sum, jnp.where(lanes == 1, second_sum, 0.0))
    store_state(product[:rows], csum, moments, state)
    pack(product[:rows], csum, moments, message)


def middle_kernel(old, m1, m2, m3, state, message):
    q, csum, moments = unpack_sum(old, (m1, m2, m3))
    store_state(q, csum, moments, state)
    pack(q, csum, moments, message)


def other_kernel(
    after,
    lengths,
    rates,
    first,
    second,
    gain,
    w_key,
    w_value,
    w_gate,
    w_output,
    keys,
    k_out,
    v_out,
    g_out,
    turn,
    weights,
    w_keep,
    keys_out,
    key_buffer,
    value_buffer,
    gate_buffer,
    sems,
    cache_sems,
):
    own = w_keep.shape[1]
    kept = pl.ds(pl.multiple_of(lax.axis_index("tp") * own, own), own)
    buffers = (key_buffer, value_buffer, gate_buffer)
    pairs = (
        (w_key, key_buffer),
        (w_value, value_buffer),
        (w_gate, gate_buffer),
        (w_output.at[:, kept], w_keep),
    )
    copies = [pltpu.make_async_copy(a, b, sems.at[i]) for i, (a, b) in enumerate(pairs)]
    for copy in copies:
        copy.start()
    lhs, wide = projection_rows(first, second, gain)
    rows = wide.shape[0]
    live = live_scalars(lengths, lax.axis_index("kv") * keys.shape[1])[: rows // 2]
    caches = copies_of(keys, keys_out, cache_sems, 0, rows // 2)
    when_live(live, caches, lambda copy: copy.start())
    half = HEAD_KEY // 2
    entry = (lane_ids(rows) % half).astype(F32)
    inverse = jnp.exp(entry * (-math.log(THETA) / half))
    angle = lengths[...].astype(F32) * inverse
    turn[0] = jnp.cos(angle)
    turn[1] = jnp.sin(angle)
    heads = rates.shape[0]
    places = lax.axis_index("kv") * LANES + lane_ids(heads)
    rate = rates[...]
    for s in range(rows):
        distance = jnp.broadcast_to(lengths[s : s + 1, :], (heads, LANES)) - places
        weight = jnp.exp(-rate * jnp.maximum(distance, 0).astype(F32)) * HEAD_KEY ** (-0.5)
        weights[s] = jnp.where(distance > 0, weight, 0.0)
    for copy, buffer, out in zip(copies, buffers, (k_out, v_out, g_out)):
        copy.wait()
        product = jnp.dot(lhs, buffer[...], preferred_element_type=F32)
        out[...] = product[: rows + 8]
    for copy in copies[len(buffers) :]:
        copy.wait()
    when_live(live, caches, lambda copy: copy.wait())


def attend_kernel(
    width,
    after,
    lengths,
    old,
    m1,
    m2,
    m3,
    k_part,
    v_part,
    g_part,
    turn,
    weights,
    keys,
    values,
    out,
    query_rows,
    cached,
    order,
):
    rows, span, key_columns = keys.shape
    heads = key_columns // HEAD_KEY
    q, csum, moments = unpack_sum(old, (m1, m2, m3))
    average = moments[:, 0:1] / width
    inverse = lax.rsqrt(moments[:, 1:2] / width - average * average + EPS)
    lanes = lane_ids(rows)
    in_first = lanes % HEAD_KEY < HEAD_KEY // 2
    low_head = lanes < HEAD_KEY
    top = rows // 2
    cosine, sine = turn[0], turn[1]
    for i in range(key_columns // LANES):
        cut = slice(i * LANES, (i + 1) * LANES)
        plain = inverse * (q[:, cut] - average * csum[i : i + 1])
        partner = jnp.where(
            in_first,
            -pltpu.roll(plain, LANES - HEAD_KEY // 2, 1),
            pltpu.roll(plain, HEAD_KEY // 2, 1),
        )
        turned = plain * cosine + partner * sine
        query_rows[:, cut] = turned.astype(BF).astype(F32)
        part = inverse * (k_part[:rows, cut] - average * k_part[rows : rows + 1, cut])
        both = plain * part * HEAD_KEY ** (-0.5)
        for j in range(2):
            picked = jnp.where(low_head == (j == 0), both, 0.0)
            score = jnp.sum(picked, 1, keepdims=True)
            high = score.astype(BF).astype(F32)
            low = score - high
            folded = jnp.where(
                lanes[:top] < HEAD_KEY,
                jnp.where(in_first[:top], high[:top], low[:top]),
                jnp.where(in_first[:top], high[top:], low[top:]),
            )
            out[2 * i + j, 3 * rows :, :] = folded.astype(BF)
    for h in range(heads):
        cut = slice(h * LANES, (h + 1) * LANES)
        for place, part in ((1, v_part), (2, g_part)):
            normed = inverse * (part[:rows, cut] - average * part[rows : rows + 1, cut])
            out[h, place * rows : (place + 1) * rows, :] = normed.astype(BF)

    head_of_key = lax.broadcasted_iota(jnp.int32, (heads, key_columns), 1) // HEAD_KEY
    own_key = head_of_key == row_ids(heads, key_columns)
    value_columns = heads * HEAD_VALUE
    head_of_value = lax.broadcasted_iota(jnp.int32, (heads, value_columns), 1) // HEAD_VALUE
    own_value = head_of_value == row_ids(heads, value_columns)
    live = live_scalars(lengths, lax.axis_index("kv") * span)
    count = jnp.int32(0)
    for s in range(rows):
        order[count] = s
        count = count + live[s].astype(jnp.int32)

    def one(s, is_live):
        row = pl.ds(s, 1)
        spread = jnp.broadcast_to(query_rows[row, :], (heads, key_columns))
        query = jnp.where(own_key, spread, 0.0).astype(BF)
        scores = lax.dot_general(
            query, keys[s], (((1,), (1,)), ((), ())), preferred_element_type=F32
        )
        weight = weights[s]
        coefficients = jnp.where(weight > 0.0, scores * weight, 0.0).astype(BF)
        product = jnp.dot(coefficients, values[s], preferred_element_type=F32)
        kept = jnp.logical_and(own_value, is_live)
        cached[row, :] = jnp.sum(jnp.where(kept, product, 0.0), 0, keepdims=True)

    steps = [n for n in (4, 8) if n < rows] + [rows]
    for least, most in zip([-1] + steps[:-1], steps):

        @pl.when(jnp.logical_and(count > least, count <= most))
        def _():
            if most == rows:
                for s in range(rows):
                    one(s, live[s])
            else:
                cached[...] = jnp.zeros_like(cached)
                for i in range(most):
                    one(order[jnp.minimum(i, jnp.maximum(count - 1, 0))], count > 0)

    for h in range(heads):
        out[h, :rows, :] = cached[:, h * LANES : (h + 1) * LANES].astype(BF)


def gate_kernel(pieces, head_gain, out):
    rows = out.shape[1]
    total = jnp.sum(pieces[...].astype(F32), 0)
    cached, value, gate = (total[i * rows : (i + 1) * rows] for i in range(3))
    folded = total[3 * rows :]
    half = HEAD_KEY // 2
    score = jnp.concatenate(
        [folded[:, i : i + 1] + folded[:, i + half : i + half + 1] for i in (0, HEAD_KEY)], 0
    )
    retained = cached + score * value
    centered = retained - jnp.mean(retained, -1, keepdims=True)
    spread = lax.rsqrt(jnp.mean(centered * centered, -1, keepdims=True) + EPS)
    gains = head_gain[...].astype(F32)
    mine = row_ids(gains.shape[0]) == lax.axis_index("kv")
    gain = jnp.sum(jnp.where(mine, gains, 0.0), 0, keepdims=True)
    normed = centered * spread * gain
    gated = (gate * jax.nn.sigmoid(gate) * normed).astype(BF)
    out[...] = jnp.broadcast_to(gated[None], out.shape)


def output_kernel(gated, w_keep, w_got, tokens, own, out):
    heads = gated.shape[0] // 2
    t = lax.axis_index("tp")
    branch = 0.0
    width = own.shape[1]
    columns = pl.ds(pl.multiple_of(t * width, width), width)
    for group, w in ((t, w_keep[...]), (1 - t, w_got[:, columns])):
        lhs = jnp.concatenate([gated[2 * h + group] for h in range(heads)], 1)
        part = jnp.dot(lhs, w, preferred_element_type=F32)
        branch = branch + part.astype(BF).astype(F32)
    residual = (tokens[...].astype(F32) + branch).astype(BF)
    own[...] = residual
    out[...] = jnp.broadcast_to(residual[None], out.shape)


def mixer_kernel(residual, mlp_gain, w_up, w_down, out):
    blocks, rows, own = residual.shape
    width = blocks * own
    first = jnp.zeros((rows, own), F32)
    second = jnp.zeros((rows, own), F32)
    scaled, gain = [], []
    gains = mlp_gain[...].astype(F32)
    for i in range(blocks):
        wide = residual[i].astype(F32)
        first = first + wide
        second = second + wide * wide
        row = gains[i : i + 1]
        scaled.append((wide * row).astype(BF))
        gain.append(jnp.broadcast_to(row, wide.shape).astype(BF))
    lhs = jnp.concatenate([jnp.concatenate(scaled, 1), jnp.concatenate(gain, 1)], 0)
    up = jnp.dot(lhs, w_up[...], preferred_element_type=F32)
    average = jnp.sum(first, 1, keepdims=True) / width
    inverse = lax.rsqrt(jnp.sum(second, 1, keepdims=True) / width - average * average + EPS)
    hidden = inverse * (up[:rows] - average * up[rows : rows + 1])
    hidden = jnp.square(jnp.maximum(hidden, 0.0)).astype(BF)
    down = jnp.dot(hidden, w_down[...], preferred_element_type=F32)
    for i in range(blocks):
        out[i] = down[:, i * own : (i + 1) * own].astype(BF)


def final_kernel(pieces, own, out):
    total = jnp.sum(pieces[...].astype(F32), 0)
    out[...] = (own[...].astype(F32) + total).astype(BF)


VMEM = pl.BlockSpec(memory_space=pltpu.VMEM)
HBM = pl.BlockSpec(memory_space=pltpu.HBM)
ANY = pl.BlockSpec(memory_space=pl.ANY)


def in_hbm(*arrays):
    return [pltpu.with_memory_space_constraint(x, pltpu.HBM) for x in arrays]


def call(kernel, outs, in_specs, flops=0, bytes_accessed=0, scratch=(), limit=None, aliases={}):
    return pl.pallas_call(
        kernel,
        out_shape=outs,
        in_specs=in_specs,
        out_specs=jax.tree.map(lambda _: VMEM, outs),
        scratch_shapes=list(scratch),
        input_output_aliases=aliases,
        cost_estimate=pl.CostEstimate(
            flops=flops, bytes_accessed=bytes_accessed, transcendentals=0
        ),
        compiler_params=pltpu.CompilerParams(vmem_limit_bytes=limit),
    )


def make_kernels_on_device(kv, tp):
    def on_device(
        tokens,
        lengths,
        attn_gain,
        w_query,
        w_key,
        w_value,
        w_gate,
        decay_rate,
        key_cache,
        value_cache,
        head_gain,
        w_output,
        mlp_gain,
        w_up,
        w_down,
    ):
        S, own = tokens.shape
        H = decay_rate.shape[0]
        width = own * kv * tp
        qc, vc = H * HEAD_KEY, H * HEAD_VALUE
        swap = [(0, 1), (1, 0)]
        mib = 1 << 20
        sds = jax.ShapeDtypeStruct

        other = lax.ppermute(tokens, "tp", swap)
        w_got = lax.ppermute(w_output, "tp", swap)
        gain = attn_gain.reshape(-1, LANES)
        w_query, tokens, gain, length_rows, rates = call(
            first_load_kernel,
            (
                sds(w_query.shape, BF),
                sds(tokens.shape, BF),
                sds(gain.shape, BF),
                sds((S, LANES), jnp.int32),
                sds((H, LANES), F32),
            ),
            [HBM] * 5,
            flops=10**9,
            scratch=[
                pltpu.SMEM((S,), jnp.int32),
                pltpu.SMEM((H,), F32),
                pltpu.SemaphoreType.DMA((5,)),
            ],
            limit=2 * mib,
        )(*in_hbm(w_query, tokens, gain, lengths, decay_rate))
        columns = qc + 2 * LANES
        message_types = (sds((S, columns), F32), sds((S, columns), BF))
        state, message = call(
            query_kernel, message_types, [VMEM] * 4, limit=2 * mib
        )(tokens, other, gain, w_query)

        def exchange(message, stride):
            got = []
            for j in range(1, 4):
                pairs = [(i, i ^ (j * stride)) for i in range(kv)]
                got.append(lax.ppermute(message, "kv", pairs))
            return got

        got = exchange(message, 1)
        k_part, v_part, g_part, turn, weights, w_keep, keys = call(
            other_kernel,
            (
                sds((S + 8, qc), F32),
                sds((S + 8, vc), F32),
                sds((S + 8, vc), F32),
                sds((2, S, LANES), F32),
                sds((S, H, LANES), F32),
                sds((w_output.shape[0], own), BF),
                sds(key_cache.shape, BF),
            ),
            [ANY] + [VMEM] * 5 + [HBM] * 5,
            flops=10**9,
            scratch=[pltpu.VMEM(w.shape, BF) for w in (w_key, w_value, w_gate)]
            + [pltpu.SemaphoreType.DMA((4,)), pltpu.SemaphoreType.DMA((S // 2,))],
            limit=6 * mib,
        )(
            message,
            length_rows,
            rates,
            tokens,
            other,
            gain,
            *in_hbm(w_key, w_value, w_gate, w_output, key_cache),
        )

        stride = 4
        while stride < kv:
            state, message = call(
                middle_kernel, message_types, [VMEM] * 4, limit=2 * mib
            )(state, *got)
            got = exchange(message, stride)
            stride *= 4
        keys, values = call(
            cache_load_kernel,
            (sds(key_cache.shape, BF), sds(value_cache.shape, BF)),
            [ANY, VMEM] + [HBM] * 2 + [VMEM],
            flops=10**9,
            scratch=[pltpu.SemaphoreType.DMA((S,))] * 2,
            limit=2 * mib,
            aliases={4: 0},
        )(message, length_rows, *in_hbm(key_cache, value_cache), keys)

        pieces = call(
            functools.partial(attend_kernel, width),
            sds((H, 3 * S + S // 2, LANES), BF),
            [ANY] + [VMEM] * 12,
            scratch=[
                pltpu.VMEM((S, qc), F32),
                pltpu.VMEM((S, vc), F32),
                pltpu.SMEM((S,), jnp.int32),
            ],
            limit=4 * mib,
        )(w_got, length_rows, state, *got, k_part, v_part, g_part, turn, weights, keys, values)

        pieces = lax.all_to_all(pieces, "kv", 0, 0, tiled=True)
        gated = call(
            gate_kernel, sds((kv * tp, S, LANES), BF), [VMEM] * 2, limit=2 * mib
        )(pieces, head_gain.reshape(H, HEAD_VALUE))
        gated = lax.all_to_all(gated, ("kv", "tp"), 0, 0, tiled=True)
        residual, spread = call(
            output_kernel,
            (sds((S, own), BF), sds((kv * tp, S, own), BF)),
            [VMEM] * 4,
            limit=4 * mib,
        )(gated, w_keep, w_got, tokens)
        spread = lax.all_to_all(spread, ("kv", "tp"), 0, 0, tiled=True)
        down = call(
            mixer_kernel, sds((kv * tp, S, own), BF), [VMEM] * 4, limit=16 * mib
        )(spread, mlp_gain.reshape(-1, LANES), w_up, w_down)
        down = lax.all_to_all(down, ("kv", "tp"), 0, 0, tiled=True)
        return call(final_kernel, sds((S, own), BF), [VMEM] * 2, limit=2 * mib)(down, residual)

    return on_device


def solution(mesh):
    in_specs = (
        P(None, ("kv", "tp")),
        P(),
        P("kv"),
        P("kv", "tp"),
        P("kv", "tp"),
        P("kv", "tp"),
        P("kv", "tp"),
        P("tp"),
        P(None, "kv", "tp"),
        P(None, "kv", "tp"),
        P("tp"),
        P("tp", "kv"),
        P(),
        P(None, ("kv", "tp")),
        P(("kv", "tp"), None),
    )
    kv, tp = mesh.shape["kv"], mesh.shape["tp"]

    def on_device(*arrays):
        fits = tp == 2 and arrays[7].shape[0] == kv
        fits = fits and arrays[0].shape[1] == LANES == arrays[8].shape[1]
        make = make_kernels_on_device if fits else make_on_device
        return make(kv, tp)(*arrays)

    return jax.shard_map(
        on_device,
        mesh=mesh,
        in_specs=in_specs,
        out_specs=P(None, ("kv", "tp")),
        check_vma=False,
    )
```

```python
import functools
import math

import jax
import jax.numpy as jnp
from jax import lax
from jax.experimental import pallas as pl
from jax.experimental.pallas import tpu as pltpu
from jax.sharding import PartitionSpec as P


HEAD_KEY = 64
HEAD_VALUE = 128
EPS = 1e-05
THETA = 10000.0
LANES = 128

BF = jnp.bfloat16
F32 = jnp.float32


def split_two(x):
    high = x.astype(BF)
    return high, (x - high.astype(F32)).astype(BF)


def rotate(flat, cosine, sine):
    rows = flat.shape[0]
    grouped = flat.reshape(rows, -1, HEAD_KEY)
    half = HEAD_KEY // 2
    a, b = grouped[..., :half], grouped[..., half:]
    c, s = cosine[:, None, :], sine[:, None, :]
    return jnp.concatenate([a * c - b * s, b * c + a * s], -1).reshape(rows, -1)


def broadcast_gather(x, axes, size):
    spread = jnp.broadcast_to(x[None], (size,) + x.shape)
    return lax.all_to_all(spread, axes, 0, 0, tiled=True)


def make_on_device(kv, tp):
    def on_device(
        tokens,
        lengths,
        attn_gain,
        w_query,
        w_key,
        w_value,
        w_gate,
        decay_rate,
        key_cache,
        value_cache,
        head_gain,
        w_output,
        mlp_gain,
        w_up,
        w_down,
    ):
        S = tokens.shape[0]
        H = decay_rate.shape[0]
        span = key_cache.shape[1]
        width = tokens.shape[1] * kv * tp
        own = tokens.shape[1]
        kvi = lax.axis_index("kv")
        tpi = lax.axis_index("tp")
        groups = kv // H
        rows = S // groups

        if tp == 2:
            other = lax.ppermute(tokens, "tp", [(0, 1), (1, 0)])
            low = jnp.where(tpi == 0, tokens, other)
            high = jnp.where(tpi == 0, other, tokens)
            block = jnp.concatenate([low, high], 1)
        else:
            block = lax.all_gather(tokens, "tp", axis=1, tiled=True)
        wide = block.astype(F32)
        scaled = (wide * attn_gain.astype(F32)).astype(BF)
        lhs = jnp.concatenate([scaled, attn_gain[None, :]], 0)
        part_q = jnp.dot(lhs, w_query, preferred_element_type=F32)
        moments = jnp.stack([jnp.sum(wide, -1), jnp.sum(wide * wide, -1)], -1)

        small = jnp.concatenate([part_q[S], moments.reshape(-1)])
        q_sum = part_q[:S]
        stride = 1
        while stride < kv:
            count = 4 if kv % (stride * 4) == 0 else 2
            high, low = split_two(small)
            tail = jnp.concatenate([high, low])
            pad = -tail.shape[0] % S
            tail = jnp.pad(tail, (0, pad)).reshape(S, -1)
            message = jnp.concatenate([q_sum.astype(BF), tail], 1)
            for j in range(1, count):
                got = lax.ppermute(message, "kv", [(i, i ^ (j * stride)) for i in range(kv)])
                got = got.astype(F32)
                q_sum = q_sum + got[:, : q_sum.shape[1]]
                flat = got[:, q_sum.shape[1] :].reshape(-1)
                n = small.shape[0]
                small = small + flat[:n] + flat[n : 2 * n]
            stride *= count
        csum_q = small[: q_sum.shape[1]]
        moments = small[q_sum.shape[1] :].reshape(S, 2)
        average = moments[:, 0] / width
        inverse = lax.rsqrt(moments[:, 1] / width - average * average + EPS)

        half = HEAD_KEY // 2
        turn = jnp.power(THETA, -jnp.arange(half, dtype=F32) / half)
        angles = lengths.astype(F32)[:, None] * turn[None, :]
        q_plain = inverse[:, None] * (q_sum - average[:, None] * csum_q[None, :])
        queries = rotate(q_plain, jnp.cos(angles), jnp.sin(angles)).astype(BF)
        queries = queries.reshape(S, H, HEAD_KEY)

        def partial(w):
            p = jnp.dot(lhs, w, preferred_element_type=F32)
            return inverse[:, None] * (p[:S] - average[:, None] * p[S:])

        part_k = partial(w_key).reshape(S, H, HEAD_KEY)
        part_v = partial(w_value).reshape(S, H, HEAD_VALUE)
        part_g = partial(w_gate).reshape(S, H, HEAD_VALUE)
        part_score = jnp.sum(q_plain.reshape(S, H, HEAD_KEY) * part_k, -1) * HEAD_KEY ** (-0.5)

        keys = key_cache.reshape(S, span, H, HEAD_KEY)
        values = value_cache.reshape(S, span, H, HEAD_VALUE)
        scores = jnp.einsum("bhd,bjhd->bhj", queries, keys, preferred_element_type=F32)
        places = kvi * span + jnp.arange(span, dtype=jnp.int32)
        distance = jnp.maximum(lengths[:, None] - places[None, :], 0).astype(F32)
        live = (places[None, :] < lengths[:, None])[:, None, :]
        decays = jnp.where(
            live, jnp.exp(-decay_rate[None, :, None] * distance[:, None, :]), 0.0
        )
        coefficients = (scores * HEAD_KEY ** (-0.5) * decays).astype(BF)
        part_c = jnp.einsum("bhj,bjhe->bhe", coefficients, values, preferred_element_type=F32)

        high, low = split_two(part_score)
        pieces = jnp.concatenate(
            [
                part_c.astype(BF),
                part_v.astype(BF),
                part_g.astype(BF),
                high[..., None],
                low[..., None],
                jnp.zeros((S, H, 126), BF),
            ],
            -1,
        )
        pieces = pieces.transpose(1, 0, 2).reshape(kv, rows, 4 * HEAD_VALUE)
        mine = jnp.sum(
            lax.all_to_all(pieces, "kv", 0, 0, tiled=True).astype(F32), 0
        )
        cached, value, gate = (
            mine[:, i * HEAD_VALUE : (i + 1) * HEAD_VALUE] for i in range(3)
        )
        score = mine[:, 3 * HEAD_VALUE] + mine[:, 3 * HEAD_VALUE + 1]
        retained = cached + score[:, None] * value
        centered = retained - jnp.mean(retained, -1, keepdims=True)
        gain = lax.dynamic_slice(head_gain, ((kvi // groups) * HEAD_VALUE,), (HEAD_VALUE,))
        normed = (
            centered
            * lax.rsqrt(jnp.mean(centered * centered, -1, keepdims=True) + EPS)
            * gain.astype(F32)
        )
        gated = (jax.nn.silu(gate) * normed).astype(BF)
        gathered = broadcast_gather(gated, "kv", kv).reshape(H, S, HEAD_VALUE)
        gathered = gathered.transpose(1, 0, 2).reshape(S, H * HEAD_VALUE)
        part_b = jnp.dot(gathered, w_output, preferred_element_type=F32).astype(BF)
        part_b = part_b.reshape(S, tp, own).transpose(1, 0, 2)
        if tp == 2:
            keep = jnp.where(tpi == 0, part_b[0], part_b[1])
            send = jnp.where(tpi == 0, part_b[1], part_b[0])
            got = lax.ppermute(send, "tp", [(0, 1), (1, 0)])
            branch = keep.astype(F32) + got.astype(F32)
        else:
            branch = jnp.sum(
                lax.all_to_all(part_b, "tp", 0, 0, tiled=True).astype(F32), 0
            )
        own_residual = (tokens.astype(F32) + branch).astype(BF)

        residual = broadcast_gather(own_residual, ("kv", "tp"), kv * tp)
        residual = residual.transpose(1, 0, 2).reshape(S, width)
        wide = residual.astype(F32)
        scaled = (wide * mlp_gain.astype(F32)).astype(BF)
        lhs = jnp.concatenate([scaled, mlp_gain[None, :]], 0)
        up = jnp.dot(lhs, w_up, preferred_element_type=F32)
        average = jnp.sum(wide, -1) / width
        inverse = lax.rsqrt(jnp.sum(wide * wide, -1) / width - average * average + EPS)
        hidden = inverse[:, None] * (up[:S] - average[:, None] * up[S:])
        hidden = jnp.square(jax.nn.relu(hidden)).astype(BF)
        down = jnp.dot(hidden, w_down, preferred_element_type=F32).astype(BF)
        down = down.reshape(S, kv * tp, own).transpose(1, 0, 2)
        mixer = jnp.sum(
            lax.all_to_all(down, ("kv", "tp"), 0, 0, tiled=True).astype(F32), 0
        )
        return (own_residual.astype(F32) + mixer).astype(BF)

    return on_device


def lane_ids(rows):
    return lax.broadcasted_iota(jnp.int32, (rows, LANES), 1)


def row_ids(rows, columns=LANES):
    return lax.broadcasted_iota(jnp.int32, (rows, columns), 0)


def column_of(scalars, rows, dtype):
    ids = row_ids(rows)
    out = jnp.zeros((rows, LANES), dtype)
    for i in range(rows):
        out = jnp.where(ids == i, scalars[i].astype(dtype), out)
    return out


def gain_row(gain, rows):
    wide = gain[...].astype(F32)
    return jnp.concatenate(
        [jnp.broadcast_to(wide[i : i + 1], (rows, LANES)) for i in range(wide.shape[0])], 1
    )


def projection_rows(first, second, gain):
    t = lax.axis_index("tp")
    a, b = first[...].astype(F32), second[...].astype(F32)
    wide = jnp.concatenate([jnp.where(t == 0, a, b), jnp.where(t == 0, b, a)], 1)
    row = gain_row(gain, wide.shape[0])
    return jnp.concatenate([(wide * row).astype(BF), row.astype(BF)], 0), wide


def pack(q, csum, moments, message):
    columns = q.shape[1]
    half = csum.shape[0]
    message[:, :columns] = q.astype(BF)
    high = csum.astype(BF)
    low = (csum - high.astype(F32)).astype(BF)
    message[:, columns : columns + LANES] = jnp.concatenate([high, low], 0)
    high = moments.astype(BF).astype(F32)
    low = moments - high
    lanes = lane_ids(q.shape[0])
    both = jnp.where(lanes < 2, high, jnp.where(lanes < 4, pltpu.roll(low, 2, 1), 0.0))
    message[:, columns + LANES :] = both.astype(BF)
    assert 2 * half == q.shape[0]


def unpack_sum(state, messages):
    rows, total = state.shape
    columns = total - 2 * LANES
    half = rows // 2
    q = state[:, :columns]
    csum = state[:half, columns : columns + LANES]
    moments = state[:, columns + LANES :]
    for m in messages:
        q = q + m[:, :columns].astype(F32)
        c = m[:, columns : columns + LANES].astype(F32)
        csum = csum + c[:half] + c[half:]
        v = m[:, columns + LANES :].astype(F32)
        moments = moments + v + pltpu.roll(v, LANES - 2, 1)
    return q, csum, jnp.where(lane_ids(rows) < 2, moments, 0.0)


def store_state(q, csum, moments, state):
    columns = q.shape[1]
    state[:, :columns] = q
    state[:, columns : columns + LANES] = jnp.concatenate([csum, jnp.zeros_like(csum)], 0)
    state[:, columns + LANES :] = moments


def first_load_kernel(
    w_query,
    tokens,
    gain,
    lengths,
    decay,
    w_out,
    tokens_out,
    gain_out,
    length_out,
    rate_out,
    length_scalars,
    decay_scalars,
    sems,
):
    pairs = (
        (lengths, length_scalars),
        (decay, decay_scalars),
        (tokens, tokens_out),
        (gain, gain_out),
        (w_query, w_out),
    )
    copies = [pltpu.make_async_copy(a, b, sems.at[i]) for i, (a, b) in enumerate(pairs)]
    for copy in copies:
        copy.start()
    copies[0].wait()
    length_out[...] = column_of(length_scalars, length_out.shape[0], jnp.int32)
    copies[1].wait()
    rate_out[...] = column_of(decay_scalars, rate_out.shape[0], F32)
    for copy in copies[2:]:
        copy.wait()


def live_scalars(lengths, base):
    values = lengths[...]
    return [values[s, 0] > base for s in range(values.shape[0])]


def when_live(flags, copies, act):
    for flag, copy in zip(flags, copies):

        @pl.when(flag)
        def _():
            act(copy)


def copies_of(source, target, sems, first, count):
    return [
        pltpu.make_async_copy(source.at[s], target.at[s], sems.at[s - first])
        for s in range(first, first + count)
    ]


def cache_load_kernel(
    after, lengths, keys, values, keys_begun, keys_out, values_out, key_sems, value_sems
):
    rows, span = keys.shape[:2]
    live = live_scalars(lengths, lax.axis_index("kv") * span)
    half = rows // 2
    copies = copies_of(keys, keys_out, key_sems, half, rows - half)
    copies += copies_of(values, values_out, value_sems, 0, rows)
    when_live(live[half:] + live, copies, lambda copy: copy.start())
    when_live(live[half:] + live, copies, lambda copy: copy.wait())


def query_kernel(first, second, gain, w_query, state, message):
    lhs, wide = projection_rows(first, second, gain)
    rows = wide.shape[0]
    product = jnp.dot(lhs, w_query[...], preferred_element_type=F32)
    half = rows // 2
    ids = row_ids(half)
    csum = jnp.zeros((half, LANES), F32)
    for i in range(product.shape[1] // LANES):
        csum = jnp.where(
            ids == i, product[rows : rows + half, i * LANES : (i + 1) * LANES], csum
        )
    lanes = lane_ids(rows)
    first_sum = jnp.sum(wide, 1, keepdims=True)
    second_sum = jnp.sum(wide * wide, 1, keepdims=True)
    moments = jnp.where(lanes == 0, first_sum, jnp.where(lanes == 1, second_sum, 0.0))
    store_state(product[:rows], csum, moments, state)
    pack(product[:rows], csum, moments, message)


def middle_kernel(old, m1, m2, m3, state, message):
    q, csum, moments = unpack_sum(old, (m1, m2, m3))
    store_state(q, csum, moments, state)
    pack(q, csum, moments, message)


def other_kernel(
    after,
    lengths,
    rates,
    first,
    second,
    gain,
    w_key,
    w_value,
    w_gate,
    w_output,
    keys,
    k_out,
    v_out,
    g_out,
    turn,
    weights,
    w_keep,
    keys_out,
    key_buffer,
    value_buffer,
    gate_buffer,
    sems,
    cache_sems,
):
    own = w_keep.shape[1]
    kept = pl.ds(pl.multiple_of(lax.axis_index("tp") * own, own), own)
    buffers = (key_buffer, value_buffer, gate_buffer)
    pairs = (
        (w_key, key_buffer),
        (w_value, value_buffer),
        (w_gate, gate_buffer),
        (w_output.at[:, kept], w_keep),
    )
    copies = [pltpu.make_async_copy(a, b, sems.at[i]) for i, (a, b) in enumerate(pairs)]
    for copy in copies:
        copy.start()
    lhs, wide = projection_rows(first, second, gain)
    rows = wide.shape[0]
    live = live_scalars(lengths, lax.axis_index("kv") * keys.shape[1])[: rows // 2]
    caches = copies_of(keys, keys_out, cache_sems, 0, rows // 2)
    when_live(live, caches, lambda copy: copy.start())
    half = HEAD_KEY // 2
    entry = (lane_ids(rows) % half).astype(F32)
    inverse = jnp.exp(entry * (-math.log(THETA) / half))
    angle = lengths[...].astype(F32) * inverse
    turn[0] = jnp.cos(angle)
    turn[1] = jnp.sin(angle)
    heads = rates.shape[0]
    places = lax.axis_index("kv") * LANES + lane_ids(heads)
    rate = rates[...]
    for s in range(rows):
        distance = jnp.broadcast_to(lengths[s : s + 1, :], (heads, LANES)) - places
        weight = jnp.exp(-rate * jnp.maximum(distance, 0).astype(F32)) * HEAD_KEY ** (-0.5)
        weights[s] = jnp.where(distance > 0, weight, 0.0)
    for copy, buffer, out in zip(copies, buffers, (k_out, v_out, g_out)):
        copy.wait()
        product = jnp.dot(lhs, buffer[...], preferred_element_type=F32)
        out[...] = product[: rows + 8]
    for copy in copies[len(buffers) :]:
        copy.wait()
    when_live(live, caches, lambda copy: copy.wait())


def attend_kernel(
    width,
    after,
    lengths,
    old,
    m1,
    m2,
    m3,
    k_part,
    v_part,
    g_part,
    turn,
    weights,
    keys,
    values,
    out,
    query_rows,
    plain_rows,
    cached,
    order,
):
    rows, span, key_columns = keys.shape
    heads = key_columns // HEAD_KEY
    q, csum, moments = unpack_sum(old, (m1, m2, m3))
    average = moments[:, 0:1] / width
    inverse = lax.rsqrt(moments[:, 1:2] / width - average * average + EPS)
    lanes = lane_ids(rows)
    in_first = lanes % HEAD_KEY < HEAD_KEY // 2
    low_head = lanes < HEAD_KEY
    top = rows // 2
    cosine, sine = turn[0], turn[1]
    for i in range(key_columns // LANES):
        cut = slice(i * LANES, (i + 1) * LANES)
        plain = inverse * (q[:, cut] - average * csum[i : i + 1])
        partner = jnp.where(
            in_first,
            -pltpu.roll(plain, LANES - HEAD_KEY // 2, 1),
            pltpu.roll(plain, HEAD_KEY // 2, 1),
        )
        plain_rows[:, cut] = plain
        query_rows[:, cut] = (plain * cosine + partner * sine).astype(BF).astype(F32)

    def normed(part, cut):
        return inverse * (part[:rows, cut] - average * part[rows : rows + 1, cut])

    def side(i):
        cut = slice(i * LANES, (i + 1) * LANES)
        both = plain_rows[:, cut] * normed(k_part, cut) * HEAD_KEY ** (-0.5)
        for j in range(2):
            h = 2 * i + j
            picked = jnp.where(low_head == (j == 0), both, 0.0)
            score = jnp.sum(picked, 1, keepdims=True)
            high = score.astype(BF).astype(F32)
            low = score - high
            folded = jnp.where(
                lanes[:top] < HEAD_KEY,
                jnp.where(in_first[:top], high[:top], low[:top]),
                jnp.where(in_first[:top], high[top:], low[top:]),
            )
            out[h, 3 * rows :, :] = folded.astype(BF)
            cut = slice(h * LANES, (h + 1) * LANES)
            for place, part in ((1, v_part), (2, g_part)):
                out[h, place * rows : (place + 1) * rows, :] = normed(part, cut).astype(BF)

    head_of_key = lax.broadcasted_iota(jnp.int32, (heads, key_columns), 1) // HEAD_KEY
    own_key = head_of_key == row_ids(heads, key_columns)
    value_columns = heads * HEAD_VALUE
    head_of_value = lax.broadcasted_iota(jnp.int32, (heads, value_columns), 1) // HEAD_VALUE
    own_value = head_of_value == row_ids(heads, value_columns)
    live = live_scalars(lengths, lax.axis_index("kv") * span)
    count = jnp.int32(0)
    for s in range(rows):
        order[count] = s
        count = count + live[s].astype(jnp.int32)

    def one(s, is_live):
        row = pl.ds(s, 1)
        spread = jnp.broadcast_to(query_rows[row, :], (heads, key_columns))
        query = jnp.where(own_key, spread, 0.0).astype(BF)
        scores = lax.dot_general(
            query, keys[s], (((1,), (1,)), ((), ())), preferred_element_type=F32
        )
        weight = weights[s]
        coefficients = jnp.where(weight > 0.0, scores * weight, 0.0).astype(BF)
        product = jnp.dot(coefficients, values[s], preferred_element_type=F32)
        kept = jnp.logical_and(own_value, is_live)
        cached[row, :] = jnp.sum(jnp.where(kept, product, 0.0), 0, keepdims=True)

    quarter = rows // 4
    pairs = heads // 2
    for most in range(quarter, rows + 1, quarter):
        least = most - quarter if most > quarter else -1

        @pl.when(jnp.logical_and(count > least, count <= most))
        def _():
            if most < rows:
                cached[...] = jnp.zeros_like(cached)
            done = 0
            for i in range(most):
                if most == rows:
                    one(i, live[i])
                else:
                    one(order[jnp.minimum(i, jnp.maximum(count - 1, 0))], count > 0)
                while done * most < (i + 1) * pairs:
                    side(done)
                    done += 1

    for h in range(heads):
        out[h, :rows, :] = cached[:, h * LANES : (h + 1) * LANES].astype(BF)


def gate_kernel(pieces, head_gain, out):
    rows = out.shape[1]
    total = jnp.sum(pieces[...].astype(F32), 0)
    cached, value, gate = (total[i * rows : (i + 1) * rows] for i in range(3))
    folded = total[3 * rows :]
    half = HEAD_KEY // 2
    score = jnp.concatenate(
        [folded[:, i : i + 1] + folded[:, i + half : i + half + 1] for i in (0, HEAD_KEY)], 0
    )
    retained = cached + score * value
    centered = retained - jnp.mean(retained, -1, keepdims=True)
    spread = lax.rsqrt(jnp.mean(centered * centered, -1, keepdims=True) + EPS)
    gains = head_gain[...].astype(F32)
    mine = row_ids(gains.shape[0]) == lax.axis_index("kv")
    gain = jnp.sum(jnp.where(mine, gains, 0.0), 0, keepdims=True)
    normed = centered * spread * gain
    gated = (gate * jax.nn.sigmoid(gate) * normed).astype(BF)
    out[...] = jnp.broadcast_to(gated[None], out.shape)


def output_kernel(gated, w_keep, w_got, tokens, own, out):
    heads = gated.shape[0] // 2
    t = lax.axis_index("tp")
    branch = 0.0
    width = own.shape[1]
    columns = pl.ds(pl.multiple_of(t * width, width), width)
    for group, w in ((t, w_keep[...]), (1 - t, w_got[:, columns])):
        lhs = jnp.concatenate([gated[2 * h + group] for h in range(heads)], 1)
        part = jnp.dot(lhs, w, preferred_element_type=F32)
        branch = branch + part.astype(BF).astype(F32)
    residual = (tokens[...].astype(F32) + branch).astype(BF)
    own[...] = residual
    out[...] = jnp.broadcast_to(residual[None], out.shape)


def mixer_kernel(residual, mlp_gain, w_up, w_down, out):
    blocks, rows, own = residual.shape
    width = blocks * own
    first = jnp.zeros((rows, own), F32)
    second = jnp.zeros((rows, own), F32)
    scaled, gain = [], []
    gains = mlp_gain[...].astype(F32)
    for i in range(blocks):
        wide = residual[i].astype(F32)
        first = first + wide
        second = second + wide * wide
        row = gains[i : i + 1]
        scaled.append((wide * row).astype(BF))
        gain.append(jnp.broadcast_to(row, wide.shape).astype(BF))
    lhs = jnp.concatenate([jnp.concatenate(scaled, 1), jnp.concatenate(gain, 1)], 0)
    up = jnp.dot(lhs, w_up[...], preferred_element_type=F32)
    average = jnp.sum(first, 1, keepdims=True) / width
    inverse = lax.rsqrt(jnp.sum(second, 1, keepdims=True) / width - average * average + EPS)
    hidden = inverse * (up[:rows] - average * up[rows : rows + 1])
    hidden = jnp.square(jnp.maximum(hidden, 0.0)).astype(BF)
    down = jnp.dot(hidden, w_down[...], preferred_element_type=F32)
    for i in range(blocks):
        out[i] = down[:, i * own : (i + 1) * own].astype(BF)


def final_kernel(pieces, own, out):
    total = jnp.sum(pieces[...].astype(F32), 0)
    out[...] = (own[...].astype(F32) + total).astype(BF)


VMEM = pl.BlockSpec(memory_space=pltpu.VMEM)
HBM = pl.BlockSpec(memory_space=pltpu.HBM)
ANY = pl.BlockSpec(memory_space=pl.ANY)


def in_hbm(*arrays):
    return [pltpu.with_memory_space_constraint(x, pltpu.HBM) for x in arrays]


def call(kernel, outs, in_specs, flops=0, bytes_accessed=0, scratch=(), limit=None, aliases={}):
    return pl.pallas_call(
        kernel,
        out_shape=outs,
        in_specs=in_specs,
        out_specs=jax.tree.map(lambda _: VMEM, outs),
        scratch_shapes=list(scratch),
        input_output_aliases=aliases,
        cost_estimate=pl.CostEstimate(
            flops=flops, bytes_accessed=bytes_accessed, transcendentals=0
        ),
        compiler_params=pltpu.CompilerParams(vmem_limit_bytes=limit),
    )


def make_kernels_on_device(kv, tp):
    def on_device(
        tokens,
        lengths,
        attn_gain,
        w_query,
        w_key,
        w_value,
        w_gate,
        decay_rate,
        key_cache,
        value_cache,
        head_gain,
        w_output,
        mlp_gain,
        w_up,
        w_down,
    ):
        S, own = tokens.shape
        H = decay_rate.shape[0]
        width = own * kv * tp
        qc, vc = H * HEAD_KEY, H * HEAD_VALUE
        swap = [(0, 1), (1, 0)]
        mib = 1 << 20
        sds = jax.ShapeDtypeStruct

        other = lax.ppermute(tokens, "tp", swap)
        w_got = lax.ppermute(w_output, "tp", swap)
        gain = attn_gain.reshape(-1, LANES)
        w_query, tokens, gain, length_rows, rates = call(
            first_load_kernel,
            (
                sds(w_query.shape, BF),
                sds(tokens.shape, BF),
                sds(gain.shape, BF),
                sds((S, LANES), jnp.int32),
                sds((H, LANES), F32),
            ),
            [HBM] * 5,
            flops=10**9,
            scratch=[
                pltpu.SMEM((S,), jnp.int32),
                pltpu.SMEM((H,), F32),
                pltpu.SemaphoreType.DMA((5,)),
            ],
            limit=2 * mib,
        )(*in_hbm(w_query, tokens, gain, lengths, decay_rate))
        columns = qc + 2 * LANES
        message_types = (sds((S, columns), F32), sds((S, columns), BF))
        state, message = call(
            query_kernel, message_types, [VMEM] * 4, limit=2 * mib
        )(tokens, other, gain, w_query)

        def exchange(message, stride):
            got = []
            for j in range(1, 4):
                pairs = [(i, i ^ (j * stride)) for i in range(kv)]
                got.append(lax.ppermute(message, "kv", pairs))
            return got

        got = exchange(message, 1)
        k_part, v_part, g_part, turn, weights, w_keep, keys = call(
            other_kernel,
            (
                sds((S + 8, qc), F32),
                sds((S + 8, vc), F32),
                sds((S + 8, vc), F32),
                sds((2, S, LANES), F32),
                sds((S, H, LANES), F32),
                sds((w_output.shape[0], own), BF),
                sds(key_cache.shape, BF),
            ),
            [ANY] + [VMEM] * 5 + [HBM] * 5,
            flops=10**9,
            scratch=[pltpu.VMEM(w.shape, BF) for w in (w_key, w_value, w_gate)]
            + [pltpu.SemaphoreType.DMA((4,)), pltpu.SemaphoreType.DMA((S // 2,))],
            limit=6 * mib,
        )(
            message,
            length_rows,
            rates,
            tokens,
            other,
            gain,
            *in_hbm(w_key, w_value, w_gate, w_output, key_cache),
        )

        stride = 4
        while stride < kv:
            state, message = call(
                middle_kernel, message_types, [VMEM] * 4, limit=2 * mib
            )(state, *got)
            got = exchange(message, stride)
            stride *= 4
        keys, values = call(
            cache_load_kernel,
            (sds(key_cache.shape, BF), sds(value_cache.shape, BF)),
            [ANY, VMEM] + [HBM] * 2 + [VMEM],
            flops=10**9,
            scratch=[pltpu.SemaphoreType.DMA((S,))] * 2,
            limit=2 * mib,
            aliases={4: 0},
        )(message, length_rows, *in_hbm(key_cache, value_cache), keys)

        pieces = call(
            functools.partial(attend_kernel, width),
            sds((H, 3 * S + S // 2, LANES), BF),
            [ANY] + [VMEM] * 12,
            scratch=[
                pltpu.VMEM((S, qc), F32),
                pltpu.VMEM((S, qc), F32),
                pltpu.VMEM((S, vc), F32),
                pltpu.SMEM((S,), jnp.int32),
            ],
            limit=4 * mib,
        )(w_got, length_rows, state, *got, k_part, v_part, g_part, turn, weights, keys, values)

        pieces = lax.all_to_all(pieces, "kv", 0, 0, tiled=True)
        gated = call(
            gate_kernel, sds((kv * tp, S, LANES), BF), [VMEM] * 2, limit=2 * mib
        )(pieces, head_gain.reshape(H, HEAD_VALUE))
        gated = lax.all_to_all(gated, ("kv", "tp"), 0, 0, tiled=True)
        residual, spread = call(
            output_kernel,
            (sds((S, own), BF), sds((kv * tp, S, own), BF)),
            [VMEM] * 4,
            limit=4 * mib,
        )(gated, w_keep, w_got, tokens)
        spread = lax.all_to_all(spread, ("kv", "tp"), 0, 0, tiled=True)
        down = call(
            mixer_kernel, sds((kv * tp, S, own), BF), [VMEM] * 4, limit=16 * mib
        )(spread, mlp_gain.reshape(-1, LANES), w_up, w_down)
        down = lax.all_to_all(down, ("kv", "tp"), 0, 0, tiled=True)
        return call(final_kernel, sds((S, own), BF), [VMEM] * 2, limit=2 * mib)(down, residual)

    return on_device


def solution(mesh):
    in_specs = (
        P(None, ("kv", "tp")),
        P(),
        P("kv"),
        P("kv", "tp"),
        P("kv", "tp"),
        P("kv", "tp"),
        P("kv", "tp"),
        P("tp"),
        P(None, "kv", "tp"),
        P(None, "kv", "tp"),
        P("tp"),
        P("tp", "kv"),
        P(),
        P(None, ("kv", "tp")),
        P(("kv", "tp"), None),
    )
    kv, tp = mesh.shape["kv"], mesh.shape["tp"]

    def on_device(*arrays):
        fits = tp == 2 and arrays[7].shape[0] == kv
        fits = fits and arrays[0].shape[1] == LANES == arrays[8].shape[1]
        make = make_kernels_on_device if fits else make_on_device
        return make(kv, tp)(*arrays)

    return jax.shard_map(
        on_device,
        mesh=mesh,
        in_specs=in_specs,
        out_specs=P(None, ("kv", "tp")),
        check_vma=False,
    )
```

```python
import functools
import math

import jax
import jax.numpy as jnp
from jax import lax
from jax.experimental import pallas as pl
from jax.experimental.pallas import tpu as pltpu
from jax.sharding import PartitionSpec as P


HEAD_KEY = 64
HEAD_VALUE = 128
EPS = 1e-05
THETA = 10000.0
LANES = 128

BF = jnp.bfloat16
F32 = jnp.float32


def split_two(x):
    high = x.astype(BF)
    return high, (x - high.astype(F32)).astype(BF)


def rotate(flat, cosine, sine):
    rows = flat.shape[0]
    grouped = flat.reshape(rows, -1, HEAD_KEY)
    half = HEAD_KEY // 2
    a, b = grouped[..., :half], grouped[..., half:]
    c, s = cosine[:, None, :], sine[:, None, :]
    return jnp.concatenate([a * c - b * s, b * c + a * s], -1).reshape(rows, -1)


def broadcast_gather(x, axes, size):
    spread = jnp.broadcast_to(x[None], (size,) + x.shape)
    return lax.all_to_all(spread, axes, 0, 0, tiled=True)


def make_on_device(kv, tp):
    def on_device(
        tokens,
        lengths,
        attn_gain,
        w_query,
        w_key,
        w_value,
        w_gate,
        decay_rate,
        key_cache,
        value_cache,
        head_gain,
        w_output,
        mlp_gain,
        w_up,
        w_down,
    ):
        S = tokens.shape[0]
        H = decay_rate.shape[0]
        span = key_cache.shape[1]
        width = tokens.shape[1] * kv * tp
        own = tokens.shape[1]
        kvi = lax.axis_index("kv")
        tpi = lax.axis_index("tp")
        groups = kv // H
        rows = S // groups

        if tp == 2:
            other = lax.ppermute(tokens, "tp", [(0, 1), (1, 0)])
            low = jnp.where(tpi == 0, tokens, other)
            high = jnp.where(tpi == 0, other, tokens)
            block = jnp.concatenate([low, high], 1)
        else:
            block = lax.all_gather(tokens, "tp", axis=1, tiled=True)
        wide = block.astype(F32)
        scaled = (wide * attn_gain.astype(F32)).astype(BF)
        lhs = jnp.concatenate([scaled, attn_gain[None, :]], 0)
        part_q = jnp.dot(lhs, w_query, preferred_element_type=F32)
        moments = jnp.stack([jnp.sum(wide, -1), jnp.sum(wide * wide, -1)], -1)

        small = jnp.concatenate([part_q[S], moments.reshape(-1)])
        q_sum = part_q[:S]
        stride = 1
        while stride < kv:
            count = 4 if kv % (stride * 4) == 0 else 2
            high, low = split_two(small)
            tail = jnp.concatenate([high, low])
            pad = -tail.shape[0] % S
            tail = jnp.pad(tail, (0, pad)).reshape(S, -1)
            message = jnp.concatenate([q_sum.astype(BF), tail], 1)
            for j in range(1, count):
                got = lax.ppermute(message, "kv", [(i, i ^ (j * stride)) for i in range(kv)])
                got = got.astype(F32)
                q_sum = q_sum + got[:, : q_sum.shape[1]]
                flat = got[:, q_sum.shape[1] :].reshape(-1)
                n = small.shape[0]
                small = small + flat[:n] + flat[n : 2 * n]
            stride *= count
        csum_q = small[: q_sum.shape[1]]
        moments = small[q_sum.shape[1] :].reshape(S, 2)
        average = moments[:, 0] / width
        inverse = lax.rsqrt(moments[:, 1] / width - average * average + EPS)

        half = HEAD_KEY // 2
        turn = jnp.power(THETA, -jnp.arange(half, dtype=F32) / half)
        angles = lengths.astype(F32)[:, None] * turn[None, :]
        q_plain = inverse[:, None] * (q_sum - average[:, None] * csum_q[None, :])
        queries = rotate(q_plain, jnp.cos(angles), jnp.sin(angles)).astype(BF)
        queries = queries.reshape(S, H, HEAD_KEY)

        def partial(w):
            p = jnp.dot(lhs, w, preferred_element_type=F32)
            return inverse[:, None] * (p[:S] - average[:, None] * p[S:])

        part_k = partial(w_key).reshape(S, H, HEAD_KEY)
        part_v = partial(w_value).reshape(S, H, HEAD_VALUE)
        part_g = partial(w_gate).reshape(S, H, HEAD_VALUE)
        part_score = jnp.sum(q_plain.reshape(S, H, HEAD_KEY) * part_k, -1) * HEAD_KEY ** (-0.5)

        keys = key_cache.reshape(S, span, H, HEAD_KEY)
        values = value_cache.reshape(S, span, H, HEAD_VALUE)
        scores = jnp.einsum("bhd,bjhd->bhj", queries, keys, preferred_element_type=F32)
        places = kvi * span + jnp.arange(span, dtype=jnp.int32)
        distance = jnp.maximum(lengths[:, None] - places[None, :], 0).astype(F32)
        live = (places[None, :] < lengths[:, None])[:, None, :]
        decays = jnp.where(
            live, jnp.exp(-decay_rate[None, :, None] * distance[:, None, :]), 0.0
        )
        coefficients = (scores * HEAD_KEY ** (-0.5) * decays).astype(BF)
        part_c = jnp.einsum("bhj,bjhe->bhe", coefficients, values, preferred_element_type=F32)

        high, low = split_two(part_score)
        pieces = jnp.concatenate(
            [
                part_c.astype(BF),
                part_v.astype(BF),
                part_g.astype(BF),
                high[..., None],
                low[..., None],
                jnp.zeros((S, H, 126), BF),
            ],
            -1,
        )
        pieces = pieces.transpose(1, 0, 2).reshape(kv, rows, 4 * HEAD_VALUE)
        mine = jnp.sum(
            lax.all_to_all(pieces, "kv", 0, 0, tiled=True).astype(F32), 0
        )
        cached, value, gate = (
            mine[:, i * HEAD_VALUE : (i + 1) * HEAD_VALUE] for i in range(3)
        )
        score = mine[:, 3 * HEAD_VALUE] + mine[:, 3 * HEAD_VALUE + 1]
        retained = cached + score[:, None] * value
        centered = retained - jnp.mean(retained, -1, keepdims=True)
        gain = lax.dynamic_slice(head_gain, ((kvi // groups) * HEAD_VALUE,), (HEAD_VALUE,))
        normed = (
            centered
            * lax.rsqrt(jnp.mean(centered * centered, -1, keepdims=True) + EPS)
            * gain.astype(F32)
        )
        gated = (jax.nn.silu(gate) * normed).astype(BF)
        gathered = broadcast_gather(gated, "kv", kv).reshape(H, S, HEAD_VALUE)
        gathered = gathered.transpose(1, 0, 2).reshape(S, H * HEAD_VALUE)
        part_b = jnp.dot(gathered, w_output, preferred_element_type=F32).astype(BF)
        part_b = part_b.reshape(S, tp, own).transpose(1, 0, 2)
        if tp == 2:
            keep = jnp.where(tpi == 0, part_b[0], part_b[1])
            send = jnp.where(tpi == 0, part_b[1], part_b[0])
            got = lax.ppermute(send, "tp", [(0, 1), (1, 0)])
            branch = keep.astype(F32) + got.astype(F32)
        else:
            branch = jnp.sum(
                lax.all_to_all(part_b, "tp", 0, 0, tiled=True).astype(F32), 0
            )
        own_residual = (tokens.astype(F32) + branch).astype(BF)

        residual = broadcast_gather(own_residual, ("kv", "tp"), kv * tp)
        residual = residual.transpose(1, 0, 2).reshape(S, width)
        wide = residual.astype(F32)
        scaled = (wide * mlp_gain.astype(F32)).astype(BF)
        lhs = jnp.concatenate([scaled, mlp_gain[None, :]], 0)
        up = jnp.dot(lhs, w_up, preferred_element_type=F32)
        average = jnp.sum(wide, -1) / width
        inverse = lax.rsqrt(jnp.sum(wide * wide, -1) / width - average * average + EPS)
        hidden = inverse[:, None] * (up[:S] - average[:, None] * up[S:])
        hidden = jnp.square(jax.nn.relu(hidden)).astype(BF)
        down = jnp.dot(hidden, w_down, preferred_element_type=F32).astype(BF)
        down = down.reshape(S, kv * tp, own).transpose(1, 0, 2)
        mixer = jnp.sum(
            lax.all_to_all(down, ("kv", "tp"), 0, 0, tiled=True).astype(F32), 0
        )
        return (own_residual.astype(F32) + mixer).astype(BF)

    return on_device


def lane_ids(rows):
    return lax.broadcasted_iota(jnp.int32, (rows, LANES), 1)


def row_ids(rows, columns=LANES):
    return lax.broadcasted_iota(jnp.int32, (rows, columns), 0)


def column_of(scalars, rows, dtype):
    ids = row_ids(rows)
    out = jnp.zeros((rows, LANES), dtype)
    for i in range(rows):
        out = jnp.where(ids == i, scalars[i].astype(dtype), out)
    return out


def gain_row(gain, rows):
    wide = gain[...].astype(F32)
    return jnp.concatenate(
        [jnp.broadcast_to(wide[i : i + 1], (rows, LANES)) for i in range(wide.shape[0])], 1
    )


def projection_rows(first, second, gain):
    t = lax.axis_index("tp")
    a, b = first[...].astype(F32), second[...].astype(F32)
    wide = jnp.concatenate([jnp.where(t == 0, a, b), jnp.where(t == 0, b, a)], 1)
    row = gain_row(gain, wide.shape[0])
    return jnp.concatenate([(wide * row).astype(BF), row.astype(BF)], 0), wide


def pack(q, csum, moments, message):
    columns = q.shape[1]
    half = csum.shape[0]
    message[:, :columns] = q.astype(BF)
    high = csum.astype(BF)
    low = (csum - high.astype(F32)).astype(BF)
    message[:, columns : columns + LANES] = jnp.concatenate([high, low], 0)
    high = moments.astype(BF).astype(F32)
    low = moments - high
    lanes = lane_ids(q.shape[0])
    both = jnp.where(lanes < 2, high, jnp.where(lanes < 4, pltpu.roll(low, 2, 1), 0.0))
    message[:, columns + LANES :] = both.astype(BF)
    assert 2 * half == q.shape[0]


def unpack_sum(state, messages):
    rows, total = state.shape
    columns = total - 2 * LANES
    half = rows // 2
    q = state[:, :columns]
    csum = state[:half, columns : columns + LANES]
    moments = state[:, columns + LANES :]
    for m in messages:
        q = q + m[:, :columns].astype(F32)
        c = m[:, columns : columns + LANES].astype(F32)
        csum = csum + c[:half] + c[half:]
        v = m[:, columns + LANES :].astype(F32)
        moments = moments + v + pltpu.roll(v, LANES - 2, 1)
    return q, csum, jnp.where(lane_ids(rows) < 2, moments, 0.0)


def store_state(q, csum, moments, state):
    columns = q.shape[1]
    state[:, :columns] = q
    state[:, columns : columns + LANES] = jnp.concatenate([csum, jnp.zeros_like(csum)], 0)
    state[:, columns + LANES :] = moments


def first_load_kernel(
    w_query,
    tokens,
    gain,
    lengths,
    decay,
    w_out,
    tokens_out,
    gain_out,
    length_out,
    rate_out,
    length_scalars,
    decay_scalars,
    sems,
):
    pairs = (
        (lengths, length_scalars),
        (decay, decay_scalars),
        (tokens, tokens_out),
        (gain, gain_out),
        (w_query, w_out),
    )
    copies = [pltpu.make_async_copy(a, b, sems.at[i]) for i, (a, b) in enumerate(pairs)]
    for copy in copies:
        copy.start()
    copies[0].wait()
    length_out[...] = column_of(length_scalars, length_out.shape[0], jnp.int32)
    copies[1].wait()
    rate_out[...] = column_of(decay_scalars, rate_out.shape[0], F32)
    for copy in copies[2:]:
        copy.wait()


def live_scalars(lengths, base):
    values = lengths[...]
    return [values[s, 0] > base for s in range(values.shape[0])]


def when_live(flags, copies, act):
    for flag, copy in zip(flags, copies):

        @pl.when(flag)
        def _():
            act(copy)


def copies_of(source, target, sems, first, count):
    return [
        pltpu.make_async_copy(source.at[s], target.at[s], sems.at[s - first])
        for s in range(first, first + count)
    ]


def cache_load_kernel(
    after, lengths, keys, values, keys_begun, keys_out, values_out, key_sems, value_sems
):
    rows, span = keys.shape[:2]
    live = live_scalars(lengths, lax.axis_index("kv") * span)
    half = rows * 3 // 4
    copies = copies_of(keys, keys_out, key_sems, half, rows - half)
    copies += copies_of(values, values_out, value_sems, 0, rows)
    when_live(live[half:] + live, copies, lambda copy: copy.start())
    when_live(live[half:] + live, copies, lambda copy: copy.wait())


def query_kernel(first, second, gain, w_query, state, message):
    lhs, wide = projection_rows(first, second, gain)
    rows = wide.shape[0]
    product = jnp.dot(lhs, w_query[...], preferred_element_type=F32)
    half = rows // 2
    ids = row_ids(half)
    csum = jnp.zeros((half, LANES), F32)
    for i in range(product.shape[1] // LANES):
        csum = jnp.where(
            ids == i, product[rows : rows + half, i * LANES : (i + 1) * LANES], csum
        )
    lanes = lane_ids(rows)
    first_sum = jnp.sum(wide, 1, keepdims=True)
    second_sum = jnp.sum(wide * wide, 1, keepdims=True)
    moments = jnp.where(lanes == 0, first_sum, jnp.where(lanes == 1, second_sum, 0.0))
    store_state(product[:rows], csum, moments, state)
    pack(product[:rows], csum, moments, message)


def middle_kernel(old, m1, m2, m3, state, message):
    q, csum, moments = unpack_sum(old, (m1, m2, m3))
    store_state(q, csum, moments, state)
    pack(q, csum, moments, message)


def other_kernel(
    after,
    lengths,
    rates,
    first,
    second,
    gain,
    w_key,
    w_value,
    w_gate,
    w_output,
    keys,
    k_out,
    v_out,
    g_out,
    turn,
    weights,
    w_keep,
    keys_out,
    key_buffer,
    value_buffer,
    gate_buffer,
    sems,
    cache_sems,
):
    own = w_keep.shape[1]
    kept = pl.ds(pl.multiple_of(lax.axis_index("tp") * own, own), own)
    buffers = (key_buffer, value_buffer, gate_buffer)
    pairs = (
        (w_key, key_buffer),
        (w_value, value_buffer),
        (w_gate, gate_buffer),
        (w_output.at[:, kept], w_keep),
    )
    copies = [pltpu.make_async_copy(a, b, sems.at[i]) for i, (a, b) in enumerate(pairs)]
    for copy in copies:
        copy.start()
    lhs, wide = projection_rows(first, second, gain)
    rows = wide.shape[0]
    live = live_scalars(lengths, lax.axis_index("kv") * keys.shape[1])[: rows * 3 // 4]
    caches = copies_of(keys, keys_out, cache_sems, 0, rows * 3 // 4)
    when_live(live, caches, lambda copy: copy.start())
    half = HEAD_KEY // 2
    entry = (lane_ids(rows) % half).astype(F32)
    inverse = jnp.exp(entry * (-math.log(THETA) / half))
    angle = lengths[...].astype(F32) * inverse
    turn[0] = jnp.cos(angle)
    turn[1] = jnp.sin(angle)
    heads = rates.shape[0]
    places = lax.axis_index("kv") * LANES + lane_ids(heads)
    rate = rates[...]
    for s in range(rows):
        distance = jnp.broadcast_to(lengths[s : s + 1, :], (heads, LANES)) - places
        weight = jnp.exp(-rate * jnp.maximum(distance, 0).astype(F32)) * HEAD_KEY ** (-0.5)
        weights[s] = jnp.where(distance > 0, weight, 0.0)
    for copy, buffer, out in zip(copies, buffers, (k_out, v_out, g_out)):
        copy.wait()
        product = jnp.dot(lhs, buffer[...], preferred_element_type=F32)
        out[...] = product[: rows + 8]
    for copy in copies[len(buffers) :]:
        copy.wait()
    when_live(live, caches, lambda copy: copy.wait())


def attend_kernel(
    width,
    after,
    lengths,
    old,
    m1,
    m2,
    m3,
    k_part,
    v_part,
    g_part,
    turn,
    weights,
    keys,
    values,
    out,
    query_rows,
    plain_rows,
    cached,
    order,
):
    rows, span, key_columns = keys.shape
    heads = key_columns // HEAD_KEY
    q, csum, moments = unpack_sum(old, (m1, m2, m3))
    average = moments[:, 0:1] / width
    inverse = lax.rsqrt(moments[:, 1:2] / width - average * average + EPS)
    lanes = lane_ids(rows)
    in_first = lanes % HEAD_KEY < HEAD_KEY // 2
    low_head = lanes < HEAD_KEY
    top = rows // 2
    cosine, sine = turn[0], turn[1]
    for i in range(key_columns // LANES):
        cut = slice(i * LANES, (i + 1) * LANES)
        plain = inverse * (q[:, cut] - average * csum[i : i + 1])
        partner = jnp.where(
            in_first,
            -pltpu.roll(plain, LANES - HEAD_KEY // 2, 1),
            pltpu.roll(plain, HEAD_KEY // 2, 1),
        )
        plain_rows[:, cut] = plain
        query_rows[:, cut] = (plain * cosine + partner * sine).astype(BF).astype(F32)

    def normed(part, cut):
        return inverse * (part[:rows, cut] - average * part[rows : rows + 1, cut])

    def side(i):
        cut = slice(i * LANES, (i + 1) * LANES)
        both = plain_rows[:, cut] * normed(k_part, cut) * HEAD_KEY ** (-0.5)
        for j in range(2):
            h = 2 * i + j
            picked = jnp.where(low_head == (j == 0), both, 0.0)
            score = jnp.sum(picked, 1, keepdims=True)
            high = score.astype(BF).astype(F32)
            low = score - high
            folded = jnp.where(
                lanes[:top] < HEAD_KEY,
                jnp.where(in_first[:top], high[:top], low[:top]),
                jnp.where(in_first[:top], high[top:], low[top:]),
            )
            out[h, 3 * rows :, :] = folded.astype(BF)
            cut = slice(h * LANES, (h + 1) * LANES)
            for place, part in ((1, v_part), (2, g_part)):
                out[h, place * rows : (place + 1) * rows, :] = normed(part, cut).astype(BF)

    head_of_key = lax.broadcasted_iota(jnp.int32, (heads, key_columns), 1) // HEAD_KEY
    own_key = head_of_key == row_ids(heads, key_columns)
    value_columns = heads * HEAD_VALUE
    head_of_value = lax.broadcasted_iota(jnp.int32, (heads, value_columns), 1) // HEAD_VALUE
    own_value = head_of_value == row_ids(heads, value_columns)
    live = live_scalars(lengths, lax.axis_index("kv") * span)
    count = jnp.int32(0)
    for s in range(rows):
        order[count] = s
        count = count + live[s].astype(jnp.int32)

    def one(s, is_live):
        row = pl.ds(s, 1)
        spread = jnp.broadcast_to(query_rows[row, :], (heads, key_columns))
        query = jnp.where(own_key, spread, 0.0).astype(BF)
        scores = lax.dot_general(
            query, keys[s], (((1,), (1,)), ((), ())), preferred_element_type=F32
        )
        weight = weights[s]
        coefficients = jnp.where(weight > 0.0, scores * weight, 0.0).astype(BF)
        product = jnp.dot(coefficients, values[s], preferred_element_type=F32)
        kept = jnp.logical_and(own_value, is_live)
        cached[row, :] = jnp.sum(jnp.where(kept, product, 0.0), 0, keepdims=True)

    quarter = rows // 4
    pairs = heads // 2
    for most in range(quarter, rows + 1, quarter):
        least = most - quarter if most > quarter else -1

        @pl.when(jnp.logical_and(count > least, count <= most))
        def _():
            if most < rows:
                cached[...] = jnp.zeros_like(cached)
            done = 0
            for i in range(most):
                if most == rows:
                    one(i, live[i])
                else:
                    one(order[jnp.minimum(i, jnp.maximum(count - 1, 0))], count > 0)
                while done * most < (i + 1) * pairs:
                    side(done)
                    done += 1

    for h in range(heads):
        out[h, :rows, :] = cached[:, h * LANES : (h + 1) * LANES].astype(BF)


def gate_kernel(pieces, head_gain, out):
    rows = out.shape[1]
    total = jnp.sum(pieces[...].astype(F32), 0)
    cached, value, gate = (total[i * rows : (i + 1) * rows] for i in range(3))
    folded = total[3 * rows :]
    half = HEAD_KEY // 2
    score = jnp.concatenate(
        [folded[:, i : i + 1] + folded[:, i + half : i + half + 1] for i in (0, HEAD_KEY)], 0
    )
    retained = cached + score * value
    centered = retained - jnp.mean(retained, -1, keepdims=True)
    spread = lax.rsqrt(jnp.mean(centered * centered, -1, keepdims=True) + EPS)
    gains = head_gain[...].astype(F32)
    mine = row_ids(gains.shape[0]) == lax.axis_index("kv")
    gain = jnp.sum(jnp.where(mine, gains, 0.0), 0, keepdims=True)
    normed = centered * spread * gain
    gated = (gate * jax.nn.sigmoid(gate) * normed).astype(BF)
    out[...] = jnp.broadcast_to(gated[None], out.shape)


def output_kernel(gated, w_keep, w_got, tokens, own, out):
    heads = gated.shape[0] // 2
    t = lax.axis_index("tp")
    branch = 0.0
    width = own.shape[1]
    columns = pl.ds(pl.multiple_of(t * width, width), width)
    for group, w in ((t, w_keep[...]), (1 - t, w_got[:, columns])):
        lhs = jnp.concatenate([gated[2 * h + group] for h in range(heads)], 1)
        part = jnp.dot(lhs, w, preferred_element_type=F32)
        branch = branch + part.astype(BF).astype(F32)
    residual = (tokens[...].astype(F32) + branch).astype(BF)
    own[...] = residual
    out[...] = jnp.broadcast_to(residual[None], out.shape)


def mixer_kernel(residual, mlp_gain, w_up, w_down, out):
    blocks, rows, own = residual.shape
    width = blocks * own
    first = jnp.zeros((rows, own), F32)
    second = jnp.zeros((rows, own), F32)
    scaled, gain = [], []
    gains = mlp_gain[...].astype(F32)
    for i in range(blocks):
        wide = residual[i].astype(F32)
        first = first + wide
        second = second + wide * wide
        row = gains[i : i + 1]
        scaled.append((wide * row).astype(BF))
        gain.append(jnp.broadcast_to(row, wide.shape).astype(BF))
    lhs = jnp.concatenate([jnp.concatenate(scaled, 1), jnp.concatenate(gain, 1)], 0)
    up = jnp.dot(lhs, w_up[...], preferred_element_type=F32)
    average = jnp.sum(first, 1, keepdims=True) / width
    inverse = lax.rsqrt(jnp.sum(second, 1, keepdims=True) / width - average * average + EPS)
    hidden = inverse * (up[:rows] - average * up[rows : rows + 1])
    hidden = jnp.square(jnp.maximum(hidden, 0.0)).astype(BF)
    down = jnp.dot(hidden, w_down[...], preferred_element_type=F32)
    for i in range(blocks):
        out[i] = down[:, i * own : (i + 1) * own].astype(BF)


def final_kernel(pieces, own, out):
    total = jnp.sum(pieces[...].astype(F32), 0)
    out[...] = (own[...].astype(F32) + total).astype(BF)


VMEM = pl.BlockSpec(memory_space=pltpu.VMEM)
HBM = pl.BlockSpec(memory_space=pltpu.HBM)
ANY = pl.BlockSpec(memory_space=pl.ANY)


def in_hbm(*arrays):
    return [pltpu.with_memory_space_constraint(x, pltpu.HBM) for x in arrays]


def call(kernel, outs, in_specs, flops=0, bytes_accessed=0, scratch=(), limit=None, aliases={}):
    return pl.pallas_call(
        kernel,
        out_shape=outs,
        in_specs=in_specs,
        out_specs=jax.tree.map(lambda _: VMEM, outs),
        scratch_shapes=list(scratch),
        input_output_aliases=aliases,
        cost_estimate=pl.CostEstimate(
            flops=flops, bytes_accessed=bytes_accessed, transcendentals=0
        ),
        compiler_params=pltpu.CompilerParams(vmem_limit_bytes=limit),
    )


def make_kernels_on_device(kv, tp):
    def on_device(
        tokens,
        lengths,
        attn_gain,
        w_query,
        w_key,
        w_value,
        w_gate,
        decay_rate,
        key_cache,
        value_cache,
        head_gain,
        w_output,
        mlp_gain,
        w_up,
        w_down,
    ):
        S, own = tokens.shape
        H = decay_rate.shape[0]
        width = own * kv * tp
        qc, vc = H * HEAD_KEY, H * HEAD_VALUE
        swap = [(0, 1), (1, 0)]
        mib = 1 << 20
        sds = jax.ShapeDtypeStruct

        other = lax.ppermute(tokens, "tp", swap)
        w_got = lax.ppermute(w_output, "tp", swap)
        gain = attn_gain.reshape(-1, LANES)
        w_query, tokens, gain, length_rows, rates = call(
            first_load_kernel,
            (
                sds(w_query.shape, BF),
                sds(tokens.shape, BF),
                sds(gain.shape, BF),
                sds((S, LANES), jnp.int32),
                sds((H, LANES), F32),
            ),
            [HBM] * 5,
            flops=10**9,
            scratch=[
                pltpu.SMEM((S,), jnp.int32),
                pltpu.SMEM((H,), F32),
                pltpu.SemaphoreType.DMA((5,)),
            ],
            limit=2 * mib,
        )(*in_hbm(w_query, tokens, gain, lengths, decay_rate))
        columns = qc + 2 * LANES
        message_types = (sds((S, columns), F32), sds((S, columns), BF))
        state, message = call(
            query_kernel, message_types, [VMEM] * 4, limit=2 * mib
        )(tokens, other, gain, w_query)

        def exchange(message, stride):
            got = []
            for j in range(1, 4):
                pairs = [(i, i ^ (j * stride)) for i in range(kv)]
                got.append(lax.ppermute(message, "kv", pairs))
            return got

        got = exchange(message, 1)
        k_part, v_part, g_part, turn, weights, w_keep, keys = call(
            other_kernel,
            (
                sds((S + 8, qc), F32),
                sds((S + 8, vc), F32),
                sds((S + 8, vc), F32),
                sds((2, S, LANES), F32),
                sds((S, H, LANES), F32),
                sds((w_output.shape[0], own), BF),
                sds(key_cache.shape, BF),
            ),
            [ANY] + [VMEM] * 5 + [HBM] * 5,
            flops=10**9,
            scratch=[pltpu.VMEM(w.shape, BF) for w in (w_key, w_value, w_gate)]
            + [pltpu.SemaphoreType.DMA((4,)), pltpu.SemaphoreType.DMA((S,))],
            limit=6 * mib,
        )(
            message,
            length_rows,
            rates,
            tokens,
            other,
            gain,
            *in_hbm(w_key, w_value, w_gate, w_output, key_cache),
        )

        stride = 4
        while stride < kv:
            state, message = call(
                middle_kernel, message_types, [VMEM] * 4, limit=2 * mib
            )(state, *got)
            got = exchange(message, stride)
            stride *= 4
        keys, values = call(
            cache_load_kernel,
            (sds(key_cache.shape, BF), sds(value_cache.shape, BF)),
            [ANY, VMEM] + [HBM] * 2 + [VMEM],
            flops=10**9,
            scratch=[pltpu.SemaphoreType.DMA((S,))] * 2,
            limit=2 * mib,
            aliases={4: 0},
        )(message, length_rows, *in_hbm(key_cache, value_cache), keys)

        pieces = call(
            functools.partial(attend_kernel, width),
            sds((H, 3 * S + S // 2, LANES), BF),
            [ANY] + [VMEM] * 12,
            scratch=[
                pltpu.VMEM((S, qc), F32),
                pltpu.VMEM((S, qc), F32),
                pltpu.VMEM((S, vc), F32),
                pltpu.SMEM((S,), jnp.int32),
            ],
            limit=4 * mib,
        )(w_got, length_rows, state, *got, k_part, v_part, g_part, turn, weights, keys, values)

        pieces = lax.all_to_all(pieces, "kv", 0, 0, tiled=True)
        gated = call(
            gate_kernel, sds((kv * tp, S, LANES), BF), [VMEM] * 2, limit=2 * mib
        )(pieces, head_gain.reshape(H, HEAD_VALUE))
        gated = lax.all_to_all(gated, ("kv", "tp"), 0, 0, tiled=True)
        residual, spread = call(
            output_kernel,
            (sds((S, own), BF), sds((kv * tp, S, own), BF)),
            [VMEM] * 4,
            limit=4 * mib,
        )(gated, w_keep, w_got, tokens)
        spread = lax.all_to_all(spread, ("kv", "tp"), 0, 0, tiled=True)
        down = call(
            mixer_kernel, sds((kv * tp, S, own), BF), [VMEM] * 4, limit=16 * mib
        )(spread, mlp_gain.reshape(-1, LANES), w_up, w_down)
        down = lax.all_to_all(down, ("kv", "tp"), 0, 0, tiled=True)
        return call(final_kernel, sds((S, own), BF), [VMEM] * 2, limit=2 * mib)(down, residual)

    return on_device


def solution(mesh):
    in_specs = (
        P(None, ("kv", "tp")),
        P(),
        P("kv"),
        P("kv", "tp"),
        P("kv", "tp"),
        P("kv", "tp"),
        P("kv", "tp"),
        P("tp"),
        P(None, "kv", "tp"),
        P(None, "kv", "tp"),
        P("tp"),
        P("tp", "kv"),
        P(),
        P(None, ("kv", "tp")),
        P(("kv", "tp"), None),
    )
    kv, tp = mesh.shape["kv"], mesh.shape["tp"]

    def on_device(*arrays):
        fits = tp == 2 and arrays[7].shape[0] == kv
        fits = fits and arrays[0].shape[1] == LANES == arrays[8].shape[1]
        make = make_kernels_on_device if fits else make_on_device
        return make(kv, tp)(*arrays)

    return jax.shard_map(
        on_device,
        mesh=mesh,
        in_specs=in_specs,
        out_specs=P(None, ("kv", "tp")),
        check_vma=False,
    )
```
